32 devices in a mesh: grp: 2 (over y), sp: 4 (over z), tp: 4 (over x, core).
Axes of the slice: x: 2, y: 2, z: 4, core: 2. Of those that a mesh axis runs over, the one named last changes fastest.
Arguments:
- tokens_in: bfloat16 [2048, 2048], P(('grp', 'sp')), parts along dimension 0, may hold values from -6 to 6
- input_gain: float32 [2048], replicated, may hold values from 0.1 to 1.9
- w_query: bfloat16 [2048, 1024], P('sp', 'tp'), may hold values from -0.125 to 0.125
- w_key: bfloat16 [2048, 1024], P('sp', 'tp'), may hold values from -1 to 1
- w_value: bfloat16 [2048, 1024], P('sp', 'tp'), may hold values from -0.125 to 0.125
- w_gates: bfloat16 [2048, 32], P('sp', 'tp'), may hold values from -3 to 3
- w_glu_value: bfloat16 [2048, 1024], P('sp', 'tp'), may hold values from -0.125 to 0.125
- sigmoid_opener_matrix: bfloat16 [2048, 1024], P('sp', 'tp'), may hold values from -0.125 to 0.125
- log_decay: float32 [2048, 16], P(('grp', 'sp'), 'tp'), parts along dimension 0, may hold values from -1 to 0
- head_gain: float32 [128], replicated, may hold values from 0.1 to 1.9
- conv_kernel: float32 [31, 1024], P(None, 'tp'), may hold values from -12 to 12
- norm_gain: float32 [1024], P('tp'), may hold values from 0.1 to 1.9
- norm_shift: float32 [1024], P('tp'), may hold values from -3 to 3
- out_delta: bfloat16 [2048, 1024], P(None, 'tp'), may hold values from -0.125 to 0.125
- out_conv: bfloat16 [2048, 1024], P(None, 'tp'), may hold values from -0.125 to 0.125
Outputs:
- mixed: bfloat16 [2048, 2048], P(('grp', 'sp'), 'tp'), parts along dimension 0
The draws below stay inside these ranges and needn't reach their ends.
There are 2 independent parts, one for each index of `grp`. The reference program is written for one: setup_inputs(seed, part) draws one part's arguments, and reference() takes and returns one part's arrays. A program takes and returns all parts, laid end to end along the dimension named above; an argument that names none is the same for every part. Nothing has to cross between parts.
All inputs are finite; a program needn't handle non-finite values.
Results may differ from the reference program's by a relative error of at most 0.015.
Values may be sent and summed in bfloat16 or wider, within the bound.
A program may use at most 64 MiB of HBM per device.

```python
import jax
import jax.numpy as jnp
from jax import lax

D = 2048
HEADS = 8
HEAD_DIM = 128
CONV_CH = 1024
KERNEL = 31
BLOCK = 64
TOK_DEV = 256
SEQ = 1024
A_W = 1024
N_TP = 4


def draw_log_decay(key, part):
    streams = jax.random.split(jax.random.fold_in(key, 11), 6)
    columns = 2 * HEADS
    fast_share = 0.5
    picker = jax.random.uniform(streams[0], (columns,), jnp.float32)
    fast_rate = jax.random.uniform(streams[1], (columns,), jnp.float32, 0.015, 0.04)
    slow_rate = jax.random.uniform(streams[2], (columns,), jnp.float32, 0.04, 0.16) / SEQ
    forgetting_pace = jnp.where(picker < fast_share, fast_rate, slow_rate)
    multiplier_amount = jnp.exp(jax.random.uniform(streams[3], (SEQ // TOK_DEV, columns), jnp.float32, 0.0, 1.0986))
    multiplier_amount = jnp.repeat(multiplier_amount, TOK_DEV, axis=0)
    spots = jax.random.randint(streams[4], (2, columns), 0, SEQ)
    places = jnp.arange(SEQ)[:, None]
    masked_elements = (places == spots[0][None, :]) | (places == spots[1][None, :])
    objective_readings = jax.random.uniform(streams[5], (SEQ, columns), jnp.float32, 0.2, 0.35)
    clustered_bunches = jnp.where(masked_elements, jnp.log(1.0 - objective_readings), 0.0)
    return (-(forgetting_pace[None, :] * multiplier_amount) + clustered_bunches).astype(jnp.float32)


def draw_conv_kernel(key, part):
    streams = jax.random.split(jax.random.fold_in(key, 23), 2)
    channel_slot = jnp.arange(CONV_CH).astype(jnp.float32)
    random_perturbation = jax.random.uniform(streams[1], (CONV_CH,), jnp.float32)
    entries = jnp.clip(jax.random.normal(streams[0], (KERNEL, CONV_CH), jnp.float32), -4.0, 4.0)
    reach = 10.0
    scale = reach ** ((channel_slot + random_perturbation) / CONV_CH)
    return (entries * scale[None, :] / jnp.sqrt(float(KERNEL))).astype(jnp.float32)


def unit_entries(stream, shape):
    return jnp.clip(jax.random.normal(stream, shape, jnp.float32), -4.0, 4.0)


def draw_w_key(key, part):
    streams = jax.random.split(jax.random.fold_in(key, 31), 2)
    strong_count = HEAD_DIM * 3 // 8
    weak_energy = 0.356 * (HEAD_DIM - strong_count)
    ratio_square = max(1.0, (0.04 * SEQ - weak_energy) / (0.5 * strong_count))
    orders = jax.vmap(lambda sub_key: jax.random.permutation(sub_key, HEAD_DIM))(jax.random.split(streams[0], HEADS))
    column_scale = jnp.where(orders < strong_count, ratio_square ** 0.5, 1.0).reshape(HEADS * HEAD_DIM).astype(jnp.float32)
    entries = unit_entries(streams[1], (D, HEADS * HEAD_DIM))
    return (entries * column_scale[None, :] / jnp.sqrt(float(D))).astype(jnp.bfloat16)


def draw_w_gates(key, part):
    stream = jax.random.fold_in(key, 37)
    roles = jnp.arange(4 * HEADS) % 4
    column_scale = jnp.where((roles == 1) | (roles == 3), 4.0, 1.0).astype(jnp.float32)
    entries = unit_entries(stream, (D, 4 * HEADS))
    return (entries * column_scale[None, :] / jnp.sqrt(float(D))).astype(jnp.bfloat16)


def shard_levels(key, extent, shards, smallest, top_value):
    level = 1.0
    for axis_at, parts in shards:
        heights = jax.random.uniform(jax.random.fold_in(jax.random.fold_in(key, 6), axis_at), (parts,), jnp.float32, smallest / len(shards), top_value / len(shards))
        level = level * jnp.repeat(jnp.exp(heights), extent[axis_at] // parts).reshape((-1,) + (1,) * (len(extent) - 1 - axis_at))
    return level


def bell_draw(rng, dims, scale, most, cuts=(), kind=jnp.bfloat16):
    array = jax.random.normal(rng, dims, jnp.float32) * scale
    if len(cuts) > 0:
        array = shard_levels(rng, dims, cuts, -0.22, 0.18) * array
    return jnp.clip(array, min=-most, max=most).astype(kind)


def setup_inputs(seed: int = 0, part: int = 0) -> dict:
    key_list = jax.random.split(jax.random.key(seed), 16)
    part_keys = jax.random.split(jax.random.fold_in(key_list[15], part), 16)
    tokens_in = bell_draw(part_keys[0], (SEQ, D), 1.0, 6.0, ((0, 4),))
    input_gain = jnp.clip(1.0 + 0.18 * jax.random.normal(key_list[1], (D,), jnp.float32), 0.1, 1.9)
    w_query = bell_draw(key_list[2], (D, A_W), D ** -0.5, 0.125, ((0, 4), (1, 4)))
    w_key = draw_w_key(jax.random.fold_in(key_list[15], 71), part)
    w_value = bell_draw(key_list[4], (D, A_W), D ** -0.5, 0.125, ((0, 4), (1, 4)))
    w_gates = draw_w_gates(jax.random.fold_in(key_list[15], 71), part)
    w_glu_value = bell_draw(key_list[6], (D, CONV_CH), D ** -0.5, 0.125, ((0, 4), (1, 4)))
    sigmoid_opener_matrix = bell_draw(key_list[7], (D, CONV_CH), D ** -0.5, 0.125, ((0, 4), (1, 4)))
    log_decay = draw_log_decay(jax.random.fold_in(jax.random.fold_in(key_list[15], part), 71), part)
    head_gain = jnp.clip(1.0 + 0.18 * jax.random.normal(key_list[9], (HEAD_DIM,), jnp.float32), 0.1, 1.9)
    conv_kernel = draw_conv_kernel(jax.random.fold_in(key_list[15], 71), part)
    norm_gain = jnp.clip(1.0 + 0.18 * jax.random.normal(key_list[11], (CONV_CH,), jnp.float32), 0.1, 1.9)
    norm_shift = bell_draw(key_list[12], (CONV_CH,), 0.5, 3.0, ((0, 4),), jnp.float32)
    out_delta = bell_draw(key_list[13], (D, A_W), (A_W + CONV_CH) ** -0.5, 0.125, ((1, 4),))
    out_conv = bell_draw(key_list[14], (D, CONV_CH), (A_W + CONV_CH) ** -0.5, 0.125, ((1, 4),))
    return {"tokens_in": tokens_in, "input_gain": input_gain, "w_query": w_query, "w_key": w_key, "w_value": w_value, "w_gates": w_gates, "w_glu_value": w_glu_value, "sigmoid_opener_matrix": sigmoid_opener_matrix, "log_decay": log_decay, "head_gain": head_gain, "conv_kernel": conv_kernel, "norm_gain": norm_gain, "norm_shift": norm_shift, "out_delta": out_delta, "out_conv": out_conv}


PRECISE = lax.Precision.HIGHEST
EPSILON = 1e-06
BETA_SHIFT = 6.0

def high_dot(left, right):
    return jnp.matmul(left, right, precision=PRECISE)

def swap_last(tensor):
    return jnp.swapaxes(tensor, -1, -2)

def block_terms(query, key_rows, values, decay_log, beta_rate, block):
    head_count, length = (query.shape[0], query.shape[1])
    blocks = length // block

    def to_blocks(tensor):
        return tensor.reshape((head_count, blocks, block) + tensor.shape[2:])
    query, key_rows, values, decay_log, beta_rate = (to_blocks(tensor) for tensor in (query, key_rows, values, decay_log, beta_rate))
    cumulative = jnp.cumsum(decay_log, axis=-1)
    positions = jnp.arange(block)
    on_or_below = positions[:, None] >= positions[None, :]
    strict = positions[:, None] > positions[None, :]
    log_gaps = cumulative[..., :, None] - cumulative[..., None, :]
    weighting = jnp.where(on_or_below, jnp.exp(jnp.where(on_or_below, log_gaps, 0.0)), 0.0)
    scaled_keys = key_rows * beta_rate[..., None]
    lower_part = jnp.where(strict, high_dot(scaled_keys, swap_last(key_rows)) * weighting, 0.0)
    identity = jnp.eye(block, dtype=jnp.float32)
    inverse = jax.scipy.linalg.solve_triangular(identity + lower_part, jnp.broadcast_to(identity, lower_part.shape), lower=True, unit_diagonal=True)
    update = high_dot(inverse, values * beta_rate[..., None])
    mixed_keys = high_dot(inverse, scaled_keys * jnp.exp(cumulative)[..., None])
    in_block = jnp.where(on_or_below, high_dot(query, swap_last(key_rows)) * weighting, 0.0)
    q_decayed = query * jnp.exp(cumulative)[..., None]
    k_decayed = key_rows * jnp.exp(cumulative[..., -1:] - cumulative)[..., None]
    end_decay = jnp.exp(cumulative[..., -1])
    return tuple((jnp.moveaxis(tensor, 1, 0) for tensor in (update, mixed_keys, in_block, q_decayed, k_decayed, end_decay)))

def delta_scan(query, key_rows, values, decay_log, beta_rate):
    stacked = block_terms(query, key_rows, values, decay_log, beta_rate, BLOCK)
    head_count, length, head_width = query.shape

    def advance(state_now, pieces):
        update, mixed_keys, in_block, q_decayed, k_decayed, end_decay = pieces
        new_values = update - high_dot(mixed_keys, state_now)
        output = high_dot(q_decayed, state_now) + high_dot(in_block, new_values)
        state_now = state_now * end_decay[:, None, None] + high_dot(swap_last(k_decayed), new_values)
        return (state_now, output)
    zero_state = jnp.zeros((head_count, head_width, values.shape[2]), jnp.float32)
    _, output = lax.scan(advance, zero_state, stacked)
    return jnp.moveaxis(output, 0, 1).reshape(head_count, length, values.shape[2])

def reference(tokens_in, input_gain, w_query, w_key, w_value, w_gates, w_glu_value, sigmoid_opener_matrix, log_decay, head_gain, conv_kernel, norm_gain, norm_shift, out_delta, out_conv):
    rows = tokens_in.astype(jnp.float32)
    normed = (rows * lax.rsqrt(lax.optimization_barrier(jnp.mean(rows * rows, axis=-1, keepdims=True)) + EPSILON) * input_gain).astype(jnp.bfloat16)

    def project(weight):
        return jnp.dot(normed.astype(jnp.float32), weight.astype(jnp.float32), preferred_element_type=jnp.float32)

    def by_head(tensor):
        return jnp.swapaxes(jax.nn.silu(tensor).reshape(SEQ, HEADS, HEAD_DIM), 0, 1)

    def unit_rows(tensor):
        return tensor * lax.rsqrt(lax.optimization_barrier(jnp.sum(tensor * tensor, axis=-1, keepdims=True)) + EPSILON)
    query = unit_rows(by_head(project(w_query))) * HEAD_DIM ** (-0.5)
    key_rows = unit_rows(by_head(project(w_key)))
    values = by_head(project(w_value))
    gate_parts = project(w_gates).reshape(SEQ, HEADS, 4)
    rate_parts = log_decay.reshape(SEQ, HEADS, 2)
    decay_fore = jnp.swapaxes(rate_parts[:, :, 0] * (0.5 + jax.nn.sigmoid(gate_parts[:, :, 0])), 0, 1)
    beta_fore = jnp.swapaxes(jax.nn.sigmoid(gate_parts[:, :, 1] - BETA_SHIFT), 0, 1)
    decay_back = jnp.swapaxes(rate_parts[:, :, 1] * (0.5 + jax.nn.sigmoid(gate_parts[:, :, 2])), 0, 1)
    beta_back = jnp.swapaxes(jax.nn.sigmoid(gate_parts[:, :, 3] - BETA_SHIFT), 0, 1)

    def reversed_rows(tensor):
        return jnp.flip(tensor, axis=1)
    fore = delta_scan(query, key_rows, values, decay_fore, beta_fore)
    back = reversed_rows(delta_scan(reversed_rows(query), reversed_rows(key_rows), reversed_rows(values), reversed_rows(decay_back), reversed_rows(beta_back)))
    joined = fore + back
    joined = joined * lax.rsqrt(lax.optimization_barrier(jnp.mean(joined * joined, axis=-1, keepdims=True)) + EPSILON) * head_gain
    delta_mix = jnp.swapaxes(joined, 0, 1).reshape(SEQ, HEADS * HEAD_DIM).astype(jnp.bfloat16)
    glu_rows = (project(w_glu_value) * jax.nn.sigmoid(project(sigmoid_opener_matrix))).astype(jnp.bfloat16)
    half_width = KERNEL // 2
    padded = jnp.pad(glu_rows.astype(jnp.float32), ((half_width, half_width), (0, 0)))
    conv_rows = padded[0:SEQ] * conv_kernel[0]
    for offset in range(1, KERNEL):
        conv_rows = conv_rows + padded[offset:offset + SEQ] * conv_kernel[offset]
    center = lax.optimization_barrier(jnp.mean(conv_rows, axis=-1))
    spread = lax.optimization_barrier(jnp.mean(conv_rows * conv_rows, axis=-1)) - center * center
    normal_rows = (conv_rows - center[:, None]) * lax.rsqrt(spread + EPSILON)[:, None]
    filtered_blend = jax.nn.silu(normal_rows * norm_gain + norm_shift).astype(jnp.bfloat16)
    head_cols = HEADS * HEAD_DIM // N_TP
    channel_columns = CONV_CH // N_TP
    result = jnp.zeros((SEQ, D), jnp.float32)
    for group in range(N_TP):
        partial_sum = jnp.dot(delta_mix[:, group * head_cols:(group + 1) * head_cols].astype(jnp.float32), out_delta[:, group * head_cols:(group + 1) * head_cols].T.astype(jnp.float32), preferred_element_type=jnp.float32)
        partial_sum = partial_sum + jnp.dot(filtered_blend[:, group * channel_columns:(group + 1) * channel_columns].astype(jnp.float32), out_conv[:, group * channel_columns:(group + 1) * channel_columns].T.astype(jnp.float32), preferred_element_type=jnp.float32)
        rounded = lax.optimization_barrier(partial_sum.astype(jnp.bfloat16))
        result = result + rounded.astype(jnp.float32)
    return result.astype(jnp.bfloat16)
```

```python
import functools

import jax
import jax.numpy as jnp
from jax import lax
from jax.experimental import pallas as pl
from jax.experimental.pallas import tpu as pltpu
from jax.sharding import PartitionSpec as P

EPSILON = 1e-06
BETA_SHIFT = 6.0
HALO = 16
MESH = pl.DeviceIdType.MESH
F32 = jnp.float32
BF16 = jnp.bfloat16
NT = (((1,), (1,)), ((), ()))
TN = (((0,), (0,)), ((), ()))
NN = (((1,), (0,)), ((), ()))
KEY, GATE, VALUE, QUERY, GLU, OPEN = range(6)


def bdot(left, right, dims=NN):
    return lax.dot_general(
        left.astype(BF16), right.astype(BF16), dims, preferred_element_type=F32
    )


def each(count, action):
    if count <= 8:
        for step in range(count):
            action(step)
    else:
        def body(step, carry):
            action(step)
            return carry

        lax.fori_loop(0, count, body, 0)


def kernel(cfg, tok_h, gain, wk_h, wg_h, wv_h, wq_h, wa_h, wb_h, ld, ldt, hgain, ck, ng, ns, od_h, oc_h,
           out,
           tok, normed, wk, wg, wv, wq, wa, wb, od, oc,
           keys, vals, betas, cums, xinv, gaps, rhs, local_out, reads, maps, ends,
           chain_in, chain_out, glu, halo, pad, conv, stat_out, stat_in, conv_acc, part_out, part_in, pair_out, pair_in,
           local_sem, z_send, z_recv, y_send, y_recv, chain_send, chain_recv,
           halo_send, halo_recv, stat_send, stat_recv, part_send, part_recv, pair_send, pair_recv):
    n_grp, n_sp, n_tp, conv_total = cfg
    grp, sp, tp = lax.axis_index("grp"), lax.axis_index("sp"), lax.axis_index("tp")
    length, width = tok.shape
    rows = wk_h.shape[0]
    channels = wa.shape[1]
    head_width = hgain.shape[1]
    heads = wk.shape[1] // head_width
    share = (rows // 2) // 16 * 16 if n_grp == 2 else 0
    pulled = rows - share

    sources = (wk_h, wg_h, wv_h, wq_h, wa_h, wb_h)
    targets = (wk, wg, wv, wq, wa, wb)

    def block_of(w, index, start, count):
        if w == GATE:
            return targets[w].at[index]
        return targets[w].at[pl.ds(pl.multiple_of(index * rows + start, 16), count)]

    load_tok = pltpu.make_async_copy(tok_h, tok, local_sem.at[0])
    load_tok.start()
    own = [
        pltpu.make_async_copy(sources[w], block_of(w, sp, 0, rows), local_sem.at[1 + w])
        for w in range(6)
    ]
    for copy in own:
        copy.start()
    load_od = pltpu.make_async_copy(od_h, od, local_sem.at[7])
    load_oc = pltpu.make_async_copy(oc_h, oc, local_sem.at[8])

    barrier = pltpu.get_barrier_semaphore()

    def greet(axis, me, count):
        def one(step):
            pl.semaphore_signal(
                barrier, inc=1, device_id={axis: lax.rem(me + step + 1, count)}, device_id_type=MESH
            )

        each(count - 1, one)

    greet("sp", sp, n_sp)
    greet("tp", tp, n_tp)
    greet("grp", grp, n_grp)
    pl.semaphore_wait(barrier, n_sp + n_tp + n_grp - 3)

    def origin(side, d):
        return sp - d if side == 0 else sp + d

    def arrives(side, d):
        return sp - d >= 0 if side == 0 else sp + d < n_sp

    def leaves(side, d):
        if side == 0:
            return (sp - (d - 1) >= 0) & (sp < n_sp - 1)
        return (sp + (d - 1) < n_sp) & (sp > 0)

    def part_of(w, index, side_of):
        if w == GATE:
            return block_of(w, index, 0, 0)
        if not share:
            return block_of(w, index, 0, rows)
        if side_of is None:
            return block_of(w, index, pl.multiple_of(grp * share, 16), pulled)
        return block_of(w, index, pl.multiple_of(side_of * pulled, 16), share)

    def z_copy(w, side, d, first=False):
        target = part_of(w, origin(side, d - 1), None)
        source = target
        if first:
            source = sources[w]
            if w != GATE and share:
                source = source.at[pl.ds(pl.multiple_of(grp * share, 16), pulled)]
        return pltpu.make_async_remote_copy(
            src_ref=source, dst_ref=target,
            send_sem=z_send.at[w, side, d - 1], recv_sem=z_recv.at[w, side, d - 1],
            device_id={"sp": sp + 1 if side == 0 else sp - 1}, device_id_type=MESH,
        )

    def z_arrival(w, side, d):
        place = part_of(w, origin(side, d), None)
        return pltpu.make_async_remote_copy(
            src_ref=place, dst_ref=place,
            send_sem=z_send.at[w, side, d - 1], recv_sem=z_recv.at[w, side, d - 1],
            device_id={"sp": sp + 1 if side == 0 else sp - 1}, device_id_type=MESH,
        )

    def y_copy(w, side, d, arriving=False):
        place = part_of(w, origin(side, d), 1 - grp if arriving else grp)
        return pltpu.make_async_remote_copy(
            src_ref=place, dst_ref=place,
            send_sem=y_send.at[w, side, d - 1], recv_sem=y_recv.at[w, side, d - 1],
            device_id={"grp": 1 - grp}, device_id_type=MESH,
        )

    def offer(w):
        for side in range(2):
            @pl.when(leaves(side, 1))
            def _(side=side):
                z_copy(w, side, 1, True).start()

    def relay_hop(w, d):
        for side in range(2):
            @pl.when(arrives(side, d))
            def _(side=side):
                z_arrival(w, side, d).wait_recv()

                @pl.when(leaves(side, d + 1))
                def _():
                    z_copy(w, side, d + 1).start()

                if share and w != GATE:
                    y_copy(w, side, d).start()

    def relay(w, low=1, high=None):
        if high is None:
            each(n_sp - low, lambda step: relay_hop(w, step + low))
        else:
            for d in range(low, min(high, n_sp - 1) + 1):
                relay_hop(w, d)

    def complete(w):
        own[w].wait()
        if share and w != GATE:
            def one(step):
                for side in range(2):
                    @pl.when(arrives(side, step + 1))
                    def _(side=side):
                        y_copy(w, side, step + 1, True).wait_recv()

            each(n_sp - 1, one)

    offer(KEY)
    offer(GATE)
    offer(VALUE)
    load_od.start()
    load_oc.start()

    load_tok.wait()
    chunk = 64
    for at in range(0, length, chunk):
        here = tok[at:at + chunk, :].astype(F32)
        scale = lax.rsqrt(jnp.mean(here * here, axis=-1, keepdims=True) + EPSILON)
        normed[at:at + chunk, :] = (here * scale * gain[...]).astype(BF16)

    def project(w):
        return jnp.dot(normed[...], targets[w][...], preferred_element_type=F32)

    def unit_rows(tensor):
        return tensor * lax.rsqrt(jnp.sum(tensor * tensor, axis=-1, keepdims=True) + EPSILON)

    def silu(tensor):
        return tensor * jax.nn.sigmoid(tensor)

    relay(GATE)
    relay(KEY)
    offer(QUERY)
    complete(GATE)
    gate_cols = jnp.zeros((length, 4 * heads), F32)
    gate_rows = jnp.zeros((4 * heads, length), F32)
    for index in range(n_sp):
        normed_part = normed[:, index * rows:(index + 1) * rows]
        gate_cols = gate_cols + lax.dot_general(normed_part, wg[index], NT, preferred_element_type=F32)
        gate_rows = gate_rows + lax.dot_general(wg[index], normed_part, NT, preferred_element_type=F32)

    row_at = lax.broadcasted_iota(jnp.int32, (length, length), 0)
    col_at = lax.broadcasted_iota(jnp.int32, (length, length), 1)

    complete(KEY)
    key_proj = silu(project(KEY))
    pairs = [(h, r) for h in range(heads) for r in range(2)]
    for h in range(heads):
        keys[h] = unit_rows(key_proj[:, h * head_width:(h + 1) * head_width])
    relay(VALUE, 1, 1)
    for h in range(heads):
        grams = bdot(keys[h], keys[h], NT)
        for r in range(2):
            p = 2 * h + r
            decay_col = ld[:, p:p + 1] * (0.5 + jax.nn.sigmoid(gate_cols[:, 2 * p:2 * p + 1]))
            decay_row = ldt[p:p + 1, :] * (0.5 + jax.nn.sigmoid(gate_rows[2 * p:2 * p + 1, :]))
            beta = jax.nn.sigmoid(gate_cols[:, 2 * p + 1:2 * p + 2] - BETA_SHIFT)
            if r == 0:
                seen_down, seen_across = row_at <= col_at, col_at <= row_at
            else:
                seen_down, seen_across = row_at >= col_at, col_at >= row_at
            cum_row = jnp.sum(jnp.where(seen_down, decay_col, 0.0), axis=0, keepdims=True)
            cum_col = jnp.sum(jnp.where(seen_across, decay_row, 0.0), axis=1, keepdims=True)
            weighting = jnp.where(
                seen_across, jnp.exp(jnp.where(seen_across, cum_col - cum_row, 0.0)), 0.0
            )
            gaps[p] = weighting
            betas[p] = jnp.broadcast_to(beta, (length, head_width))
            cums[p] = jnp.broadcast_to(cum_col, (length, head_width))
            lower = jnp.where(row_at != col_at, grams * weighting * beta, 0.0)
            rhs[p] = lower
            near = (row_at // 2 == col_at // 2)
            xinv[p] = jnp.where(row_at == col_at, 1.0, jnp.where(near, -lower, 0.0))

    size = 2
    while size < length:
        inside = (row_at // (2 * size) == col_at // (2 * size)) & (row_at // size != col_at // size)
        for p in range(len(pairs)):
            across = jnp.where(inside, rhs[p], 0.0)
            inverse = xinv[p]
            xinv[p] = inverse - bdot(inverse, bdot(across, inverse))
        if size == 2:
            relay(VALUE, 2)
            offer(GLU)
        if size == 32:
            relay(QUERY, 1, 1)
        if size == 128:
            relay(QUERY, 2, 2)
        size *= 2

    complete(VALUE)
    value_proj = silu(project(VALUE))
    eye = (
        lax.broadcasted_iota(jnp.int32, (head_width, head_width), 0)
        == lax.broadcasted_iota(jnp.int32, (head_width, head_width), 1)
    )
    for h, r in pairs:
        p = 2 * h + r
        beta, cum, key = betas[p], cums[p], keys[h]
        value = value_proj[:, h * head_width:(h + 1) * head_width]
        total = cum[length - 1:length, :] if r == 0 else cum[0:1, :]
        right = jnp.concatenate([beta * value, beta * key * jnp.exp(cum)], axis=1)
        solved = bdot(xinv[p], right)
        vals[p] = solved.astype(BF16)
        passed = bdot(key * jnp.exp(total - cum), solved, TN)
        ends[p] = passed[:, :head_width]
        maps[p] = (jnp.where(eye, jnp.exp(total), 0.0) - passed[:, head_width:]).astype(BF16)

    def place_of(r):
        return sp if r == 0 else n_sp - 1 - sp

    def chain_copy(r):
        dest = lax.rem(sp + 1, n_sp) if r == 0 else lax.rem(sp + n_sp - 1, n_sp)
        return pltpu.make_async_remote_copy(
            src_ref=chain_out.at[r], dst_ref=chain_in.at[r],
            send_sem=chain_send.at[r], recv_sem=chain_recv.at[r],
            device_id={"sp": dest}, device_id_type=MESH,
        )

    def chain_point(low, high):
        for r in range(2):
            at = place_of(r)

            @pl.when((at >= low) & (at <= high))
            def _(r=r, at=at):
                if low == 0:
                    for h in range(heads):
                        chain_in[r, h] = jnp.zeros((head_width, head_width), BF16)
                        chain_out[r, h] = ends[2 * h + r].astype(BF16)
                else:
                    chain_copy(r).wait_recv()
                    for h in range(heads):
                        p = 2 * h + r
                        chain_out[r, h] = (bdot(maps[p], chain_in[r, h]) + ends[p]).astype(BF16)

                @pl.when(at < n_sp - 1)
                def _():
                    chain_copy(r).start()

    chain_point(0, 0)
    relay(QUERY, 3)
    offer(OPEN)
    relay(GLU, 1, 1)
    complete(QUERY)
    query_proj = silu(project(QUERY))
    for h in range(heads):
        query = unit_rows(query_proj[:, h * head_width:(h + 1) * head_width]) * head_width ** -0.5
        scores = bdot(query, keys[h], NT)
        for r in range(2):
            p = 2 * h + r
            both = jnp.dot((scores * gaps[p]).astype(BF16), vals[p], preferred_element_type=F32)
            reads[p] = (query * jnp.exp(cums[p]) - both[:, head_width:]).astype(BF16)
            if r == 0:
                local_out[h] = both[:, :head_width]
            else:
                local_out[h] = local_out[h] + both[:, :head_width]
    chain_point(1, 1)
    relay(GLU, 2, 2)
    chain_point(2, 2)
    relay(GLU, 3)
    relay(OPEN, 1, 1)
    chain_point(3, n_sp - 1)
    complete(GLU)
    glu_proj = project(GLU)
    relay(OPEN, 2)
    complete(OPEN)
    gated = (glu_proj * jax.nn.sigmoid(project(OPEN))).astype(BF16)
    glu[...] = gated
    pad[HALO:HALO + length, :] = gated.astype(F32)

    def halo_copy(r):
        start = length - HALO if r == 0 else 0
        dest = lax.rem(sp + 1, n_sp) if r == 0 else lax.rem(sp + n_sp - 1, n_sp)
        return pltpu.make_async_remote_copy(
            src_ref=glu.at[pl.ds(start, HALO)], dst_ref=halo.at[r],
            send_sem=halo_send.at[r], recv_sem=halo_recv.at[r],
            device_id={"sp": dest}, device_id_type=MESH,
        )

    for r in range(2):
        @pl.when(place_of(r) < n_sp - 1)
        def _(r=r):
            halo_copy(r).start()
    for r in range(2):
        start = 0 if r == 0 else HALO + length

        @pl.when(place_of(r) > 0)
        def _(r=r, start=start):
            halo_copy(r).wait_recv()
            pad[start:start + HALO, :] = halo[r].astype(F32)

        @pl.when(place_of(r) == 0)
        def _(start=start):
            pad[start:start + HALO, :] = jnp.zeros((HALO, channels), F32)

    taps = ck.shape[0]
    for at in range(0, length, chunk):
        first = at + HALO - taps // 2
        total = pad[first:first + chunk, :] * ck[0:1, :]
        for j in range(1, taps):
            total = total + pad[first + j:first + j + chunk, :] * ck[j:j + 1, :]
        conv[at:at + chunk, :] = total
    filtered = conv[...]
    sum_col = jnp.sum(filtered, axis=-1, keepdims=True)
    square_col = jnp.sum(filtered * filtered, axis=-1, keepdims=True)
    same = row_at == col_at
    stat_out[...] = jnp.zeros(stat_out.shape, F32)
    stat_out[0:1, :] = jnp.sum(jnp.where(same, sum_col, 0.0), axis=0, keepdims=True)
    stat_out[1:2, :] = jnp.sum(jnp.where(same, square_col, 0.0), axis=0, keepdims=True)

    def stat_copy(step):
        return pltpu.make_async_remote_copy(
            src_ref=stat_out, dst_ref=stat_in.at[step],
            send_sem=stat_send.at[step], recv_sem=stat_recv.at[step],
            device_id={"tp": lax.rem(tp + step + 1, n_tp)}, device_id_type=MESH,
        )

    for step in range(n_tp - 1):
        stat_copy(step).start()

    joined_heads = []
    for h in range(heads):
        joined = local_out[h] + jnp.dot(reads[2 * h], chain_in[0, h], preferred_element_type=F32)
        joined = joined + jnp.dot(reads[2 * h + 1], chain_in[1, h], preferred_element_type=F32)
        scale = lax.rsqrt(jnp.mean(joined * joined, axis=-1, keepdims=True) + EPSILON)
        joined_heads.append((joined * scale * hgain[...]).astype(BF16))
    delta_mix = jnp.concatenate(joined_heads, axis=1) if heads > 1 else joined_heads[0]
    load_od.wait()
    load_oc.wait()
    columns = width // n_tp
    for dest in range(n_tp):
        at = slice(dest * columns, (dest + 1) * columns)
        conv_acc[dest] = lax.dot_general(delta_mix, od[at, :], NT, preferred_element_type=F32)

    stats = stat_out[0:2, :]
    for step in range(n_tp - 1):
        stat_copy(step).wait_recv()
        stats = stats + stat_in[step, 0:2, :]
    center = jnp.sum(jnp.where(same, stats[0:1, :], 0.0), axis=1, keepdims=True) / conv_total
    squares = jnp.sum(jnp.where(same, stats[1:2, :], 0.0), axis=1, keepdims=True) / conv_total
    spread = squares - center * center
    normal = (filtered - center) * lax.rsqrt(spread + EPSILON)
    conv_mix = silu(normal * ng[...] + ns[...]).astype(BF16)

    chip, core = tp // 2, lax.rem(tp, 2)
    chips = n_tp // 2
    sibling = chip * 2 + 1 - core

    def there(p, place):
        return lax.rem(chip + p, chips) * 2 + place

    def term_of(dest):
        at = pl.ds(pl.multiple_of(dest * columns, 16), columns)
        return conv_acc[dest] + lax.dot_general(conv_mix, oc[at, :], NT, preferred_element_type=F32)

    def pair_copy(p):
        return pltpu.make_async_remote_copy(
            src_ref=pair_out.at[p], dst_ref=pair_in.at[p],
            send_sem=pair_send.at[p], recv_sem=pair_recv.at[p],
            device_id={"tp": sibling}, device_id_type=MESH,
        )

    def part_copy(p):
        return pltpu.make_async_remote_copy(
            src_ref=part_out.at[p - 1], dst_ref=part_in.at[p - 1],
            send_sem=part_send.at[p - 1], recv_sem=part_recv.at[p - 1],
            device_id={"tp": there(p, core)}, device_id_type=MESH,
        )

    slots = list(range(1, chips)) + [0]
    for p in slots:
        pair_out[p] = term_of(there(p, 1 - core)).astype(BF16)
        pair_copy(p).start()
    for p in slots:
        term = term_of(there(p, core))
        pair_copy(p).wait_recv()
        term = term + pair_in[p].astype(F32)
        if p:
            part_out[p - 1] = term.astype(BF16)
            part_copy(p).start()
        else:
            result = term
    for p in range(1, chips):
        part_copy(p).wait_recv()
        result = result + part_in[p - 1].astype(F32)
    out[...] = result.astype(BF16)

    for w in range(6):
        def one(step, w=w):
            for side in range(2):
                @pl.when(leaves(side, step + 1))
                def _(side=side):
                    z_copy(w, side, step + 1).wait_send()

                if share and w != GATE:
                    @pl.when(arrives(side, step + 1))
                    def _(side=side):
                        y_copy(w, side, step + 1).wait_send()

        each(n_sp - 1, one)
    for r in range(2):
        @pl.when(place_of(r) < n_sp - 1)
        def _(r=r):
            chain_copy(r).wait_send()
            halo_copy(r).wait_send()
    for step in range(n_tp - 1):
        stat_copy(step).wait_send()
    for p in range(chips):
        pair_copy(p).wait_send()
        if p:
            part_copy(p).wait_send()


def fused(cfg, tok_h, gain, wk_h, wg_h, wv_h, wq_h, wa_h, wb_h, ldt, hgain, ck, ng, ns, od_h, oc_h,
          out,
          tok, nt, wk, wv, wq, wab, wg, odg, ocg, ldo,
          keys, vals, betas, cums, xinv, gaps, rhs, local_out, reads, maps, ends,
          chain_in, chain_out, gout, gend, main_in, edge_in, pad, conv, stat_out, stat_in,
          dall, dm_out, call,
          local_sem, z_send, z_recv, ty_send, ty_recv, tf_send, tf_recv, tz_send, tz_recv,
          ld_send, ld_recv, od_send, od_recv, chain_send, chain_recv,
          main_send, main_recv, edge_send, edge_recv, far_send, rim_send,
          stat_send, stat_recv, dg_send, dg_recv, df_send, df_recv, cg_send, cg_recv, cf_send, cf_recv):
    n_sp, n_tp, conv_total = cfg
    grp, sp, tp = lax.axis_index("grp"), lax.axis_index("sp"), lax.axis_index("tp")
    length, width = tok.shape
    rows = wk_h.shape[0]
    head_width = hgain.shape[1]
    cols = wk.shape[1]
    heads = cols // head_width
    channels = wab.shape[1] // 2
    columns = out.shape[1]
    units = [(j, h) for j in range(2) for h in range(heads)]
    n_units = len(units)
    pairs = [(u, r) for u in range(n_units) for r in range(2)]
    chip, core = tp // 2, lax.rem(tp, 2)
    chips = n_tp // 2
    sibling = tp + 1 - 2 * core
    other = 1 - grp
    edge = (sp == 0) | (sp == n_sp - 1)
    inner = (sp > 0) & (sp < n_sp - 1)
    helps = (sp == 1) | (sp == n_sp - 2)
    helper = jnp.where(sp == 0, 1, n_sp - 2)
    helped = jnp.where(sp == 1, 0, n_sp - 1)
    sources = (wk_h, wg_h, wv_h, wq_h, wa_h, wb_h)
    plain = {KEY: wk, VALUE: wv, QUERY: wq}

    def remote(src, dst, send, recv, **where):
        return pltpu.make_async_remote_copy(
            src_ref=src, dst_ref=dst, send_sem=send, recv_sem=recv, device_id=where, device_id_type=MESH
        )

    def source(w):
        if w == GATE:
            return wg_h
        size = channels if w in (GLU, OPEN) else cols
        return sources[w].at[:, pl.ds(pl.multiple_of(grp * size, 128), size)]

    def target(w, index):
        if w == GATE:
            return wg.at[index]
        at = pl.ds(pl.multiple_of(index * rows, 16), rows)
        if w in (GLU, OPEN):
            return wab.at[at, pl.ds(channels if w == OPEN else 0, channels)]
        return plain[w].at[at]

    load_tok = pltpu.make_async_copy(tok_h, tok, local_sem.at[0])
    load_tok.start()
    own = [pltpu.make_async_copy(source(w), target(w, sp), local_sem.at[1 + w]) for w in range(6)]
    for w in (KEY, GATE, VALUE, QUERY):
        own[w].start()

    @pl.when(inner)
    def _():
        own[GLU].start()
        own[OPEN].start()

    def od_rows(index):
        return pl.ds(pl.multiple_of(index * columns, 16), columns)

    load_od = pltpu.make_async_copy(od_h.at[od_rows(tp)], odg.at[tp], local_sem.at[7])
    load_oc = pltpu.make_async_copy(oc_h.at[od_rows(tp)], ocg.at[tp], local_sem.at[8])
    load_od.start()
    load_oc.start()

    barrier = pltpu.get_barrier_semaphore()

    def greet(**where):
        pl.semaphore_signal(barrier, inc=1, device_id=where, device_id_type=MESH)

    for step in range(n_tp - 1):
        peer = lax.rem(tp + step + 1, n_tp)
        greet(tp=peer)
        greet(tp=peer, grp=other)
    greet(grp=other)

    @pl.when(sp > 0)
    def _():
        greet(sp=sp - 1)
        greet(sp=sp - 1, grp=other)

    @pl.when(sp < n_sp - 1)
    def _():
        greet(sp=sp + 1)
        greet(sp=sp + 1, grp=other)

    load_tok.wait()
    chunk = 64
    for at in range(0, length, chunk):
        here = tok[at:at + chunk, :].astype(F32)
        scale = lax.rsqrt(jnp.mean(here * here, axis=-1, keepdims=True) + EPSILON)
        nt[at:at + chunk, :] = (here * scale * gain[...]).astype(BF16)

    @pl.when(edge)
    def _():
        pl.semaphore_wait(barrier, 2 * n_tp + 1)

    @pl.when(inner)
    def _():
        pl.semaphore_wait(barrier, 2 * n_tp + 3)

    def wide(w):
        return 1 if w in (GLU, OPEN) else 0

    def arrives(w, side, d):
        ok = (sp - d >= 0) if side == 0 else (sp + d < n_sp)
        return ok & inner if wide(w) else ok

    def leaves(w, side, d):
        if side == 0:
            return (sp - (d - 1) >= 0) & (sp < n_sp - 1 - wide(w))
        return (sp + (d - 1) < n_sp) & (sp > wide(w))

    def z_copy(w, side, d):
        back = d - 1
        place = target(w, sp - back if side == 0 else sp + back)
        return remote(
            source(w) if d == 1 else place, place, z_send.at[w, side, d - 1], z_recv.at[w, side, d - 1],
            sp=sp + 1 if side == 0 else sp - 1,
        )

    def z_arrival(w, side, d):
        place = target(w, sp - d if side == 0 else sp + d)
        return remote(
            place, place, z_send.at[w, side, d - 1], z_recv.at[w, side, d - 1],
            sp=sp + 1 if side == 0 else sp - 1,
        )

    def offer(w, where):
        for side in range(2):
            @pl.when(leaves(w, side, 1) & where)
            def _(side=side):
                z_copy(w, side, 1).start()

    def relay(w, d):
        if d > n_sp - 1:
            return
        for side in range(2):
            @pl.when(arrives(w, side, d))
            def _(side=side):
                z_arrival(w, side, d).wait_recv()
                if d < n_sp - 1:
                    @pl.when(leaves(w, side, d + 1))
                    def _():
                        z_copy(w, side, d + 1).start()

    pieces = ty_send.shape[1]
    half = length // 2
    piece = half // pieces

    def part(block, side, c):
        return nt.at[pl.ds(pl.multiple_of(block * length + side * half + c * piece, 16), piece)]

    def tok_y(k, c):
        return remote(part(2 * k, core, c), part(2 * k + 1, core, c), ty_send.at[k, c], ty_recv.at[k, c], grp=other)

    def tok_z(c):
        return remote(part(0, core, c), part(2, core, c), tz_send.at[c], tz_recv.at[c], sp=helper)

    def tok_f(block, c):
        return remote(
            part(block, core, c), part(block, core, c), tf_send.at[block - 1, c], tf_recv.at[block - 1, c], tp=sibling
        )

    def tok_f_arrival(block, c):
        place = part(block, 1 - core, c)
        return remote(place, place, tf_send.at[block - 1, c], tf_recv.at[block - 1, c], tp=sibling)

    def pass_y(k, c):
        tok_y(k, c).wait_recv()
        tok_f(2 * k + 1, c).start()

    def pass_z(c):
        @pl.when(helps)
        def _():
            tok_z(c).wait_recv()
            tok_y(1, c).start()
            tok_f(2, c).start()

    def pass_far(c):
        @pl.when(helps)
        def _():
            pass_y(1, c)

    ld_copy = remote(ldt, ldo, ld_send.at[0], ld_recv.at[0], grp=other)

    def od_copy(m, step):
        dest = lax.rem(tp + step + 1, n_tp)
        src, dst = ((od_h, odg), (oc_h, ocg))[m]
        return remote(src.at[od_rows(dest)], dst.at[tp], od_send.at[m, step], od_recv.at[m, step], tp=dest)

    def od_arrival(m, step):
        origin = lax.rem(tp + n_tp - step - 1, n_tp)
        place = (odg, ocg)[m].at[origin]
        return remote(place, place, od_send.at[m, step], od_recv.at[m, step], tp=origin)

    everywhere = sp >= 0
    offer(GATE, everywhere)
    offer(KEY, everywhere)
    for c in range(pieces):
        tok_y(0, c).start()
    ld_copy.start()
    offer(VALUE, everywhere)
    offer(GLU, edge)

    @pl.when(edge)
    def _():
        for c in range(pieces):
            tok_z(c).start()

    offer(OPEN, edge)
    offer(QUERY, edge)
    for m in (1, 0):
        for step in range(n_tp - 1):
            od_copy(m, step).start()

    def dot(a, b, dims=NN):
        return lax.dot_general(a, b, dims, preferred_element_type=F32)

    def unit_rows(tensor):
        return tensor * lax.rsqrt(jnp.sum(tensor * tensor, axis=-1, keepdims=True) + EPSILON)

    def silu(tensor):
        return tensor * jax.nn.sigmoid(tensor)

    relay(GATE, 1)
    relay(KEY, 1)
    relay(GATE, 2)
    relay(KEY, 2)
    relay(VALUE, 1)
    offer(GLU, inner)
    for d in range(3, n_sp):
        relay(GATE, d)
        relay(KEY, d)
    relay(GLU, 1)
    offer(OPEN, inner)
    offer(QUERY, inner)
    for c in range(pieces):
        pass_y(0, c)
    pass_z(0)
    own[GATE].wait()
    own[KEY].wait()
    ld_copy.wait_recv()
    for c in range(pieces):
        tok_f_arrival(1, c).wait_recv()

    both = 2 * length
    gate_cols = jnp.zeros((both, wg.shape[1]), F32)
    gate_rows = jnp.zeros((wg.shape[1], both), F32)
    for index in range(n_sp):
        normed_part = nt[0:both, index * rows:(index + 1) * rows]
        gate_cols = gate_cols + dot(normed_part, wg[index], NT)
        gate_rows = gate_rows + dot(wg[index], normed_part, NT)
    mine = grp == 0
    gates = 4 * heads
    gate_cols = jnp.where(mine, gate_cols[:, :gates], gate_cols[:, gates:])
    gate_rows = jnp.where(mine, gate_rows[:gates, :], gate_rows[gates:, :])
    rates = [
        jnp.where(mine, log[:2 * heads, :], log[2 * heads:, :]) for log in (ldt[...], ldo[...])
    ]

    row_at = lax.broadcasted_iota(jnp.int32, (length, length), 0)
    col_at = lax.broadcasted_iota(jnp.int32, (length, length), 1)
    same = row_at == col_at

    key_proj = silu(dot(nt[0:both, :], wk[...]))
    pass_z(1)
    relay(VALUE, 2)
    for u, (j, h) in enumerate(units):
        keys[u] = unit_rows(key_proj[j * length:(j + 1) * length, h * head_width:(h + 1) * head_width])
    for u, (j, h) in enumerate(units):
        grams = bdot(keys[u], keys[u], NT)
        for r in range(2):
            p = 2 * u + r
            g = 4 * h + 2 * r
            span = slice(j * length, (j + 1) * length)
            decay_row = rates[j][2 * h + r:2 * h + r + 1, :] * (0.5 + jax.nn.sigmoid(gate_rows[g:g + 1, span]))
            beta = jax.nn.sigmoid(gate_cols[span, g + 1:g + 2] - BETA_SHIFT)
            seen = col_at <= row_at if r == 0 else col_at >= row_at
            cum_col = jnp.sum(jnp.where(seen, decay_row, 0.0), axis=1, keepdims=True)
            cum_row = jnp.sum(jnp.where(same, cum_col, 0.0), axis=0, keepdims=True)
            weighting = jnp.where(seen, jnp.exp(jnp.where(seen, cum_col - cum_row, 0.0)), 0.0)
            gaps[p] = weighting
            betas[p] = jnp.broadcast_to(beta, (length, head_width))
            cums[p] = jnp.broadcast_to(cum_col, (length, head_width))
            lower = jnp.where(same, 0.0, grams * weighting * beta)
            rhs[p] = lower
            near = (row_at // 2 == col_at // 2)
            xinv[p] = jnp.where(same, 1.0, jnp.where(near, -lower, 0.0))

    service = {
        2: [lambda: pass_z(2), lambda: pass_far(0)],
        8: [lambda: pass_z(3), lambda: pass_far(1)],
        32: [lambda: pass_far(2)],
        64: [lambda: relay(GLU, 2)],
        128: [lambda: pass_far(3), lambda: relay(OPEN, 1)],
    }
    size = 2
    while size < length:
        inside = (row_at // (2 * size) == col_at // (2 * size)) & (row_at // size != col_at // size)
        for p in range(len(pairs)):
            across = jnp.where(inside, rhs[p], 0.0)
            inverse = xinv[p]
            xinv[p] = inverse - bdot(inverse, bdot(across, inverse))
        for act in service.get(size, ()):
            act()
        size *= 2

    own[VALUE].wait()
    for d in range(3, n_sp):
        relay(VALUE, d)
    value_proj = silu(dot(nt[0:both, :], wv[...]))
    eye = (
        lax.broadcasted_iota(jnp.int32, (head_width, head_width), 0)
        == lax.broadcasted_iota(jnp.int32, (head_width, head_width), 1)
    )
    for u, r in pairs:
        p = 2 * u + r
        j, h = units[u]
        beta, cum, key = betas[p], cums[p], keys[u]
        value = value_proj[j * length:(j + 1) * length, h * head_width:(h + 1) * head_width]
        total = cum[length - 1:length, :] if r == 0 else cum[0:1, :]
        right = jnp.concatenate([beta * value, beta * key * jnp.exp(cum)], axis=1)
        solved = bdot(xinv[p], right)
        vals[p] = solved.astype(BF16)
        passed = bdot(key * jnp.exp(total - cum), solved, TN)
        ends[p] = passed[:, :head_width]
        maps[p] = (jnp.where(eye, jnp.exp(total), 0.0) - passed[:, head_width:]).astype(BF16)

    def place_of(r):
        return sp if r == 0 else n_sp - 1 - sp

    def chain_copy(r):
        dest = sp + 1 if r == 0 else sp - 1
        return remote(chain_out.at[r], chain_in.at[r], chain_send.at[r], chain_recv.at[r], sp=dest)

    def chain_point(low, high):
        for r in range(2):
            at = place_of(r)

            @pl.when((at >= low) & (at <= high))
            def _(r=r, at=at):
                if low == 0:
                    for u in range(n_units):
                        chain_in[r, u] = jnp.zeros((head_width, head_width), BF16)
                        chain_out[r, u] = ends[2 * u + r].astype(BF16)
                else:
                    chain_copy(r).wait_recv()
                    for u in range(n_units):
                        p = 2 * u + r
                        chain_out[r, u] = (bdot(maps[p], chain_in[r, u]) + ends[p]).astype(BF16)

                @pl.when(at < n_sp - 1)
                def _():
                    chain_copy(r).start()

    chain_point(0, 0)
    for d in range(3, n_sp):
        relay(GLU, d)
    relay(QUERY, 1)
    relay(OPEN, 2)
    for d in range(3, n_sp):
        relay(OPEN, d)

    def gated(first, count):
        x = dot(nt[first * length:(first + count) * length, :], wab[...])
        return (x[:, :channels] * jax.nn.sigmoid(x[:, channels:])).astype(BF16)

    def owner(j):
        return grp if j == 0 else other

    def main_y():
        return remote(gout, main_in.at[grp], main_send.at[0], main_recv.at[grp], grp=other)

    def main_arrival(h):
        return remote(main_in.at[h], main_in.at[h], main_send.at[0], main_recv.at[h], grp=other)

    def far_copy(j):
        return remote(gend.at[j], main_in.at[grp], far_send.at[j], main_recv.at[grp], sp=helped, grp=owner(j))

    def edge_copy(side, j):
        start = length - HALO if side == 0 else 0
        src = main_in.at[grp, pl.ds(start, HALO)] if j == 0 else gout.at[pl.ds(start, HALO)]
        return remote(
            src, edge_in.at[side, grp], edge_send.at[side, j], edge_recv.at[side, grp],
            sp=sp + 1 if side == 0 else sp - 1, grp=owner(j),
        )

    def rim_copy(side):
        start = length - HALO if side == 0 else 0
        return remote(
            gend.at[1, pl.ds(start, HALO)], edge_in.at[side, grp], rim_send.at[side], edge_recv.at[side, grp], grp=other
        )

    def edge_arrival(side, h):
        place = edge_in.at[side, h]
        return remote(place, place, edge_send.at[side, 0], edge_recv.at[side, h], grp=other)

    @pl.when(inner)
    def _():
        own[GLU].wait()
        own[OPEN].wait()

        @pl.when(helps)
        def _():
            for c in range(pieces):
                tok_f_arrival(2, c).wait_recv()
                tok_f_arrival(3, c).wait_recv()
            far = gated(2, 2)
            gend[0] = far[:length]
            gend[1] = far[length:]
            for j in range(2):
                far_copy(j).start()
            for side, at in ((0, 1), (1, n_sp - 2)):
                @pl.when(sp == at)
                def _(side=side):
                    rim_copy(side).start()
                    start = length - HALO if side == 0 else 0
                    edge_in[side, grp] = gend[0, start:start + HALO, :]

        near = gated(0, 2)
        main_in[grp] = near[:length]
        gout[...] = near[length:]
        main_y().start()
        for side in range(2):
            for j in range(2):
                edge_copy(side, j).start()

    chain_point(1, 1)
    relay(QUERY, 2)
    for at in range(2, n_sp - 1):
        chain_point(at, at)
        relay(QUERY, at + 1)
    chain_point(n_sp - 1, n_sp - 1)

    for h in range(2):
        @pl.when(~(inner & (grp == h)))
        def _(h=h):
            main_arrival(h).wait_recv()

        @pl.when((sp > 0) & ~((sp == 1) & (grp == h)))
        def _(h=h):
            edge_arrival(0, h).wait_recv()

        @pl.when((sp < n_sp - 1) & ~((sp == n_sp - 2) & (grp == h)))
        def _(h=h):
            edge_arrival(1, h).wait_recv()

        pad[h, HALO:HALO + length, :] = main_in[h].astype(F32)
        for side, start, none in ((0, 0, 0), (1, HALO + length, n_sp - 1)):
            @pl.when(sp != none)
            def _(h=h, side=side, start=start):
                pad[h, start:start + HALO, :] = edge_in[side, h].astype(F32)

            @pl.when(sp == none)
            def _(h=h, start=start):
                pad[h, start:start + HALO, :] = jnp.zeros((HALO, channels), F32)

    taps = ck.shape[0]
    for h in range(2):
        lanes = slice(h * channels, (h + 1) * channels)
        for at in range(0, length, chunk):
            first = at + HALO - taps // 2
            total = pad[h, first:first + chunk, :] * ck[0:1, lanes]
            for k in range(1, taps):
                total = total + pad[h, first + k:first + k + chunk, :] * ck[k:k + 1, lanes]
            conv[at:at + chunk, lanes] = total
    filtered = conv[...]
    sum_col = jnp.sum(filtered, axis=-1, keepdims=True)
    square_col = jnp.sum(filtered * filtered, axis=-1, keepdims=True)
    stat_out[...] = jnp.zeros(stat_out.shape, F32)
    stat_out[0:1, :] = jnp.sum(jnp.where(same, sum_col, 0.0), axis=0, keepdims=True)
    stat_out[1:2, :] = jnp.sum(jnp.where(same, square_col, 0.0), axis=0, keepdims=True)

    def stat_copy(step):
        return remote(
            stat_out, stat_in.at[step], stat_send.at[step], stat_recv.at[step], tp=lax.rem(tp + step + 1, n_tp)
        )

    for step in range(n_tp - 1):
        stat_copy(step).start()

    own[QUERY].wait()
    query_proj = silu(dot(nt[0:both, :], wq[...]))
    for u, (j, h) in enumerate(units):
        query = query_proj[j * length:(j + 1) * length, h * head_width:(h + 1) * head_width]
        query = unit_rows(query) * head_width ** -0.5
        scores = bdot(query, keys[u], NT)
        for r in range(2):
            p = 2 * u + r
            pair = dot((scores * gaps[p]).astype(BF16), vals[p])
            reads[p] = (query * jnp.exp(cums[p]) - pair[:, head_width:]).astype(BF16)
            if r == 0:
                local_out[u] = pair[:, :head_width]
            else:
                local_out[u] = local_out[u] + pair[:, :head_width]

    def mixed_head(u):
        joined = local_out[u] + dot(reads[2 * u], chain_in[0, u]) + dot(reads[2 * u + 1], chain_in[1, u])
        scale = lax.rsqrt(jnp.mean(joined * joined, axis=-1, keepdims=True) + EPSILON)
        return (joined * scale * hgain[...]).astype(BF16)

    def chip_at(q):
        return lax.rem(chip + q, chips)

    def chip_back(q):
        return lax.rem(chip + chips - q, chips)

    def dg_copy(a, q):
        src = dall.at[tp, grp] if a == 0 else dm_out
        where = {"tp": chip_at(q) * 2 + core}
        if a:
            where["grp"] = other
        return remote(src, dall.at[tp, grp], dg_send.at[a, q], dg_recv.at[a, q], **where)

    def d_block(a, q, side):
        return dall.at[chip_back(q) * 2 + side, other if a else grp]

    def dg_arrival(a, q):
        place = d_block(a, q, core)
        return remote(place, place, dg_send.at[a, q], dg_recv.at[a, q], tp=sibling)

    def df_copy(a, q, arriving=False):
        place = d_block(a, q, 1 - core if arriving else core)
        return remote(place, place, df_send.at[a, q], df_recv.at[a, q], tp=sibling)

    def cg_copy(q):
        return remote(call.at[tp], call.at[tp], cg_send.at[q], cg_recv.at[q], tp=chip_at(q) * 2 + core)

    def cg_arrival(q):
        place = call.at[chip_back(q) * 2 + core]
        return remote(place, place, cg_send.at[q], cg_recv.at[q], tp=sibling)

    def cf_copy(q, arriving=False):
        place = call.at[chip_back(q) * 2 + (1 - core if arriving else core)]
        return remote(place, place, cf_send.at[q], cf_recv.at[q], tp=sibling)

    direct = [(a, q) for q in range(chips) for a in (1, 0) if (a, q) != (0, 0)]

    for h in range(heads):
        dm_out[:, h * head_width:(h + 1) * head_width] = mixed_head(heads + h)
    for q in range(chips - 1, -1, -1):
        dg_copy(1, q).start()
    for h in range(heads):
        dall[tp, grp, :, h * head_width:(h + 1) * head_width] = mixed_head(h)
    for q in range(1, chips):
        dg_copy(0, q).start()
    df_copy(0, 0).start()

    stats = stat_out[0:2, :]
    for step in range(n_tp - 1):
        stat_copy(step).wait_recv()
        stats = stats + stat_in[step, 0:2, :]
    center = jnp.sum(jnp.where(same, stats[0:1, :], 0.0), axis=1, keepdims=True) / conv_total
    squares = jnp.sum(jnp.where(same, stats[1:2, :], 0.0), axis=1, keepdims=True) / conv_total
    spread = squares - center * center
    normal = (conv[...] - center) * lax.rsqrt(spread + EPSILON)
    call[tp] = silu(normal * ng[...] + ns[...]).astype(BF16)
    for q in range(1, chips):
        cg_copy(q).start()
    cf_copy(0).start()

    for m in range(2):
        for step in range(n_tp - 1):
            od_arrival(m, step).wait_recv()
    load_od.wait()
    load_oc.wait()

    for a, q in direct:
        dg_arrival(a, q).wait_recv()
        df_copy(a, q).start()
    for q in range(1, chips):
        cg_arrival(q).wait_recv()
        cf_copy(q).start()

    def delta_term(t):
        return dot(jnp.concatenate([dall[t, 0], dall[t, 1]], axis=1), odg[t], NT)

    def conv_term(t):
        return dot(call[t], ocg[t], NT)

    result = delta_term(tp)
    for q in range(chips):
        t = chip_back(q) * 2 + core
        if q:
            result = result + delta_term(t)
        result = result + conv_term(t)
    for q in range(chips):
        t = chip_back(q) * 2 + 1 - core
        df_copy(0, q, True).wait_recv()
        df_copy(1, q, True).wait_recv()
        result = result + delta_term(t)
    for q in range(chips):
        t = chip_back(q) * 2 + 1 - core
        cf_copy(q, True).wait_recv()
        result = result + conv_term(t)
    out[...] = result.astype(BF16)

    for w in range(6):
        for d in range(1, n_sp):
            for side in range(2):
                @pl.when(leaves(w, side, d))
                def _(w=w, d=d, side=side):
                    z_copy(w, side, d).wait_send()
    for c in range(pieces):
        tok_y(0, c).wait_send()
        tok_f(1, c).wait_send()

        @pl.when(edge)
        def _(c=c):
            tok_z(c).wait_send()

        @pl.when(helps)
        def _(c=c):
            tok_y(1, c).wait_send()
            tok_f(2, c).wait_send()
            tok_f(3, c).wait_send()
    ld_copy.wait_send()
    for m in range(2):
        for step in range(n_tp - 1):
            od_copy(m, step).wait_send()
    for r in range(2):
        @pl.when(place_of(r) < n_sp - 1)
        def _(r=r):
            chain_copy(r).wait_send()

    @pl.when(inner)
    def _():
        main_y().wait_send()
        for side in range(2):
            for j in range(2):
                edge_copy(side, j).wait_send()

    @pl.when(helps)
    def _():
        for j in range(2):
            far_copy(j).wait_send()
    for side, at in ((0, 1), (1, n_sp - 2)):
        @pl.when(sp == at)
        def _(side=side):
            rim_copy(side).wait_send()
    for step in range(n_tp - 1):
        stat_copy(step).wait_send()
    df_copy(0, 0).wait_send()
    for a, q in direct:
        dg_copy(a, q).wait_send()
        df_copy(a, q).wait_send()
    for q in range(chips):
        if q:
            cg_copy(q).wait_send()
        cf_copy(q).wait_send()


def solution(mesh):
    n_grp, n_sp, n_tp = mesh.shape["grp"], mesh.shape["sp"], mesh.shape["tp"]

    def on_device(tokens_in, input_gain, w_query, w_key, w_value, w_gates, w_glu_value,
                  sigmoid_opener_matrix, log_decay, head_gain, conv_kernel, norm_gain, norm_shift,
                  out_delta, out_conv):
        length, width = tokens_in.shape
        head_width = head_gain.shape[0]
        head_cols = w_query.shape[1]
        heads = head_cols // head_width
        channels = w_glu_value.shape[1]
        rows = w_query.shape[0]
        pairs = 2 * heads
        columns = width // n_tp
        dma, vmem = pltpu.SemaphoreType.DMA, pltpu.VMEM
        anywhere = pl.BlockSpec(memory_space=pltpu.HBM)
        inside = pl.BlockSpec(memory_space=pltpu.VMEM)
        if n_grp == 2 and n_sp >= 4 and n_tp % 2 == 0 and heads % 2 == 0 and channels % 256 == 0:
            cols, ch, chips, steps = head_cols // 2, channels // 2, n_tp // 2, n_tp - 1
            pieces = 4
            scratch = [
                vmem((length, width), BF16), vmem((4 * length, width), BF16),
                vmem((width, cols), BF16), vmem((width, cols), BF16), vmem((width, cols), BF16),
                vmem((width, 2 * ch), BF16), vmem((n_sp, 4 * heads, rows), BF16),
                vmem((n_tp, columns, head_cols), BF16), vmem((n_tp, columns, channels), BF16),
                vmem((pairs, length), F32),
                vmem((heads, length, head_width), F32), vmem((pairs, length, 2 * head_width), BF16),
                vmem((pairs, length, head_width), F32), vmem((pairs, length, head_width), F32),
                vmem((pairs, length, length), F32), vmem((pairs, length, length), F32),
                vmem((pairs, length, length), F32),
                vmem((heads, length, head_width), F32), vmem((pairs, length, head_width), BF16),
                vmem((pairs, head_width, head_width), BF16), vmem((pairs, head_width, head_width), F32),
                vmem((2, heads, head_width, head_width), BF16), vmem((2, heads, head_width, head_width), BF16),
                vmem((length, ch), BF16), vmem((2, length, ch), BF16), vmem((2, length, ch), BF16),
                vmem((2, 2, HALO, ch), BF16),
                vmem((2, length + 2 * HALO, ch), F32), vmem((length, channels), F32),
                vmem((8, length), F32), vmem((steps, 8, length), F32),
                vmem((n_tp, 2, length, cols), BF16), vmem((length, cols), BF16),
                vmem((n_tp, length, channels), BF16),
                dma((9,)),
                dma((6, 2, n_sp - 1)), dma((6, 2, n_sp - 1)),
                dma((2, pieces)), dma((2, pieces)), dma((3, pieces)), dma((3, pieces)),
                dma((pieces,)), dma((pieces,)),
                dma((1,)), dma((1,)), dma((2, steps)), dma((2, steps)), dma((2,)), dma((2,)),
                dma((1,)), dma((2,)), dma((2, 2)), dma((2, 2)), dma((2,)), dma((2,)),
                dma((steps,)), dma((steps,)),
                dma((2, chips)), dma((2, chips)), dma((2, chips)), dma((2, chips)),
                dma((chips,)), dma((chips,)), dma((chips,)), dma((chips,)),
            ]
            return pl.pallas_call(
                functools.partial(fused, (n_sp, n_tp, float(channels * n_tp))),
                out_shape=jax.ShapeDtypeStruct((length, columns), BF16),
                in_specs=[anywhere, inside] + [anywhere] * 6 + [inside] * 5 + [anywhere] * 2,
                out_specs=inside,
                scratch_shapes=scratch,
                compiler_params=pltpu.CompilerParams(
                    collective_id=0, has_side_effects=True, vmem_limit_bytes=48 * 1024 * 1024
                ),
            )(
                tokens_in, input_gain.reshape(1, width), w_key, w_gates.T, w_value, w_query,
                w_glu_value, sigmoid_opener_matrix, log_decay.T,
                head_gain.reshape(1, head_width), conv_kernel, norm_gain.reshape(1, channels),
                norm_shift.reshape(1, channels), out_delta, out_conv,
            )
        scratch = [
            vmem((length, width), BF16), vmem((length, width), BF16),
            vmem((width, head_cols), BF16), vmem((n_sp, 4 * heads, rows), BF16),
            vmem((width, head_cols), BF16), vmem((width, head_cols), BF16),
            vmem((width, channels), BF16), vmem((width, channels), BF16),
            vmem((width, head_cols), BF16), vmem((width, channels), BF16),
            vmem((heads, length, head_width), F32), vmem((pairs, length, 2 * head_width), BF16),
            vmem((pairs, length, head_width), F32), vmem((pairs, length, head_width), F32),
            vmem((pairs, length, length), F32), vmem((pairs, length, length), F32),
            vmem((pairs, length, length), F32),
            vmem((heads, length, head_width), F32), vmem((pairs, length, head_width), BF16),
            vmem((pairs, head_width, head_width), BF16), vmem((pairs, head_width, head_width), F32),
            vmem((2, heads, head_width, head_width), BF16), vmem((2, heads, head_width, head_width), BF16),
            vmem((length, channels), BF16), vmem((2, HALO, channels), BF16),
            vmem((length + 2 * HALO, channels), F32), vmem((length, channels), F32),
            vmem((8, length), F32), vmem((n_tp - 1, 8, length), F32),
            vmem((n_tp, length, columns), F32),
            vmem((n_tp // 2, length, columns), BF16), vmem((n_tp // 2, length, columns), BF16),
            vmem((n_tp // 2, length, columns), BF16), vmem((n_tp // 2, length, columns), BF16),
            dma((9,)),
            dma((6, 2, n_sp - 1)), dma((6, 2, n_sp - 1)),
            dma((6, 2, n_sp - 1)), dma((6, 2, n_sp - 1)),
            dma((2,)), dma((2,)), dma((2,)), dma((2,)),
            dma((n_tp - 1,)), dma((n_tp - 1,)), dma((n_tp // 2,)), dma((n_tp // 2,)),
            dma((n_tp // 2,)), dma((n_tp // 2,)),
        ]
        return pl.pallas_call(
            functools.partial(kernel, (n_grp, n_sp, n_tp, float(channels * n_tp))),
            out_shape=jax.ShapeDtypeStruct((length, columns), BF16),
            in_specs=[anywhere, inside] + [anywhere] * 6 + [inside] * 6 + [anywhere] * 2,
            out_specs=inside,
            scratch_shapes=scratch,
            compiler_params=pltpu.CompilerParams(
                collective_id=0, has_side_effects=True, vmem_limit_bytes=60 * 1024 * 1024
            ),
        )(
            tokens_in, input_gain.reshape(1, width), w_key, w_gates.T, w_value, w_query,
            w_glu_value, sigmoid_opener_matrix, log_decay, log_decay.T,
            head_gain.reshape(1, head_width), conv_kernel, norm_gain.reshape(1, channels),
            norm_shift.reshape(1, channels), out_delta, out_conv,
        )

    placed = (
        P(("grp", "sp"), None), P(), P("sp", "tp"), P("sp", "tp"), P("sp", "tp"), P("sp", "tp"),
        P("sp", "tp"), P("sp", "tp"), P(("grp", "sp"), "tp"), P(), P(None, "tp"), P("tp"), P("tp"),
        P(None, "tp"), P(None, "tp"),
    )
    return jax.shard_map(
        on_device, mesh=mesh, in_specs=placed, out_specs=P(("grp", "sp"), "tp"), check_vma=False
    )
```

```python
import functools

import jax
import jax.numpy as jnp
from jax import lax
from jax.experimental import pallas as pl
from jax.experimental.pallas import tpu as pltpu
from jax.sharding import PartitionSpec as P

EPSILON = 1e-06
BETA_SHIFT = 6.0
HALO = 16
MESH = pl.DeviceIdType.MESH
F32 = jnp.float32
BF16 = jnp.bfloat16
NT = (((1,), (1,)), ((), ()))
TN = (((0,), (0,)), ((), ()))
NN = (((1,), (0,)), ((), ()))
KEY, GATE, VALUE, QUERY, GLU, OPEN = range(6)


def bdot(left, right, dims=NN):
    return lax.dot_general(
        left.astype(BF16), right.astype(BF16), dims, preferred_element_type=F32
    )


def each(count, action):
    if count <= 8:
        for step in range(count):
            action(step)
    else:
        def body(step, carry):
            action(step)
            return carry

        lax.fori_loop(0, count, body, 0)


def kernel(cfg, tok_h, gain, wk_h, wg_h, wv_h, wq_h, wa_h, wb_h, ld, ldt, hgain, ck, ng, ns, od_h, oc_h,
           out,
           tok, normed, wk, wg, wv, wq, wa, wb, od, oc,
           keys, vals, betas, cums, xinv, gaps, rhs, local_out, reads, maps, ends,
           chain_in, chain_out, glu, halo, pad, conv, stat_out, stat_in, conv_acc, part_out, part_in, pair_out, pair_in,
           local_sem, z_send, z_recv, y_send, y_recv, chain_send, chain_recv,
           halo_send, halo_recv, stat_send, stat_recv, part_send, part_recv, pair_send, pair_recv):
    n_grp, n_sp, n_tp, conv_total = cfg
    grp, sp, tp = lax.axis_index("grp"), lax.axis_index("sp"), lax.axis_index("tp")
    length, width = tok.shape
    rows = wk_h.shape[0]
    channels = wa.shape[1]
    head_width = hgain.shape[1]
    heads = wk.shape[1] // head_width
    share = (rows // 2) // 16 * 16 if n_grp == 2 else 0
    pulled = rows - share

    sources = (wk_h, wg_h, wv_h, wq_h, wa_h, wb_h)
    targets = (wk, wg, wv, wq, wa, wb)

    def block_of(w, index, start, count):
        if w == GATE:
            return targets[w].at[index]
        return targets[w].at[pl.ds(pl.multiple_of(index * rows + start, 16), count)]

    load_tok = pltpu.make_async_copy(tok_h, tok, local_sem.at[0])
    load_tok.start()
    own = [
        pltpu.make_async_copy(sources[w], block_of(w, sp, 0, rows), local_sem.at[1 + w])
        for w in range(6)
    ]
    for copy in own:
        copy.start()
    load_od = pltpu.make_async_copy(od_h, od, local_sem.at[7])
    load_oc = pltpu.make_async_copy(oc_h, oc, local_sem.at[8])

    barrier = pltpu.get_barrier_semaphore()

    def greet(axis, me, count):
        def one(step):
            pl.semaphore_signal(
                barrier, inc=1, device_id={axis: lax.rem(me + step + 1, count)}, device_id_type=MESH
            )

        each(count - 1, one)

    greet("sp", sp, n_sp)
    greet("tp", tp, n_tp)
    greet("grp", grp, n_grp)
    pl.semaphore_wait(barrier, n_sp + n_tp + n_grp - 3)

    def origin(side, d):
        return sp - d if side == 0 else sp + d

    def arrives(side, d):
        return sp - d >= 0 if side == 0 else sp + d < n_sp

    def leaves(side, d):
        if side == 0:
            return (sp - (d - 1) >= 0) & (sp < n_sp - 1)
        return (sp + (d - 1) < n_sp) & (sp > 0)

    def part_of(w, index, side_of):
        if w == GATE:
            return block_of(w, index, 0, 0)
        if not share:
            return block_of(w, index, 0, rows)
        if side_of is None:
            return block_of(w, index, pl.multiple_of(grp * share, 16), pulled)
        return block_of(w, index, pl.multiple_of(side_of * pulled, 16), share)

    def z_copy(w, side, d, first=False):
        target = part_of(w, origin(side, d - 1), None)
        source = target
        if first:
            source = sources[w]
            if w != GATE and share:
                source = source.at[pl.ds(pl.multiple_of(grp * share, 16), pulled)]
        return pltpu.make_async_remote_copy(
            src_ref=source, dst_ref=target,
            send_sem=z_send.at[w, side, d - 1], recv_sem=z_recv.at[w, side, d - 1],
            device_id={"sp": sp + 1 if side == 0 else sp - 1}, device_id_type=MESH,
        )

    def z_arrival(w, side, d):
        place = part_of(w, origin(side, d), None)
        return pltpu.make_async_remote_copy(
            src_ref=place, dst_ref=place,
            send_sem=z_send.at[w, side, d - 1], recv_sem=z_recv.at[w, side, d - 1],
            device_id={"sp": sp + 1 if side == 0 else sp - 1}, device_id_type=MESH,
        )

    def y_copy(w, side, d, arriving=False):
        place = part_of(w, origin(side, d), 1 - grp if arriving else grp)
        return pltpu.make_async_remote_copy(
            src_ref=place, dst_ref=place,
            send_sem=y_send.at[w, side, d - 1], recv_sem=y_recv.at[w, side, d - 1],
            device_id={"grp": 1 - grp}, device_id_type=MESH,
        )

    def offer(w):
        for side in range(2):
            @pl.when(leaves(side, 1))
            def _(side=side):
                z_copy(w, side, 1, True).start()

    def relay_hop(w, d):
        for side in range(2):
            @pl.when(arrives(side, d))
            def _(side=side):
                z_arrival(w, side, d).wait_recv()

                @pl.when(leaves(side, d + 1))
                def _():
                    z_copy(w, side, d + 1).start()

                if share and w != GATE:
                    y_copy(w, side, d).start()

    def relay(w, low=1, high=None):
        if high is None:
            each(n_sp - low, lambda step: relay_hop(w, step + low))
        else:
            for d in range(low, min(high, n_sp - 1) + 1):
                relay_hop(w, d)

    def complete(w):
        own[w].wait()
        if share and w != GATE:
            def one(step):
                for side in range(2):
                    @pl.when(arrives(side, step + 1))
                    def _(side=side):
                        y_copy(w, side, step + 1, True).wait_recv()

            each(n_sp - 1, one)

    offer(KEY)
    offer(GATE)
    offer(VALUE)
    load_od.start()
    load_oc.start()

    load_tok.wait()
    chunk = 64
    for at in range(0, length, chunk):
        here = tok[at:at + chunk, :].astype(F32)
        scale = lax.rsqrt(jnp.mean(here * here, axis=-1, keepdims=True) + EPSILON)
        normed[at:at + chunk, :] = (here * scale * gain[...]).astype(BF16)

    def project(w):
        return jnp.dot(normed[...], targets[w][...], preferred_element_type=F32)

    def unit_rows(tensor):
        return tensor * lax.rsqrt(jnp.sum(tensor * tensor, axis=-1, keepdims=True) + EPSILON)

    def silu(tensor):
        return tensor * jax.nn.sigmoid(tensor)

    relay(GATE)
    relay(KEY)
    offer(QUERY)
    complete(GATE)
    gate_cols = jnp.zeros((length, 4 * heads), F32)
    gate_rows = jnp.zeros((4 * heads, length), F32)
    for index in range(n_sp):
        normed_part = normed[:, index * rows:(index + 1) * rows]
        gate_cols = gate_cols + lax.dot_general(normed_part, wg[index], NT, preferred_element_type=F32)
        gate_rows = gate_rows + lax.dot_general(wg[index], normed_part, NT, preferred_element_type=F32)

    row_at = lax.broadcasted_iota(jnp.int32, (length, length), 0)
    col_at = lax.broadcasted_iota(jnp.int32, (length, length), 1)

    complete(KEY)
    key_proj = silu(project(KEY))
    pairs = [(h, r) for h in range(heads) for r in range(2)]
    for h in range(heads):
        keys[h] = unit_rows(key_proj[:, h * head_width:(h + 1) * head_width])
    relay(VALUE, 1, 1)
    for h in range(heads):
        grams = bdot(keys[h], keys[h], NT)
        for r in range(2):
            p = 2 * h + r
            decay_col = ld[:, p:p + 1] * (0.5 + jax.nn.sigmoid(gate_cols[:, 2 * p:2 * p + 1]))
            decay_row = ldt[p:p + 1, :] * (0.5 + jax.nn.sigmoid(gate_rows[2 * p:2 * p + 1, :]))
            beta = jax.nn.sigmoid(gate_cols[:, 2 * p + 1:2 * p + 2] - BETA_SHIFT)
            if r == 0:
                seen_down, seen_across = row_at <= col_at, col_at <= row_at
            else:
                seen_down, seen_across = row_at >= col_at, col_at >= row_at
            cum_row = jnp.sum(jnp.where(seen_down, decay_col, 0.0), axis=0, keepdims=True)
            cum_col = jnp.sum(jnp.where(seen_across, decay_row, 0.0), axis=1, keepdims=True)
            weighting = jnp.where(
                seen_across, jnp.exp(jnp.where(seen_across, cum_col - cum_row, 0.0)), 0.0
            )
            gaps[p] = weighting
            betas[p] = jnp.broadcast_to(beta, (length, head_width))
            cums[p] = jnp.broadcast_to(cum_col, (length, head_width))
            lower = jnp.where(row_at != col_at, grams * weighting * beta, 0.0)
            rhs[p] = lower
            near = (row_at // 2 == col_at // 2)
            xinv[p] = jnp.where(row_at == col_at, 1.0, jnp.where(near, -lower, 0.0))

    size = 2
    while size < length:
        inside = (row_at // (2 * size) == col_at // (2 * size)) & (row_at // size != col_at // size)
        for p in range(len(pairs)):
            across = jnp.where(inside, rhs[p], 0.0)
            inverse = xinv[p]
            xinv[p] = inverse - bdot(inverse, bdot(across, inverse))
        if size == 2:
            relay(VALUE, 2)
            offer(GLU)
        if size == 32:
            relay(QUERY, 1, 1)
        if size == 128:
            relay(QUERY, 2, 2)
        size *= 2

    complete(VALUE)
    value_proj = silu(project(VALUE))
    eye = (
        lax.broadcasted_iota(jnp.int32, (head_width, head_width), 0)
        == lax.broadcasted_iota(jnp.int32, (head_width, head_width), 1)
    )
    for h, r in pairs:
        p = 2 * h + r
        beta, cum, key = betas[p], cums[p], keys[h]
        value = value_proj[:, h * head_width:(h + 1) * head_width]
        total = cum[length - 1:length, :] if r == 0 else cum[0:1, :]
        right = jnp.concatenate([beta * value, beta * key * jnp.exp(cum)], axis=1)
        solved = bdot(xinv[p], right)
        vals[p] = solved.astype(BF16)
        passed = bdot(key * jnp.exp(total - cum), solved, TN)
        ends[p] = passed[:, :head_width]
        maps[p] = (jnp.where(eye, jnp.exp(total), 0.0) - passed[:, head_width:]).astype(BF16)

    def place_of(r):
        return sp if r == 0 else n_sp - 1 - sp

    def chain_copy(r):
        dest = lax.rem(sp + 1, n_sp) if r == 0 else lax.rem(sp + n_sp - 1, n_sp)
        return pltpu.make_async_remote_copy(
            src_ref=chain_out.at[r], dst_ref=chain_in.at[r],
            send_sem=chain_send.at[r], recv_sem=chain_recv.at[r],
            device_id={"sp": dest}, device_id_type=MESH,
        )

    def chain_point(low, high):
        for r in range(2):
            at = place_of(r)

            @pl.when((at >= low) & (at <= high))
            def _(r=r, at=at):
                if low == 0:
                    for h in range(heads):
                        chain_in[r, h] = jnp.zeros((head_width, head_width), BF16)
                        chain_out[r, h] = ends[2 * h + r].astype(BF16)
                else:
                    chain_copy(r).wait_recv()
                    for h in range(heads):
                        p = 2 * h + r
                        chain_out[r, h] = (bdot(maps[p], chain_in[r, h]) + ends[p]).astype(BF16)

                @pl.when(at < n_sp - 1)
                def _():
                    chain_copy(r).start()

    chain_point(0, 0)
    relay(QUERY, 3)
    offer(OPEN)
    relay(GLU, 1, 1)
    complete(QUERY)
    query_proj = silu(project(QUERY))
    for h in range(heads):
        query = unit_rows(query_proj[:, h * head_width:(h + 1) * head_width]) * head_width ** -0.5
        scores = bdot(query, keys[h], NT)
        for r in range(2):
            p = 2 * h + r
            both = jnp.dot((scores * gaps[p]).astype(BF16), vals[p], preferred_element_type=F32)
            reads[p] = (query * jnp.exp(cums[p]) - both[:, head_width:]).astype(BF16)
            if r == 0:
                local_out[h] = both[:, :head_width]
            else:
                local_out[h] = local_out[h] + both[:, :head_width]
    chain_point(1, 1)
    relay(GLU, 2, 2)
    chain_point(2, 2)
    relay(GLU, 3)
    relay(OPEN, 1, 1)
    chain_point(3, n_sp - 1)
    complete(GLU)
    glu_proj = project(GLU)
    relay(OPEN, 2)
    complete(OPEN)
    gated = (glu_proj * jax.nn.sigmoid(project(OPEN))).astype(BF16)
    glu[...] = gated
    pad[HALO:HALO + length, :] = gated.astype(F32)

    def halo_copy(r):
        start = length - HALO if r == 0 else 0
        dest = lax.rem(sp + 1, n_sp) if r == 0 else lax.rem(sp + n_sp - 1, n_sp)
        return pltpu.make_async_remote_copy(
            src_ref=glu.at[pl.ds(start, HALO)], dst_ref=halo.at[r],
            send_sem=halo_send.at[r], recv_sem=halo_recv.at[r],
            device_id={"sp": dest}, device_id_type=MESH,
        )

    for r in range(2):
        @pl.when(place_of(r) < n_sp - 1)
        def _(r=r):
            halo_copy(r).start()
    for r in range(2):
        start = 0 if r == 0 else HALO + length

        @pl.when(place_of(r) > 0)
        def _(r=r, start=start):
            halo_copy(r).wait_recv()
            pad[start:start + HALO, :] = halo[r].astype(F32)

        @pl.when(place_of(r) == 0)
        def _(start=start):
            pad[start:start + HALO, :] = jnp.zeros((HALO, channels), F32)

    taps = ck.shape[0]
    for at in range(0, length, chunk):
        first = at + HALO - taps // 2
        total = pad[first:first + chunk, :] * ck[0:1, :]
        for j in range(1, taps):
            total = total + pad[first + j:first + j + chunk, :] * ck[j:j + 1, :]
        conv[at:at + chunk, :] = total
    filtered = conv[...]
    sum_col = jnp.sum(filtered, axis=-1, keepdims=True)
    square_col = jnp.sum(filtered * filtered, axis=-1, keepdims=True)
    same = row_at == col_at
    stat_out[...] = jnp.zeros(stat_out.shape, F32)
    stat_out[0:1, :] = jnp.sum(jnp.where(same, sum_col, 0.0), axis=0, keepdims=True)
    stat_out[1:2, :] = jnp.sum(jnp.where(same, square_col, 0.0), axis=0, keepdims=True)

    def stat_copy(step):
        return pltpu.make_async_remote_copy(
            src_ref=stat_out, dst_ref=stat_in.at[step],
            send_sem=stat_send.at[step], recv_sem=stat_recv.at[step],
            device_id={"tp": lax.rem(tp + step + 1, n_tp)}, device_id_type=MESH,
        )

    for step in range(n_tp - 1):
        stat_copy(step).start()

    joined_heads = []
    for h in range(heads):
        joined = local_out[h] + jnp.dot(reads[2 * h], chain_in[0, h], preferred_element_type=F32)
        joined = joined + jnp.dot(reads[2 * h + 1], chain_in[1, h], preferred_element_type=F32)
        scale = lax.rsqrt(jnp.mean(joined * joined, axis=-1, keepdims=True) + EPSILON)
        joined_heads.append((joined * scale * hgain[...]).astype(BF16))
    delta_mix = jnp.concatenate(joined_heads, axis=1) if heads > 1 else joined_heads[0]
    load_od.wait()
    load_oc.wait()
    columns = width // n_tp
    for dest in range(n_tp):
        at = slice(dest * columns, (dest + 1) * columns)
        conv_acc[dest] = lax.dot_general(delta_mix, od[at, :], NT, preferred_element_type=F32)

    stats = stat_out[0:2, :]
    for step in range(n_tp - 1):
        stat_copy(step).wait_recv()
        stats = stats + stat_in[step, 0:2, :]
    center = jnp.sum(jnp.where(same, stats[0:1, :], 0.0), axis=1, keepdims=True) / conv_total
    squares = jnp.sum(jnp.where(same, stats[1:2, :], 0.0), axis=1, keepdims=True) / conv_total
    spread = squares - center * center
    normal = (filtered - center) * lax.rsqrt(spread + EPSILON)
    conv_mix = silu(normal * ng[...] + ns[...]).astype(BF16)

    chip, core = tp // 2, lax.rem(tp, 2)
    chips = n_tp // 2
    sibling = chip * 2 + 1 - core

    def there(p, place):
        return lax.rem(chip + p, chips) * 2 + place

    def term_of(dest):
        at = pl.ds(pl.multiple_of(dest * columns, 16), columns)
        return conv_acc[dest] + lax.dot_general(conv_mix, oc[at, :], NT, preferred_element_type=F32)

    def pair_copy(p):
        return pltpu.make_async_remote_copy(
            src_ref=pair_out.at[p], dst_ref=pair_in.at[p],
            send_sem=pair_send.at[p], recv_sem=pair_recv.at[p],
            device_id={"tp": sibling}, device_id_type=MESH,
        )

    def part_copy(p):
        return pltpu.make_async_remote_copy(
            src_ref=part_out.at[p - 1], dst_ref=part_in.at[p - 1],
            send_sem=part_send.at[p - 1], recv_sem=part_recv.at[p - 1],
            device_id={"tp": there(p, core)}, device_id_type=MESH,
        )

    slots = list(range(1, chips)) + [0]
    for p in slots:
        pair_out[p] = term_of(there(p, 1 - core)).astype(BF16)
        pair_copy(p).start()
    for p in slots:
        term = term_of(there(p, core))
        pair_copy(p).wait_recv()
        term = term + pair_in[p].astype(F32)
        if p:
            part_out[p - 1] = term.astype(BF16)
            part_copy(p).start()
        else:
            result = term
    for p in range(1, chips):
        part_copy(p).wait_recv()
        result = result + part_in[p - 1].astype(F32)
    out[...] = result.astype(BF16)

    for w in range(6):
        def one(step, w=w):
            for side in range(2):
                @pl.when(leaves(side, step + 1))
                def _(side=side):
                    z_copy(w, side, step + 1).wait_send()

                if share and w != GATE:
                    @pl.when(arrives(side, step + 1))
                    def _(side=side):
                        y_copy(w, side, step + 1).wait_send()

        each(n_sp - 1, one)
    for r in range(2):
        @pl.when(place_of(r) < n_sp - 1)
        def _(r=r):
            chain_copy(r).wait_send()
            halo_copy(r).wait_send()
    for step in range(n_tp - 1):
        stat_copy(step).wait_send()
    for p in range(chips):
        pair_copy(p).wait_send()
        if p:
            part_copy(p).wait_send()


def fused(cfg, tok_h, gain, wk_h, wg_h, wv_h, wq_h, wa_h, wb_h, ldt, hgain, ck, ng, ns, od_h, oc_h,
          out,
          tok, nt, wk, wv, wq, wab, wg, odg, ocg, ldo,
          keys, vals, betas, cums, xinv, gaps, rhs, local_out, reads, maps, ends,
          chain_in, chain_out, gout, gend, main_in, edge_in, pad, conv, stat_out, stat_in,
          dall, dm_out, call, acc_ab, acc_q,
          local_sem, z_send, z_recv, ty_send, ty_recv, tf_send, tf_recv, tz_send, tz_recv,
          ld_send, ld_recv, od_send, od_recv, chain_send, chain_recv,
          main_send, main_recv, edge_send, edge_recv, far_send, rim_send,
          stat_send, stat_recv, dg_send, dg_recv, df_send, df_recv, cg_send, cg_recv, cf_send, cf_recv):
    n_sp, n_tp, conv_total = cfg
    grp, sp, tp = lax.axis_index("grp"), lax.axis_index("sp"), lax.axis_index("tp")
    length, width = tok.shape
    rows = wk_h.shape[0]
    head_width = hgain.shape[1]
    cols = wk.shape[1]
    heads = cols // head_width
    channels = wab.shape[1] // 2
    columns = out.shape[1]
    units = [(j, h) for j in range(2) for h in range(heads)]
    n_units = len(units)
    pairs = [(u, r) for u in range(n_units) for r in range(2)]
    chip, core = tp // 2, lax.rem(tp, 2)
    chips = n_tp // 2
    sibling = tp + 1 - 2 * core
    other = 1 - grp
    edge = (sp == 0) | (sp == n_sp - 1)
    inner = (sp > 0) & (sp < n_sp - 1)
    helps = (sp == 1) | (sp == n_sp - 2)
    helper = jnp.where(sp == 0, 1, n_sp - 2)
    helped = jnp.where(sp == 1, 0, n_sp - 1)
    sources = (wk_h, wg_h, wv_h, wq_h, wa_h, wb_h)
    plain = {KEY: wk, VALUE: wv, QUERY: wq}

    def remote(src, dst, send, recv, **where):
        return pltpu.make_async_remote_copy(
            src_ref=src, dst_ref=dst, send_sem=send, recv_sem=recv, device_id=where, device_id_type=MESH
        )

    halves = z_send.shape[3]
    slab = rows // halves

    def source(w, k=None):
        if w == GATE:
            return wg_h
        size = channels if w in (GLU, OPEN) else cols
        lanes = pl.ds(pl.multiple_of(grp * size, 128), size)
        return sources[w].at[:, lanes] if k is None else sources[w].at[pl.ds(k * slab, slab), lanes]

    def target(w, index, k=None):
        if w == GATE:
            return wg.at[index]
        if k is None:
            at = pl.ds(pl.multiple_of(index * rows, 16), rows)
        else:
            at = pl.ds(pl.multiple_of(index * rows + k * slab, 16), slab)
        if w in (GLU, OPEN):
            return wab.at[at, pl.ds(channels if w == OPEN else 0, channels)]
        return plain[w].at[at]

    load_tok = pltpu.make_async_copy(tok_h, tok, local_sem.at[0])
    load_tok.start()
    own = [pltpu.make_async_copy(source(w), target(w, sp), local_sem.at[1 + w]) for w in range(6)]
    for w in (KEY, GATE, VALUE, QUERY):
        own[w].start()

    @pl.when(inner)
    def _():
        own[GLU].start()
        own[OPEN].start()

    def od_rows(index):
        return pl.ds(pl.multiple_of(index * columns, 16), columns)

    load_od = pltpu.make_async_copy(od_h.at[od_rows(tp)], odg.at[tp], local_sem.at[7])
    load_oc = pltpu.make_async_copy(oc_h.at[od_rows(tp)], ocg.at[tp], local_sem.at[8])
    load_od.start()
    load_oc.start()

    barrier = pltpu.get_barrier_semaphore()

    def greet(**where):
        pl.semaphore_signal(barrier, inc=1, device_id=where, device_id_type=MESH)

    for step in range(n_tp - 1):
        peer = lax.rem(tp + step + 1, n_tp)
        greet(tp=peer)
        greet(tp=peer, grp=other)
    greet(grp=other)

    @pl.when(sp > 0)
    def _():
        greet(sp=sp - 1)
        greet(sp=sp - 1, grp=other)

    @pl.when(sp < n_sp - 1)
    def _():
        greet(sp=sp + 1)
        greet(sp=sp + 1, grp=other)

    load_tok.wait()
    chunk = 64
    for at in range(0, length, chunk):
        here = tok[at:at + chunk, :].astype(F32)
        scale = lax.rsqrt(jnp.mean(here * here, axis=-1, keepdims=True) + EPSILON)
        nt[at:at + chunk, :] = (here * scale * gain[...]).astype(BF16)

    @pl.when(edge)
    def _():
        pl.semaphore_wait(barrier, 2 * n_tp + 1)

    @pl.when(inner)
    def _():
        pl.semaphore_wait(barrier, 2 * n_tp + 3)

    def wide(w):
        return 1 if w in (GLU, OPEN) else 0

    def arrives(w, side, d):
        ok = (sp - d >= 0) if side == 0 else (sp + d < n_sp)
        return ok & inner if wide(w) else ok

    def leaves(w, side, d):
        if side == 0:
            return (sp - (d - 1) >= 0) & (sp < n_sp - 1 - wide(w))
        return (sp + (d - 1) < n_sp) & (sp > wide(w))

    def cuts(w):
        return range(1 if w == GATE else halves)

    def z_copy(w, side, d, k):
        back = d - 1
        place = target(w, sp - back if side == 0 else sp + back, k)
        return remote(
            source(w, k) if d == 1 else place, place,
            z_send.at[w, side, d - 1, k], z_recv.at[w, side, d - 1, k],
            sp=sp + 1 if side == 0 else sp - 1,
        )

    def z_arrival(w, side, d, k):
        place = target(w, sp - d if side == 0 else sp + d, k)
        return remote(
            place, place, z_send.at[w, side, d - 1, k], z_recv.at[w, side, d - 1, k],
            sp=sp + 1 if side == 0 else sp - 1,
        )

    def offer(w, where):
        for side in range(2):
            @pl.when(leaves(w, side, 1) & where)
            def _(side=side):
                for k in cuts(w):
                    z_copy(w, side, 1, k).start()

    def relay(w, d):
        if d > n_sp - 1:
            return
        for k in cuts(w):
            for side in range(2):
                @pl.when(arrives(w, side, d))
                def _(side=side, k=k):
                    z_arrival(w, side, d, k).wait_recv()
                    if d < n_sp - 1:
                        @pl.when(leaves(w, side, d + 1))
                        def _():
                            z_copy(w, side, d + 1, k).start()

    pieces = ty_send.shape[1]
    half = length // 2
    piece = half // pieces

    def part(block, side, c):
        return nt.at[pl.ds(pl.multiple_of(block * length + side * half + c * piece, 16), piece)]

    def tok_y(k, c):
        return remote(part(2 * k, core, c), part(2 * k + 1, core, c), ty_send.at[k, c], ty_recv.at[k, c], grp=other)

    def tok_z(c):
        return remote(part(0, core, c), part(2, core, c), tz_send.at[c], tz_recv.at[c], sp=helper)

    def tok_f(block, c):
        return remote(
            part(block, core, c), part(block, core, c), tf_send.at[block - 1, c], tf_recv.at[block - 1, c], tp=sibling
        )

    def tok_f_arrival(block, c):
        place = part(block, 1 - core, c)
        return remote(place, place, tf_send.at[block - 1, c], tf_recv.at[block - 1, c], tp=sibling)

    def pass_y(k, c):
        tok_y(k, c).wait_recv()
        tok_f(2 * k + 1, c).start()

    def pass_z(c):
        @pl.when(helps)
        def _():
            tok_z(c).wait_recv()
            tok_y(1, c).start()
            tok_f(2, c).start()

    def pass_far(c):
        @pl.when(helps)
        def _():
            pass_y(1, c)

    ld_copy = remote(ldt, ldo, ld_send.at[0], ld_recv.at[0], grp=other)

    def od_copy(m, step):
        dest = lax.rem(tp + step + 1, n_tp)
        src, dst = ((od_h, odg), (oc_h, ocg))[m]
        return remote(src.at[od_rows(dest)], dst.at[tp], od_send.at[m, step], od_recv.at[m, step], tp=dest)

    def od_arrival(m, step):
        origin = lax.rem(tp + n_tp - step - 1, n_tp)
        place = (odg, ocg)[m].at[origin]
        return remote(place, place, od_send.at[m, step], od_recv.at[m, step], tp=origin)

    everywhere = sp >= 0
    offer(GATE, everywhere)
    offer(KEY, everywhere)
    for c in range(pieces):
        tok_y(0, c).start()
    ld_copy.start()
    offer(VALUE, everywhere)
    offer(GLU, edge)

    @pl.when(edge)
    def _():
        for c in range(pieces):
            tok_z(c).start()

    offer(OPEN, edge)
    offer(QUERY, edge)
    for m in (1, 0):
        for step in range(n_tp - 1):
            od_copy(m, step).start()

    def dot(a, b, dims=NN):
        return lax.dot_general(a, b, dims, preferred_element_type=F32)

    def unit_rows(tensor):
        return tensor * lax.rsqrt(jnp.sum(tensor * tensor, axis=-1, keepdims=True) + EPSILON)

    def silu(tensor):
        return tensor * jax.nn.sigmoid(tensor)

    relay(GATE, 1)
    relay(KEY, 1)
    offer(GLU, inner)
    pass_y(0, 0)
    relay(GATE, 2)
    relay(VALUE, 1)
    pass_y(0, 1)
    offer(OPEN, inner)
    relay(KEY, 2)
    pass_y(0, 2)
    relay(GLU, 1)
    offer(QUERY, inner)
    pass_y(0, 3)
    for d in range(3, n_sp):
        relay(GATE, d)
        relay(KEY, d)
    pass_z(0)
    own[GATE].wait()
    own[KEY].wait()
    ld_copy.wait_recv()
    for c in range(pieces):
        tok_f_arrival(1, c).wait_recv()

    both = 2 * length
    gate_cols = jnp.zeros((both, wg.shape[1]), F32)
    gate_rows = jnp.zeros((wg.shape[1], both), F32)
    for index in range(n_sp):
        normed_part = nt[0:both, index * rows:(index + 1) * rows]
        gate_cols = gate_cols + dot(normed_part, wg[index], NT)
        gate_rows = gate_rows + dot(wg[index], normed_part, NT)
    mine = grp == 0
    gates = 4 * heads
    gate_cols = jnp.where(mine, gate_cols[:, :gates], gate_cols[:, gates:])
    gate_rows = jnp.where(mine, gate_rows[:gates, :], gate_rows[gates:, :])
    rates = [
        jnp.where(mine, log[:2 * heads, :], log[2 * heads:, :]) for log in (ldt[...], ldo[...])
    ]

    row_at = lax.broadcasted_iota(jnp.int32, (length, length), 0)
    col_at = lax.broadcasted_iota(jnp.int32, (length, length), 1)
    same = row_at == col_at

    key_proj = silu(dot(nt[0:both, :], wk[...]))
    pass_z(1)
    relay(VALUE, 2)
    for u, (j, h) in enumerate(units):
        keys[u] = unit_rows(key_proj[j * length:(j + 1) * length, h * head_width:(h + 1) * head_width])
    for u, (j, h) in enumerate(units):
        grams = bdot(keys[u], keys[u], NT)
        for r in range(2):
            p = 2 * u + r
            g = 4 * h + 2 * r
            span = slice(j * length, (j + 1) * length)
            decay_row = rates[j][2 * h + r:2 * h + r + 1, :] * (0.5 + jax.nn.sigmoid(gate_rows[g:g + 1, span]))
            beta = jax.nn.sigmoid(gate_cols[span, g + 1:g + 2] - BETA_SHIFT)
            seen = col_at <= row_at if r == 0 else col_at >= row_at
            cum_col = jnp.sum(jnp.where(seen, decay_row, 0.0), axis=1, keepdims=True)
            cum_row = jnp.sum(jnp.where(same, cum_col, 0.0), axis=0, keepdims=True)
            weighting = jnp.where(seen, jnp.exp(jnp.where(seen, cum_col - cum_row, 0.0)), 0.0)
            gaps[p] = weighting
            betas[p] = jnp.broadcast_to(beta, (length, head_width))
            cums[p] = jnp.broadcast_to(cum_col, (length, head_width))
            lower = jnp.where(same, 0.0, grams * weighting * beta)
            rhs[p] = lower
            near = (row_at // 2 == col_at // 2)
            xinv[p] = jnp.where(same, 1.0, jnp.where(near, -lower, 0.0))

    service = {
        2: [lambda: pass_z(2), lambda: pass_far(0)],
        8: [lambda: pass_far(1)],
        32: [lambda: pass_z(3)],
        128: [lambda: pass_far(2)],
    }
    size = 2
    while size < length:
        inside = (row_at // (2 * size) == col_at // (2 * size)) & (row_at // size != col_at // size)
        for p in range(len(pairs)):
            across = jnp.where(inside, rhs[p], 0.0)
            inverse = xinv[p]
            xinv[p] = inverse - bdot(inverse, bdot(across, inverse))
        for act in service.get(size, ()):
            act()
        size *= 2

    own[VALUE].wait()
    for d in range(3, n_sp):
        relay(VALUE, d)
    value_proj = silu(dot(nt[0:both, :], wv[...]))
    eye = (
        lax.broadcasted_iota(jnp.int32, (head_width, head_width), 0)
        == lax.broadcasted_iota(jnp.int32, (head_width, head_width), 1)
    )
    for u, r in pairs:
        p = 2 * u + r
        j, h = units[u]
        beta, cum, key = betas[p], cums[p], keys[u]
        value = value_proj[j * length:(j + 1) * length, h * head_width:(h + 1) * head_width]
        total = cum[length - 1:length, :] if r == 0 else cum[0:1, :]
        right = jnp.concatenate([beta * value, beta * key * jnp.exp(cum)], axis=1)
        solved = bdot(xinv[p], right)
        vals[p] = solved.astype(BF16)
        passed = bdot(key * jnp.exp(total - cum), solved, TN)
        ends[p] = passed[:, :head_width]
        maps[p] = (jnp.where(eye, jnp.exp(total), 0.0) - passed[:, head_width:]).astype(BF16)

    def place_of(r):
        return sp if r == 0 else n_sp - 1 - sp

    def chain_copy(r):
        dest = sp + 1 if r == 0 else sp - 1
        return remote(chain_out.at[r], chain_in.at[r], chain_send.at[r], chain_recv.at[r], sp=dest)

    def chain_point(low, high):
        for r in range(2):
            at = place_of(r)

            @pl.when((at >= low) & (at <= high))
            def _(r=r, at=at):
                if low == 0:
                    for u in range(n_units):
                        chain_in[r, u] = jnp.zeros((head_width, head_width), BF16)
                        chain_out[r, u] = ends[2 * u + r].astype(BF16)
                else:
                    chain_copy(r).wait_recv()
                    for u in range(n_units):
                        p = 2 * u + r
                        chain_out[r, u] = (bdot(maps[p], chain_in[r, u]) + ends[p]).astype(BF16)

                @pl.when(at < n_sp - 1)
                def _():
                    chain_copy(r).start()

    chain_point(0, 0)
    relay(OPEN, 1)
    pass_far(3)
    relay(QUERY, 1)
    chain_point(1, 1)

    def block_dot(first, count, w_ref, index):
        lanes = pl.ds(pl.multiple_of(index * rows, 128), rows)
        at = pl.ds(pl.multiple_of(index * rows, 128), rows)
        return dot(nt[first * length:(first + count) * length, lanes], w_ref[at, :])

    def neighbours(w, d, action):
        for side in range(2):
            @pl.when(arrives(w, side, d))
            def _(side=side):
                action(sp - d if side == 0 else sp + d)

    def add_wide(index, fresh=False):
        x = block_dot(0, 2, wab, index)
        acc_ab[0:both, :] = x if fresh else acc_ab[0:both, :] + x

        @pl.when(helps)
        def _():
            y = block_dot(2, 2, wab, index)
            acc_ab[both:, :] = y if fresh else acc_ab[both:, :] + y

    def add_query(index, fresh=False):
        x = block_dot(0, 2, wq, index)
        acc_q[...] = x if fresh else acc_q[...] + x

    @pl.when(inner)
    def _():
        own[GLU].wait()
        own[OPEN].wait()

        @pl.when(helps)
        def _():
            for c in range(pieces):
                tok_f_arrival(2, c).wait_recv()
                tok_f_arrival(3, c).wait_recv()

        add_wide(sp, True)
    neighbours(GLU, 1, add_wide)
    for d in range(2, n_sp - 1):
        relay(GLU, d)
        relay(OPEN, d)
        neighbours(GLU, d, add_wide)

    def gated(first, count):
        x = acc_ab[first * length:(first + count) * length, :]
        return (x[:, :channels] * jax.nn.sigmoid(x[:, channels:])).astype(BF16)

    def owner(j):
        return grp if j == 0 else other

    def main_y():
        return remote(gout, main_in.at[grp], main_send.at[0], main_recv.at[grp], grp=other)

    def main_arrival(h):
        return remote(main_in.at[h], main_in.at[h], main_send.at[0], main_recv.at[h], grp=other)

    def far_copy(j):
        return remote(gend.at[j], main_in.at[grp], far_send.at[j], main_recv.at[grp], sp=helped, grp=owner(j))

    def edge_copy(side, j):
        start = length - HALO if side == 0 else 0
        src = main_in.at[grp, pl.ds(start, HALO)] if j == 0 else gout.at[pl.ds(start, HALO)]
        return remote(
            src, edge_in.at[side, grp], edge_send.at[side, j], edge_recv.at[side, grp],
            sp=sp + 1 if side == 0 else sp - 1, grp=owner(j),
        )

    def rim_copy(side):
        start = length - HALO if side == 0 else 0
        return remote(
            gend.at[1, pl.ds(start, HALO)], edge_in.at[side, grp], rim_send.at[side], edge_recv.at[side, grp], grp=other
        )

    def edge_arrival(side, h):
        place = edge_in.at[side, h]
        return remote(place, place, edge_send.at[side, 0], edge_recv.at[side, h], grp=other)

    @pl.when(inner)
    def _():
        @pl.when(helps)
        def _():
            far = gated(2, 2)
            gend[0] = far[:length]
            gend[1] = far[length:]
            for j in range(2):
                far_copy(j).start()
            for side, at in ((0, 1), (1, n_sp - 2)):
                @pl.when(sp == at)
                def _(side=side):
                    rim_copy(side).start()
                    start = length - HALO if side == 0 else 0
                    edge_in[side, grp] = gend[0, start:start + HALO, :]

        near = gated(0, 2)
        main_in[grp] = near[:length]
        gout[...] = near[length:]
        main_y().start()
        for side in range(2):
            for j in range(2):
                edge_copy(side, j).start()

    own[QUERY].wait()
    add_query(sp, True)
    neighbours(QUERY, 1, add_query)
    for d in range(2, n_sp - 1):
        chain_point(d, d)
        relay(QUERY, d)
        neighbours(QUERY, d, add_query)
    chain_point(n_sp - 1, n_sp - 1)

    for h in range(2):
        @pl.when(~(inner & (grp == h)))
        def _(h=h):
            main_arrival(h).wait_recv()

        @pl.when((sp > 0) & ~((sp == 1) & (grp == h)))
        def _(h=h):
            edge_arrival(0, h).wait_recv()

        @pl.when((sp < n_sp - 1) & ~((sp == n_sp - 2) & (grp == h)))
        def _(h=h):
            edge_arrival(1, h).wait_recv()

        pad[h, HALO:HALO + length, :] = main_in[h].astype(F32)
        for side, start, none in ((0, 0, 0), (1, HALO + length, n_sp - 1)):
            @pl.when(sp != none)
            def _(h=h, side=side, start=start):
                pad[h, start:start + HALO, :] = edge_in[side, h].astype(F32)

            @pl.when(sp == none)
            def _(h=h, start=start):
                pad[h, start:start + HALO, :] = jnp.zeros((HALO, channels), F32)

    taps = ck.shape[0]
    for h in range(2):
        lanes = slice(h * channels, (h + 1) * channels)
        for at in range(0, length, chunk):
            first = at + HALO - taps // 2
            total = pad[h, first:first + chunk, :] * ck[0:1, lanes]
            for k in range(1, taps):
                total = total + pad[h, first + k:first + k + chunk, :] * ck[k:k + 1, lanes]
            conv[at:at + chunk, lanes] = total
    filtered = conv[...]
    sum_col = jnp.sum(filtered, axis=-1, keepdims=True)
    square_col = jnp.sum(filtered * filtered, axis=-1, keepdims=True)
    stat_out[...] = jnp.zeros(stat_out.shape, F32)
    stat_out[0:1, :] = jnp.sum(jnp.where(same, sum_col, 0.0), axis=0, keepdims=True)
    stat_out[1:2, :] = jnp.sum(jnp.where(same, square_col, 0.0), axis=0, keepdims=True)

    def stat_copy(step):
        return remote(
            stat_out, stat_in.at[step], stat_send.at[step], stat_recv.at[step], tp=lax.rem(tp + step + 1, n_tp)
        )

    for step in range(n_tp - 1):
        stat_copy(step).start()

    relay(QUERY, n_sp - 1)
    neighbours(QUERY, n_sp - 1, add_query)

    def read(u):
        j, h = units[u]
        query = silu(acc_q[j * length:(j + 1) * length, h * head_width:(h + 1) * head_width])
        query = unit_rows(query) * head_width ** -0.5
        scores = bdot(query, keys[u], NT)
        for r in range(2):
            p = 2 * u + r
            pair = dot((scores * gaps[p]).astype(BF16), vals[p])
            reads[p] = (query * jnp.exp(cums[p]) - pair[:, head_width:]).astype(BF16)
            if r == 0:
                local_out[u] = pair[:, :head_width]
            else:
                local_out[u] = local_out[u] + pair[:, :head_width]

    def mixed_head(u):
        joined = local_out[u] + dot(reads[2 * u], chain_in[0, u]) + dot(reads[2 * u + 1], chain_in[1, u])
        scale = lax.rsqrt(jnp.mean(joined * joined, axis=-1, keepdims=True) + EPSILON)
        return (joined * scale * hgain[...]).astype(BF16)

    def chip_at(q):
        return lax.rem(chip + q, chips)

    def chip_back(q):
        return lax.rem(chip + chips - q, chips)

    def dg_copy(a, q):
        src = dall.at[tp, grp] if a == 0 else dm_out
        where = {"tp": chip_at(q) * 2 + core}
        if a:
            where["grp"] = other
        return remote(src, dall.at[tp, grp], dg_send.at[a, q], dg_recv.at[a, q], **where)

    def d_block(a, q, side):
        return dall.at[chip_back(q) * 2 + side, other if a else grp]

    def dg_arrival(a, q):
        place = d_block(a, q, core)
        return remote(place, place, dg_send.at[a, q], dg_recv.at[a, q], tp=sibling)

    def df_copy(a, q, arriving=False):
        place = d_block(a, q, 1 - core if arriving else core)
        return remote(place, place, df_send.at[a, q], df_recv.at[a, q], tp=sibling)

    def cg_copy(q):
        return remote(call.at[tp], call.at[tp], cg_send.at[q], cg_recv.at[q], tp=chip_at(q) * 2 + core)

    def cg_arrival(q):
        place = call.at[chip_back(q) * 2 + core]
        return remote(place, place, cg_send.at[q], cg_recv.at[q], tp=sibling)

    def cf_copy(q, arriving=False):
        place = call.at[chip_back(q) * 2 + (1 - core if arriving else core)]
        return remote(place, place, cf_send.at[q], cf_recv.at[q], tp=sibling)

    direct = [(a, q) for q in range(chips) for a in (1, 0) if (a, q) != (0, 0)]

    for h in range(heads):
        read(heads + h)
        dm_out[:, h * head_width:(h + 1) * head_width] = mixed_head(heads + h)
    for q in range(chips - 1, -1, -1):
        dg_copy(1, q).start()
    for h in range(heads):
        read(h)
        dall[tp, grp, :, h * head_width:(h + 1) * head_width] = mixed_head(h)
    for q in range(1, chips):
        dg_copy(0, q).start()
    df_copy(0, 0).start()

    stats = stat_out[0:2, :]
    for step in range(n_tp - 1):
        stat_copy(step).wait_recv()
        stats = stats + stat_in[step, 0:2, :]
    center = jnp.sum(jnp.where(same, stats[0:1, :], 0.0), axis=1, keepdims=True) / conv_total
    squares = jnp.sum(jnp.where(same, stats[1:2, :], 0.0), axis=1, keepdims=True) / conv_total
    spread = squares - center * center
    normal = (conv[...] - center) * lax.rsqrt(spread + EPSILON)
    call[tp] = silu(normal * ng[...] + ns[...]).astype(BF16)
    for q in range(1, chips):
        cg_copy(q).start()
    cf_copy(0).start()

    for m in range(2):
        for step in range(n_tp - 1):
            od_arrival(m, step).wait_recv()
    load_od.wait()
    load_oc.wait()

    for a, q in direct:
        dg_arrival(a, q).wait_recv()
        df_copy(a, q).start()
    for q in range(1, chips):
        cg_arrival(q).wait_recv()
        cf_copy(q).start()

    def delta_term(t):
        return dot(jnp.concatenate([dall[t, 0], dall[t, 1]], axis=1), odg[t], NT)

    def conv_term(t):
        return dot(call[t], ocg[t], NT)

    result = delta_term(tp)
    for q in range(chips):
        t = chip_back(q) * 2 + core
        if q:
            result = result + delta_term(t)
        result = result + conv_term(t)
    for q in range(chips):
        t = chip_back(q) * 2 + 1 - core
        df_copy(0, q, True).wait_recv()
        df_copy(1, q, True).wait_recv()
        result = result + delta_term(t)
    for q in range(chips):
        t = chip_back(q) * 2 + 1 - core
        cf_copy(q, True).wait_recv()
        result = result + conv_term(t)
    out[...] = result.astype(BF16)

    for w in range(6):
        for d in range(1, n_sp):
            for side in range(2):
                @pl.when(leaves(w, side, d))
                def _(w=w, d=d, side=side):
                    for k in cuts(w):
                        z_copy(w, side, d, k).wait_send()
    for c in range(pieces):
        tok_y(0, c).wait_send()
        tok_f(1, c).wait_send()

        @pl.when(edge)
        def _(c=c):
            tok_z(c).wait_send()

        @pl.when(helps)
        def _(c=c):
            tok_y(1, c).wait_send()
            tok_f(2, c).wait_send()
            tok_f(3, c).wait_send()
    ld_copy.wait_send()
    for m in range(2):
        for step in range(n_tp - 1):
            od_copy(m, step).wait_send()
    for r in range(2):
        @pl.when(place_of(r) < n_sp - 1)
        def _(r=r):
            chain_copy(r).wait_send()

    @pl.when(inner)
    def _():
        main_y().wait_send()
        for side in range(2):
            for j in range(2):
                edge_copy(side, j).wait_send()

    @pl.when(helps)
    def _():
        for j in range(2):
            far_copy(j).wait_send()
    for side, at in ((0, 1), (1, n_sp - 2)):
        @pl.when(sp == at)
        def _(side=side):
            rim_copy(side).wait_send()
    for step in range(n_tp - 1):
        stat_copy(step).wait_send()
    df_copy(0, 0).wait_send()
    for a, q in direct:
        dg_copy(a, q).wait_send()
        df_copy(a, q).wait_send()
    for q in range(chips):
        if q:
            cg_copy(q).wait_send()
        cf_copy(q).wait_send()


def solution(mesh):
    n_grp, n_sp, n_tp = mesh.shape["grp"], mesh.shape["sp"], mesh.shape["tp"]

    def on_device(tokens_in, input_gain, w_query, w_key, w_value, w_gates, w_glu_value,
                  sigmoid_opener_matrix, log_decay, head_gain, conv_kernel, norm_gain, norm_shift,
                  out_delta, out_conv):
        length, width = tokens_in.shape
        head_width = head_gain.shape[0]
        head_cols = w_query.shape[1]
        heads = head_cols // head_width
        channels = w_glu_value.shape[1]
        rows = w_query.shape[0]
        pairs = 2 * heads
        columns = width // n_tp
        dma, vmem = pltpu.SemaphoreType.DMA, pltpu.VMEM
        anywhere = pl.BlockSpec(memory_space=pltpu.HBM)
        inside = pl.BlockSpec(memory_space=pltpu.VMEM)
        if n_grp == 2 and n_sp >= 4 and n_tp % 2 == 0 and heads % 2 == 0 and channels % 256 == 0:
            cols, ch, chips, steps = head_cols // 2, channels // 2, n_tp // 2, n_tp - 1
            pieces = 4
            scratch = [
                vmem((length, width), BF16), vmem((4 * length, width), BF16),
                vmem((width, cols), BF16), vmem((width, cols), BF16), vmem((width, cols), BF16),
                vmem((width, 2 * ch), BF16), vmem((n_sp, 4 * heads, rows), BF16),
                vmem((n_tp, columns, head_cols), BF16), vmem((n_tp, columns, channels), BF16),
                vmem((pairs, length), F32),
                vmem((heads, length, head_width), F32), vmem((pairs, length, 2 * head_width), BF16),
                vmem((pairs, length, head_width), F32), vmem((pairs, length, head_width), F32),
                vmem((pairs, length, length), F32), vmem((pairs, length, length), F32),
                vmem((pairs, length, length), F32),
                vmem((heads, length, head_width), F32), vmem((pairs, length, head_width), BF16),
                vmem((pairs, head_width, head_width), BF16), vmem((pairs, head_width, head_width), F32),
                vmem((2, heads, head_width, head_width), BF16), vmem((2, heads, head_width, head_width), BF16),
                vmem((length, ch), BF16), vmem((2, length, ch), BF16), vmem((2, length, ch), BF16),
                vmem((2, 2, HALO, ch), BF16),
                vmem((2, length + 2 * HALO, ch), F32), vmem((length, channels), F32),
                vmem((8, length), F32), vmem((steps, 8, length), F32),
                vmem((n_tp, 2, length, cols), BF16), vmem((length, cols), BF16),
                vmem((n_tp, length, channels), BF16), vmem((4 * length, 2 * ch), F32), vmem((2 * length, cols), F32),
                dma((9,)),
                dma((6, 2, n_sp - 1, 2)), dma((6, 2, n_sp - 1, 2)),
                dma((2, pieces)), dma((2, pieces)), dma((3, pieces)), dma((3, pieces)),
                dma((pieces,)), dma((pieces,)),
                dma((1,)), dma((1,)), dma((2, steps)), dma((2, steps)), dma((2,)), dma((2,)),
                dma((1,)), dma((2,)), dma((2, 2)), dma((2, 2)), dma((2,)), dma((2,)),
                dma((steps,)), dma((steps,)),
                dma((2, chips)), dma((2, chips)), dma((2, chips)), dma((2, chips)),
                dma((chips,)), dma((chips,)), dma((chips,)), dma((chips,)),
            ]
            return pl.pallas_call(
                functools.partial(fused, (n_sp, n_tp, float(channels * n_tp))),
                out_shape=jax.ShapeDtypeStruct((length, columns), BF16),
                in_specs=[anywhere, inside] + [anywhere] * 6 + [inside] * 5 + [anywhere] * 2,
                out_specs=inside,
                scratch_shapes=scratch,
                compiler_params=pltpu.CompilerParams(
                    collective_id=0, has_side_effects=True, vmem_limit_bytes=58 * 1024 * 1024
                ),
            )(
                tokens_in, input_gain.reshape(1, width), w_key, w_gates.T, w_value, w_query,
                w_glu_value, sigmoid_opener_matrix, log_decay.T,
                head_gain.reshape(1, head_width), conv_kernel, norm_gain.reshape(1, channels),
                norm_shift.reshape(1, channels), out_delta, out_conv,
            )
        scratch = [
            vmem((length, width), BF16), vmem((length, width), BF16),
            vmem((width, head_cols), BF16), vmem((n_sp, 4 * heads, rows), BF16),
            vmem((width, head_cols), BF16), vmem((width, head_cols), BF16),
            vmem((width, channels), BF16), vmem((width, channels), BF16),
            vmem((width, head_cols), BF16), vmem((width, channels), BF16),
            vmem((heads, length, head_width), F32), vmem((pairs, length, 2 * head_width), BF16),
            vmem((pairs, length, head_width), F32), vmem((pairs, length, head_width), F32),
            vmem((pairs, length, length), F32), vmem((pairs, length, length), F32),
            vmem((pairs, length, length), F32),
            vmem((heads, length, head_width), F32), vmem((pairs, length, head_width), BF16),
            vmem((pairs, head_width, head_width), BF16), vmem((pairs, head_width, head_width), F32),
            vmem((2, heads, head_width, head_width), BF16), vmem((2, heads, head_width, head_width), BF16),
            vmem((length, channels), BF16), vmem((2, HALO, channels), BF16),
            vmem((length + 2 * HALO, channels), F32), vmem((length, channels), F32),
            vmem((8, length), F32), vmem((n_tp - 1, 8, length), F32),
            vmem((n_tp, length, columns), F32),
            vmem((n_tp // 2, length, columns), BF16), vmem((n_tp // 2, length, columns), BF16),
            vmem((n_tp // 2, length, columns), BF16), vmem((n_tp // 2, length, columns), BF16),
            dma((9,)),
            dma((6, 2, n_sp - 1)), dma((6, 2, n_sp - 1)),
            dma((6, 2, n_sp - 1)), dma((6, 2, n_sp - 1)),
            dma((2,)), dma((2,)), dma((2,)), dma((2,)),
            dma((n_tp - 1,)), dma((n_tp - 1,)), dma((n_tp // 2,)), dma((n_tp // 2,)),
            dma((n_tp // 2,)), dma((n_tp // 2,)),
        ]
        return pl.pallas_call(
            functools.partial(kernel, (n_grp, n_sp, n_tp, float(channels * n_tp))),
            out_shape=jax.ShapeDtypeStruct((length, columns), BF16),
            in_specs=[anywhere, inside] + [anywhere] * 6 + [inside] * 6 + [anywhere] * 2,
            out_specs=inside,
            scratch_shapes=scratch,
            compiler_params=pltpu.CompilerParams(
                collective_id=0, has_side_effects=True, vmem_limit_bytes=60 * 1024 * 1024
            ),
        )(
            tokens_in, input_gain.reshape(1, width), w_key, w_gates.T, w_value, w_query,
            w_glu_value, sigmoid_opener_matrix, log_decay, log_decay.T,
            head_gain.reshape(1, head_width), conv_kernel, norm_gain.reshape(1, channels),
            norm_shift.reshape(1, channels), out_delta, out_conv,
        )

    placed = (
        P(("grp", "sp"), None), P(), P("sp", "tp"), P("sp", "tp"), P("sp", "tp"), P("sp", "tp"),
        P("sp", "tp"), P("sp", "tp"), P(("grp", "sp"), "tp"), P(), P(None, "tp"), P("tp"), P("tp"),
        P(None, "tp"), P(None, "tp"),
    )
    return jax.shard_map(
        on_device, mesh=mesh, in_specs=placed, out_specs=P(("grp", "sp"), "tp"), check_vma=False
    )
```

```python
import functools

import jax
import jax.numpy as jnp
from jax import lax
from jax.experimental import pallas as pl
from jax.experimental.pallas import tpu as pltpu
from jax.sharding import PartitionSpec as P

EPSILON = 1e-06
BETA_SHIFT = 6.0
HALO = 16
MESH = pl.DeviceIdType.MESH
F32 = jnp.float32
BF16 = jnp.bfloat16
NT = (((1,), (1,)), ((), ()))
TN = (((0,), (0,)), ((), ()))
NN = (((1,), (0,)), ((), ()))
KEY, GATE, VALUE, QUERY, GLU, OPEN = range(6)


def bdot(left, right, dims=NN):
    return lax.dot_general(
        left.astype(BF16), right.astype(BF16), dims, preferred_element_type=F32
    )


def each(count, action):
    if count <= 8:
        for step in range(count):
            action(step)
    else:
        def body(step, carry):
            action(step)
            return carry

        lax.fori_loop(0, count, body, 0)


def kernel(cfg, tok_h, gain, wk_h, wg_h, wv_h, wq_h, wa_h, wb_h, ld, ldt, hgain, ck, ng, ns, od_h, oc_h,
           out,
           tok, normed, wk, wg, wv, wq, wa, wb, od, oc,
           keys, vals, betas, cums, xinv, gaps, rhs, local_out, reads, maps, ends,
           chain_in, chain_out, glu, halo, pad, conv, stat_out, stat_in, conv_acc, part_out, part_in, pair_out, pair_in,
           local_sem, z_send, z_recv, y_send, y_recv, chain_send, chain_recv,
           halo_send, halo_recv, stat_send, stat_recv, part_send, part_recv, pair_send, pair_recv):
    n_grp, n_sp, n_tp, conv_total = cfg
    grp, sp, tp = lax.axis_index("grp"), lax.axis_index("sp"), lax.axis_index("tp")
    length, width = tok.shape
    rows = wk_h.shape[0]
    channels = wa.shape[1]
    head_width = hgain.shape[1]
    heads = wk.shape[1] // head_width
    share = (rows // 2) // 16 * 16 if n_grp == 2 else 0
    pulled = rows - share

    sources = (wk_h, wg_h, wv_h, wq_h, wa_h, wb_h)
    targets = (wk, wg, wv, wq, wa, wb)

    def block_of(w, index, start, count):
        if w == GATE:
            return targets[w].at[index]
        return targets[w].at[pl.ds(pl.multiple_of(index * rows + start, 16), count)]

    load_tok = pltpu.make_async_copy(tok_h, tok, local_sem.at[0])
    load_tok.start()
    own = [
        pltpu.make_async_copy(sources[w], block_of(w, sp, 0, rows), local_sem.at[1 + w])
        for w in range(6)
    ]
    for copy in own:
        copy.start()
    load_od = pltpu.make_async_copy(od_h, od, local_sem.at[7])
    load_oc = pltpu.make_async_copy(oc_h, oc, local_sem.at[8])

    barrier = pltpu.get_barrier_semaphore()

    def greet(axis, me, count):
        def one(step):
            pl.semaphore_signal(
                barrier, inc=1, device_id={axis: lax.rem(me + step + 1, count)}, device_id_type=MESH
            )

        each(count - 1, one)

    greet("sp", sp, n_sp)
    greet("tp", tp, n_tp)
    greet("grp", grp, n_grp)
    pl.semaphore_wait(barrier, n_sp + n_tp + n_grp - 3)

    def origin(side, d):
        return sp - d if side == 0 else sp + d

    def arrives(side, d):
        return sp - d >= 0 if side == 0 else sp + d < n_sp

    def leaves(side, d):
        if side == 0:
            return (sp - (d - 1) >= 0) & (sp < n_sp - 1)
        return (sp + (d - 1) < n_sp) & (sp > 0)

    def part_of(w, index, side_of):
        if w == GATE:
            return block_of(w, index, 0, 0)
        if not share:
            return block_of(w, index, 0, rows)
        if side_of is None:
            return block_of(w, index, pl.multiple_of(grp * share, 16), pulled)
        return block_of(w, index, pl.multiple_of(side_of * pulled, 16), share)

    def z_copy(w, side, d, first=False):
        target = part_of(w, origin(side, d - 1), None)
        source = target
        if first:
            source = sources[w]
            if w != GATE and share:
                source = source.at[pl.ds(pl.multiple_of(grp * share, 16), pulled)]
        return pltpu.make_async_remote_copy(
            src_ref=source, dst_ref=target,
            send_sem=z_send.at[w, side, d - 1], recv_sem=z_recv.at[w, side, d - 1],
            device_id={"sp": sp + 1 if side == 0 else sp - 1}, device_id_type=MESH,
        )

    def z_arrival(w, side, d):
        place = part_of(w, origin(side, d), None)
        return pltpu.make_async_remote_copy(
            src_ref=place, dst_ref=place,
            send_sem=z_send.at[w, side, d - 1], recv_sem=z_recv.at[w, side, d - 1],
            device_id={"sp": sp + 1 if side == 0 else sp - 1}, device_id_type=MESH,
        )

    def y_copy(w, side, d, arriving=False):
        place = part_of(w, origin(side, d), 1 - grp if arriving else grp)
        return pltpu.make_async_remote_copy(
            src_ref=place, dst_ref=place,
            send_sem=y_send.at[w, side, d - 1], recv_sem=y_recv.at[w, side, d - 1],
            device_id={"grp": 1 - grp}, device_id_type=MESH,
        )

    def offer(w):
        for side in range(2):
            @pl.when(leaves(side, 1))
            def _(side=side):
                z_copy(w, side, 1, True).start()

    def relay_hop(w, d):
        for side in range(2):
            @pl.when(arrives(side, d))
            def _(side=side):
                z_arrival(w, side, d).wait_recv()

                @pl.when(leaves(side, d + 1))
                def _():
                    z_copy(w, side, d + 1).start()

                if share and w != GATE:
                    y_copy(w, side, d).start()

    def relay(w, low=1, high=None):
        if high is None:
            each(n_sp - low, lambda step: relay_hop(w, step + low))
        else:
            for d in range(low, min(high, n_sp - 1) + 1):
                relay_hop(w, d)

    def complete(w):
        own[w].wait()
        if share and w != GATE:
            def one(step):
                for side in range(2):
                    @pl.when(arrives(side, step + 1))
                    def _(side=side):
                        y_copy(w, side, step + 1, True).wait_recv()

            each(n_sp - 1, one)

    offer(KEY)
    offer(GATE)
    offer(VALUE)
    load_od.start()
    load_oc.start()

    load_tok.wait()
    chunk = 64
    for at in range(0, length, chunk):
        here = tok[at:at + chunk, :].astype(F32)
        scale = lax.rsqrt(jnp.mean(here * here, axis=-1, keepdims=True) + EPSILON)
        normed[at:at + chunk, :] = (here * scale * gain[...]).astype(BF16)

    def project(w):
        return jnp.dot(normed[...], targets[w][...], preferred_element_type=F32)

    def unit_rows(tensor):
        return tensor * lax.rsqrt(jnp.sum(tensor * tensor, axis=-1, keepdims=True) + EPSILON)

    def silu(tensor):
        return tensor * jax.nn.sigmoid(tensor)

    relay(GATE)
    relay(KEY)
    offer(QUERY)
    complete(GATE)
    gate_cols = jnp.zeros((length, 4 * heads), F32)
    gate_rows = jnp.zeros((4 * heads, length), F32)
    for index in range(n_sp):
        normed_part = normed[:, index * rows:(index + 1) * rows]
        gate_cols = gate_cols + lax.dot_general(normed_part, wg[index], NT, preferred_element_type=F32)
        gate_rows = gate_rows + lax.dot_general(wg[index], normed_part, NT, preferred_element_type=F32)

    row_at = lax.broadcasted_iota(jnp.int32, (length, length), 0)
    col_at = lax.broadcasted_iota(jnp.int32, (length, length), 1)

    complete(KEY)
    key_proj = silu(project(KEY))
    pairs = [(h, r) for h in range(heads) for r in range(2)]
    for h in range(heads):
        keys[h] = unit_rows(key_proj[:, h * head_width:(h + 1) * head_width])
    relay(VALUE, 1, 1)
    for h in range(heads):
        grams = bdot(keys[h], keys[h], NT)
        for r in range(2):
            p = 2 * h + r
            decay_col = ld[:, p:p + 1] * (0.5 + jax.nn.sigmoid(gate_cols[:, 2 * p:2 * p + 1]))
            decay_row = ldt[p:p + 1, :] * (0.5 + jax.nn.sigmoid(gate_rows[2 * p:2 * p + 1, :]))
            beta = jax.nn.sigmoid(gate_cols[:, 2 * p + 1:2 * p + 2] - BETA_SHIFT)
            if r == 0:
                seen_down, seen_across = row_at <= col_at, col_at <= row_at
            else:
                seen_down, seen_across = row_at >= col_at, col_at >= row_at
            cum_row = jnp.sum(jnp.where(seen_down, decay_col, 0.0), axis=0, keepdims=True)
            cum_col = jnp.sum(jnp.where(seen_across, decay_row, 0.0), axis=1, keepdims=True)
            weighting = jnp.where(
                seen_across, jnp.exp(jnp.where(seen_across, cum_col - cum_row, 0.0)), 0.0
            )
            gaps[p] = weighting
            betas[p] = jnp.broadcast_to(beta, (length, head_width))
            cums[p] = jnp.broadcast_to(cum_col, (length, head_width))
            lower = jnp.where(row_at != col_at, grams * weighting * beta, 0.0)
            rhs[p] = lower
            near = (row_at // 2 == col_at // 2)
            xinv[p] = jnp.where(row_at == col_at, 1.0, jnp.where(near, -lower, 0.0))

    size = 2
    while size < length:
        inside = (row_at // (2 * size) == col_at // (2 * size)) & (row_at // size != col_at // size)
        for p in range(len(pairs)):
            across = jnp.where(inside, rhs[p], 0.0)
            inverse = xinv[p]
            xinv[p] = inverse - bdot(inverse, bdot(across, inverse))
        if size == 2:
            relay(VALUE, 2)
            offer(GLU)
        if size == 32:
            relay(QUERY, 1, 1)
        if size == 128:
            relay(QUERY, 2, 2)
        size *= 2

    complete(VALUE)
    value_proj = silu(project(VALUE))
    eye = (
        lax.broadcasted_iota(jnp.int32, (head_width, head_width), 0)
        == lax.broadcasted_iota(jnp.int32, (head_width, head_width), 1)
    )
    for h, r in pairs:
        p = 2 * h + r
        beta, cum, key = betas[p], cums[p], keys[h]
        value = value_proj[:, h * head_width:(h + 1) * head_width]
        total = cum[length - 1:length, :] if r == 0 else cum[0:1, :]
        right = jnp.concatenate([beta * value, beta * key * jnp.exp(cum)], axis=1)
        solved = bdot(xinv[p], right)
        vals[p] = solved.astype(BF16)
        passed = bdot(key * jnp.exp(total - cum), solved, TN)
        ends[p] = passed[:, :head_width]
        maps[p] = (jnp.where(eye, jnp.exp(total), 0.0) - passed[:, head_width:]).astype(BF16)

    def place_of(r):
        return sp if r == 0 else n_sp - 1 - sp

    def chain_copy(r):
        dest = lax.rem(sp + 1, n_sp) if r == 0 else lax.rem(sp + n_sp - 1, n_sp)
        return pltpu.make_async_remote_copy(
            src_ref=chain_out.at[r], dst_ref=chain_in.at[r],
            send_sem=chain_send.at[r], recv_sem=chain_recv.at[r],
            device_id={"sp": dest}, device_id_type=MESH,
        )

    def chain_point(low, high):
        for r in range(2):
            at = place_of(r)

            @pl.when((at >= low) & (at <= high))
            def _(r=r, at=at):
                if low == 0:
                    for h in range(heads):
                        chain_in[r, h] = jnp.zeros((head_width, head_width), BF16)
                        chain_out[r, h] = ends[2 * h + r].astype(BF16)
                else:
                    chain_copy(r).wait_recv()
                    for h in range(heads):
                        p = 2 * h + r
                        chain_out[r, h] = (bdot(maps[p], chain_in[r, h]) + ends[p]).astype(BF16)

                @pl.when(at < n_sp - 1)
                def _():
                    chain_copy(r).start()

    chain_point(0, 0)
    relay(QUERY, 3)
    offer(OPEN)
    relay(GLU, 1, 1)
    complete(QUERY)
    query_proj = silu(project(QUERY))
    for h in range(heads):
        query = unit_rows(query_proj[:, h * head_width:(h + 1) * head_width]) * head_width ** -0.5
        scores = bdot(query, keys[h], NT)
        for r in range(2):
            p = 2 * h + r
            both = jnp.dot((scores * gaps[p]).astype(BF16), vals[p], preferred_element_type=F32)
            reads[p] = (query * jnp.exp(cums[p]) - both[:, head_width:]).astype(BF16)
            if r == 0:
                local_out[h] = both[:, :head_width]
            else:
                local_out[h] = local_out[h] + both[:, :head_width]
    chain_point(1, 1)
    relay(GLU, 2, 2)
    chain_point(2, 2)
    relay(GLU, 3)
    relay(OPEN, 1, 1)
    chain_point(3, n_sp - 1)
    complete(GLU)
    glu_proj = project(GLU)
    relay(OPEN, 2)
    complete(OPEN)
    gated = (glu_proj * jax.nn.sigmoid(project(OPEN))).astype(BF16)
    glu[...] = gated
    pad[HALO:HALO + length, :] = gated.astype(F32)

    def halo_copy(r):
        start = length - HALO if r == 0 else 0
        dest = lax.rem(sp + 1, n_sp) if r == 0 else lax.rem(sp + n_sp - 1, n_sp)
        return pltpu.make_async_remote_copy(
            src_ref=glu.at[pl.ds(start, HALO)], dst_ref=halo.at[r],
            send_sem=halo_send.at[r], recv_sem=halo_recv.at[r],
            device_id={"sp": dest}, device_id_type=MESH,
        )

    for r in range(2):
        @pl.when(place_of(r) < n_sp - 1)
        def _(r=r):
            halo_copy(r).start()
    for r in range(2):
        start = 0 if r == 0 else HALO + length

        @pl.when(place_of(r) > 0)
        def _(r=r, start=start):
            halo_copy(r).wait_recv()
            pad[start:start + HALO, :] = halo[r].astype(F32)

        @pl.when(place_of(r) == 0)
        def _(start=start):
            pad[start:start + HALO, :] = jnp.zeros((HALO, channels), F32)

    taps = ck.shape[0]
    for at in range(0, length, chunk):
        first = at + HALO - taps // 2
        total = pad[first:first + chunk, :] * ck[0:1, :]
        for j in range(1, taps):
            total = total + pad[first + j:first + j + chunk, :] * ck[j:j + 1, :]
        conv[at:at + chunk, :] = total
    filtered = conv[...]
    sum_col = jnp.sum(filtered, axis=-1, keepdims=True)
    square_col = jnp.sum(filtered * filtered, axis=-1, keepdims=True)
    same = row_at == col_at
    stat_out[...] = jnp.zeros(stat_out.shape, F32)
    stat_out[0:1, :] = jnp.sum(jnp.where(same, sum_col, 0.0), axis=0, keepdims=True)
    stat_out[1:2, :] = jnp.sum(jnp.where(same, square_col, 0.0), axis=0, keepdims=True)

    def stat_copy(step):
        return pltpu.make_async_remote_copy(
            src_ref=stat_out, dst_ref=stat_in.at[step],
            send_sem=stat_send.at[step], recv_sem=stat_recv.at[step],
            device_id={"tp": lax.rem(tp + step + 1, n_tp)}, device_id_type=MESH,
        )

    for step in range(n_tp - 1):
        stat_copy(step).start()

    joined_heads = []
    for h in range(heads):
        joined = local_out[h] + jnp.dot(reads[2 * h], chain_in[0, h], preferred_element_type=F32)
        joined = joined + jnp.dot(reads[2 * h + 1], chain_in[1, h], preferred_element_type=F32)
        scale = lax.rsqrt(jnp.mean(joined * joined, axis=-1, keepdims=True) + EPSILON)
        joined_heads.append((joined * scale * hgain[...]).astype(BF16))
    delta_mix = jnp.concatenate(joined_heads, axis=1) if heads > 1 else joined_heads[0]
    load_od.wait()
    load_oc.wait()
    columns = width // n_tp
    for dest in range(n_tp):
        at = slice(dest * columns, (dest + 1) * columns)
        conv_acc[dest] = lax.dot_general(delta_mix, od[at, :], NT, preferred_element_type=F32)

    stats = stat_out[0:2, :]
    for step in range(n_tp - 1):
        stat_copy(step).wait_recv()
        stats = stats + stat_in[step, 0:2, :]
    center = jnp.sum(jnp.where(same, stats[0:1, :], 0.0), axis=1, keepdims=True) / conv_total
    squares = jnp.sum(jnp.where(same, stats[1:2, :], 0.0), axis=1, keepdims=True) / conv_total
    spread = squares - center * center
    normal = (filtered - center) * lax.rsqrt(spread + EPSILON)
    conv_mix = silu(normal * ng[...] + ns[...]).astype(BF16)

    chip, core = tp // 2, lax.rem(tp, 2)
    chips = n_tp // 2
    sibling = chip * 2 + 1 - core

    def there(p, place):
        return lax.rem(chip + p, chips) * 2 + place

    def term_of(dest):
        at = pl.ds(pl.multiple_of(dest * columns, 16), columns)
        return conv_acc[dest] + lax.dot_general(conv_mix, oc[at, :], NT, preferred_element_type=F32)

    def pair_copy(p):
        return pltpu.make_async_remote_copy(
            src_ref=pair_out.at[p], dst_ref=pair_in.at[p],
            send_sem=pair_send.at[p], recv_sem=pair_recv.at[p],
            device_id={"tp": sibling}, device_id_type=MESH,
        )

    def part_copy(p):
        return pltpu.make_async_remote_copy(
            src_ref=part_out.at[p - 1], dst_ref=part_in.at[p - 1],
            send_sem=part_send.at[p - 1], recv_sem=part_recv.at[p - 1],
            device_id={"tp": there(p, core)}, device_id_type=MESH,
        )

    slots = list(range(1, chips)) + [0]
    for p in slots:
        pair_out[p] = term_of(there(p, 1 - core)).astype(BF16)
        pair_copy(p).start()
    for p in slots:
        term = term_of(there(p, core))
        pair_copy(p).wait_recv()
        term = term + pair_in[p].astype(F32)
        if p:
            part_out[p - 1] = term.astype(BF16)
            part_copy(p).start()
        else:
            result = term
    for p in range(1, chips):
        part_copy(p).wait_recv()
        result = result + part_in[p - 1].astype(F32)
    out[...] = result.astype(BF16)

    for w in range(6):
        def one(step, w=w):
            for side in range(2):
                @pl.when(leaves(side, step + 1))
                def _(side=side):
                    z_copy(w, side, step + 1).wait_send()

                if share and w != GATE:
                    @pl.when(arrives(side, step + 1))
                    def _(side=side):
                        y_copy(w, side, step + 1).wait_send()

        each(n_sp - 1, one)
    for r in range(2):
        @pl.when(place_of(r) < n_sp - 1)
        def _(r=r):
            chain_copy(r).wait_send()
            halo_copy(r).wait_send()
    for step in range(n_tp - 1):
        stat_copy(step).wait_send()
    for p in range(chips):
        pair_copy(p).wait_send()
        if p:
            part_copy(p).wait_send()


def fused(cfg, tok_h, gain_h, wk_h, wg_h, wv_h, wq_h, wa_h, wb_h, ldt_h, hgain_h, ck_h, ng_h, ns_h, od_h, oc_h,
          out,
          gain, ldt, hgain, ck, ng, ns,
          tok, nt, wk, wv, wq, wab, wg, odg, ocg, ldo,
          keys, vals, betas, cums, xinv, gaps, rhs, local_out, reads, maps, ends,
          chain_in, chain_out, gout, gend, main_in, edge_in, pad, conv, stat_out, stat_in,
          dall, dm_out, call, acc_ab, acc_q, acc_k, acc_v,
          local_sem, g_send, g_recv, z_send, z_recv, ty_send, ty_recv, tx_recv, tf_send, tf_recv, tz_send, tz_recv,
          ld_send, ld_recv, od_send, od_recv, chain_send, chain_recv,
          main_send, main_recv, edge_send, edge_recv, far_send, rim_send,
          stat_send, stat_recv, dg_send, dg_recv, df_send, df_recv, cg_send, cg_recv, cf_send, cf_recv):
    n_sp, n_tp, conv_total = cfg
    grp, sp, tp = lax.axis_index("grp"), lax.axis_index("sp"), lax.axis_index("tp")
    length, width = tok.shape
    rows = wk_h.shape[0]
    head_width = hgain.shape[1]
    cols = wk.shape[1]
    heads = cols // head_width
    channels = wab.shape[1] // 2
    columns = out.shape[1]
    units = [(j, h) for j in range(2) for h in range(heads)]
    n_units = len(units)
    pairs = [(u, r) for u in range(n_units) for r in range(2)]
    chip, core = tp // 2, lax.rem(tp, 2)
    chips = n_tp // 2
    sibling = tp + 1 - 2 * core
    other = 1 - grp
    edge = (sp == 0) | (sp == n_sp - 1)
    inner = (sp > 0) & (sp < n_sp - 1)
    helps = (sp == 1) | (sp == n_sp - 2)
    helper = jnp.where(sp == 0, 1, n_sp - 2)
    helped = jnp.where(sp == 1, 0, n_sp - 1)
    sources = (wk_h, wg_h, wv_h, wq_h, wa_h, wb_h)
    plain = {KEY: wk, VALUE: wv, QUERY: wq}

    def remote(src, dst, send, recv, **where):
        return pltpu.make_async_remote_copy(
            src_ref=src, dst_ref=dst, send_sem=send, recv_sem=recv, device_id=where, device_id_type=MESH
        )

    counts = (4, 1, 2, 2, 2, 2)
    firsts = (0, 0, 4, 6, 8, 10)

    def source(w):
        if w == GATE:
            return wg_h
        size = channels if w in (GLU, OPEN) else cols
        return sources[w].at[:, pl.ds(pl.multiple_of(grp * size, 128), size)]

    def target(w, index, k=None):
        if w == GATE:
            return wg.at[index]
        slab = rows // counts[w]
        if k is None:
            at = pl.ds(pl.multiple_of(index * rows, 16), rows)
        else:
            at = pl.ds(pl.multiple_of(index * rows + k * slab, 16), slab)
        if w in (GLU, OPEN):
            return wab.at[at, pl.ds(channels if w == OPEN else 0, channels)]
        return plain[w].at[at]

    barrier = pltpu.get_barrier_semaphore()

    def greet(**where):
        pl.semaphore_signal(barrier, inc=1, device_id=where, device_id_type=MESH)

    for step in range(n_tp - 1):
        peer = lax.rem(tp + step + 1, n_tp)
        greet(tp=peer)
        greet(tp=peer, grp=other)
    greet(grp=other)

    @pl.when(sp > 0)
    def _():
        greet(sp=sp - 1)
        greet(sp=sp - 1, grp=other)

    @pl.when(sp < n_sp - 1)
    def _():
        greet(sp=sp + 1)
        greet(sp=sp + 1, grp=other)

    load_tok = pltpu.make_async_copy(tok_h, tok, local_sem.at[0])
    load_tok.start()
    small = [
        pltpu.make_async_copy(src, dst, local_sem.at[9 + i])
        for i, (src, dst) in enumerate(
            ((gain_h, gain), (ldt_h, ldt), (hgain_h, hgain), (ck_h, ck), (ng_h, ng), (ns_h, ns))
        )
    ]
    for copy in small:
        copy.start()
    own = [pltpu.make_async_copy(source(w), target(w, sp), local_sem.at[1 + w]) for w in range(6)]
    for copy in own:
        copy.start()

    def od_rows(index):
        return pl.ds(pl.multiple_of(index * columns, 16), columns)

    load_od = pltpu.make_async_copy(od_h.at[od_rows(tp)], odg.at[tp], local_sem.at[7])
    load_oc = pltpu.make_async_copy(oc_h.at[od_rows(tp)], ocg.at[tp], local_sem.at[8])
    load_od.start()
    load_oc.start()

    load_tok.wait()
    for copy in small:
        copy.wait()
    chunk = 64
    for at in range(0, length, chunk):
        here = tok[at:at + chunk, :].astype(F32)
        scale = lax.rsqrt(jnp.mean(here * here, axis=-1, keepdims=True) + EPSILON)
        nt[at:at + chunk, :] = (here * scale * gain[...]).astype(BF16)

    for w in (GATE, KEY):
        own[w].wait()

    @pl.when(edge)
    def _():
        pl.semaphore_wait(barrier, 2 * n_tp + 1)

    @pl.when(inner)
    def _():
        pl.semaphore_wait(barrier, 2 * n_tp + 3)

    def wide(w):
        return 1 if w in (GLU, OPEN) else 0

    def arrives(w, side, d):
        ok = (sp - d >= 0) if side == 0 else (sp + d < n_sp)
        return ok & inner if wide(w) else ok

    def leaves(w, side, d):
        if side == 0:
            return (sp - (d - 1) >= 0) & (sp < n_sp - 1 - wide(w))
        return (sp + (d - 1) < n_sp) & (sp > wide(w))

    def origin(side, d):
        return sp - d if side == 0 else sp + d

    def z_block(w, index, side, k):
        place = target(w, index, k)
        if w == GATE:
            send, recv = g_send.at[side], g_recv.at[index]
        else:
            send, recv = z_send.at[side], z_recv.at[index, firsts[w] + k]
        return remote(place, place, send, recv, sp=sp + 1 if side == 0 else sp - 1)

    def cuts(w):
        return range(counts[w])

    def offer(w, where, ks=None):
        for side in range(2):
            @pl.when(leaves(w, side, 1) & where)
            def _(side=side):
                for k in cuts(w) if ks is None else ks:
                    z_block(w, sp, side, k).start()

    def from_edge(side, d):
        return (sp - d == 0) if side == 0 else (sp + d == n_sp - 1)

    def relay(w, d, kind=None, ks=None):
        if d > n_sp - 1:
            return
        for k in cuts(w) if ks is None else ks:
            for side in range(2):
                onward = leaves(w, side, d + 1) if d < n_sp - 1 else sp < 0
                here = arrives(w, side, d) & onward
                if kind == "edge":
                    here = here & from_edge(side, d)
                if kind == "inner":
                    here = here & ~from_edge(side, d)

                @pl.when(here)
                def _(side=side, k=k):
                    z_block(w, origin(side, d), side, k).wait_recv()
                    z_block(w, origin(side, d), side, k).start()

    def drain(w, d):
        for k in cuts(w):
            for side in range(2):
                onward = leaves(w, side, d + 1) if d < n_sp - 1 else sp < 0

                @pl.when(arrives(w, side, d) & ~onward)
                def _(side=side, k=k):
                    z_block(w, origin(side, d), side, k).wait_recv()

    pieces = ty_recv.shape[0]
    half = length // 2
    piece = half // pieces
    grains = tz_recv.shape[0]
    grain = half // grains

    def part(block, side, c):
        size = grain if block > 1 else piece
        return nt.at[pl.ds(pl.multiple_of(block * length + side * half + c * size, 16), size)]

    def tok_y(k, c):
        return remote(
            part(2 * k, core, c), part(2 * k + 1, core, c), ty_send.at[k], (ty_recv, tx_recv)[k].at[c], grp=other
        )

    def tok_z(c):
        src = nt.at[pl.ds(pl.multiple_of(core * half + c * grain, 16), grain)]
        return remote(src, part(2, core, c), tz_send.at[0], tz_recv.at[c], sp=helper)

    def tok_f(block, c):
        return remote(
            part(block, core, c), part(block, core, c), tf_send.at[block - 1], tf_recv.at[block - 1], tp=sibling
        )

    def tok_f_arrival(block):
        place = nt.at[pl.ds(pl.multiple_of(block * length + (1 - core) * half, 16), half)]
        return remote(place, place, tf_send.at[block - 1], tf_recv.at[block - 1], tp=sibling)

    def half_rows(send):
        place = nt.at[pl.ds(0, half)]
        return remote(place, place, send, send, tp=sibling)

    def pass_y(k, c):
        tok_y(k, c).wait_recv()
        tok_f(2 * k + 1, c).start()

    def pass_z(c):
        @pl.when(helps)
        def _():
            tok_z(c).wait_recv()
            tok_y(1, c).start()
            tok_f(2, c).start()

    def pass_far(c):
        @pl.when(helps)
        def _():
            pass_y(1, c)

    ld_copy = remote(ldt, ldo, ld_send.at[0], ld_recv.at[0], grp=other)

    def od_copy(m, step):
        dest = lax.rem(tp + step + 1, n_tp)
        src, dst = ((od_h, odg), (oc_h, ocg))[m]
        return remote(src.at[od_rows(dest)], dst.at[tp], od_send.at[m], od_recv.at[m], tp=dest)

    def od_all(m):
        place = (odg, ocg)[m].at[pl.ds(0, n_tp - 1)]
        return remote(place, place, od_send.at[m], od_recv.at[m], tp=sibling)

    everywhere = sp >= 0
    offer(GATE, everywhere)
    offer(KEY, everywhere)
    for c in range(pieces):
        tok_y(0, c).start()
    ld_copy.start()
    for w in (VALUE, GLU, OPEN, QUERY):
        own[w].wait()
    offer(VALUE, edge)
    offer(GLU, edge)
    offer(OPEN, edge)

    @pl.when(edge)
    def _():
        for c in range(grains):
            tok_z(c).start()

    offer(QUERY, edge)
    for m in (1, 0):
        for step in range(n_tp - 1):
            od_copy(m, step).start()

    def dot(a, b, dims=NN):
        return lax.dot_general(a, b, dims, preferred_element_type=F32)

    def unit_rows(tensor):
        return tensor * lax.rsqrt(jnp.sum(tensor * tensor, axis=-1, keepdims=True) + EPSILON)

    def silu(tensor):
        return tensor * jax.nn.sigmoid(tensor)

    def block_dot(first, count, w_ref, index):
        lanes = pl.ds(pl.multiple_of(index * rows, 128), rows)
        at = pl.ds(pl.multiple_of(index * rows, 128), rows)
        return dot(nt[first * length:(first + count) * length, lanes], w_ref[at, :])

    def neighbours(w, d, action):
        for side in range(2):
            @pl.when(arrives(w, side, d))
            def _(side=side):
                action(sp - d if side == 0 else sp + d)

    def adder(acc, w_ref, first, count):
        span = slice(first * length, (first + count) * length)

        def add(index, fresh=False):
            x = block_dot(first, count, w_ref, index)
            acc[span, :] = x if fresh else acc[span, :] + x

        return add

    row_at = lax.broadcasted_iota(jnp.int32, (length, length), 0)
    col_at = lax.broadcasted_iota(jnp.int32, (length, length), 1)
    same = row_at == col_at
    mine = grp == 0
    gates = 4 * heads

    def weights_of(j):
        span = slice(j * length, (j + 1) * length)
        cols_part = jnp.zeros((length, wg.shape[1]), F32)
        for index in range(n_sp):
            cols_part = cols_part + dot(nt[span, index * rows:(index + 1) * rows], wg[index], NT)
        rows_part = jnp.transpose(cols_part)
        gate_cols = jnp.where(mine, cols_part[:, :gates], cols_part[:, gates:])
        gate_rows = jnp.where(mine, rows_part[:gates, :], rows_part[gates:, :])
        log = (ldt, ldo)[j]
        rates = jnp.where(mine, log[:2 * heads, :], log[2 * heads:, :])
        for h in range(heads):
            for r in range(2):
                p = 2 * (j * heads + h) + r
                g = 4 * h + 2 * r
                decay_row = rates[2 * h + r:2 * h + r + 1, :] * (0.5 + jax.nn.sigmoid(gate_rows[g:g + 1, :]))
                beta = jax.nn.sigmoid(gate_cols[:, g + 1:g + 2] - BETA_SHIFT)
                seen = col_at <= row_at if r == 0 else col_at >= row_at
                cum_col = jnp.sum(jnp.where(seen, decay_row, 0.0), axis=1, keepdims=True)
                cum_row = jnp.sum(jnp.where(same, cum_col, 0.0), axis=0, keepdims=True)
                gaps[p] = jnp.where(seen, jnp.exp(jnp.where(seen, cum_col - cum_row, 0.0)), 0.0)
                betas[p] = jnp.broadcast_to(beta, (length, head_width))
                cums[p] = jnp.broadcast_to(cum_col, (length, head_width))

    add_key = [adder(acc_k, wk, j, 1) for j in range(2)]
    add_value = [adder(acc_v, wv, j, 1) for j in range(2)]

    relay(GATE, 1)
    relay(KEY, 1, None, (0, 1))
    offer(VALUE, inner, (0,))
    relay(KEY, 1, None, (2, 3))
    offer(VALUE, inner, (1,))
    relay(GATE, 2)
    pass_y(0, 0)
    for d in range(2, n_sp - 1):
        relay(KEY, d, None, (0, 1))
    relay(VALUE, 1, None, (0,))
    for d in range(2, n_sp - 1):
        relay(KEY, d, None, (2, 3))
    offer(GLU, inner)
    pass_y(0, 1)
    relay(VALUE, 1, None, (1,))
    offer(OPEN, inner)
    def pass_value():
        for d in range(2, n_sp - 1):
            relay(VALUE, d)

    drain(KEY, 1)
    add_key[0](sp, True)
    neighbours(KEY, 1, add_key[0])
    pass_y(0, 2)
    offer(QUERY, inner)
    drain(VALUE, 1)
    add_value[0](sp, True)
    neighbours(VALUE, 1, add_value[0])
    relay(GLU, 1)
    for d in range(1, n_sp):
        drain(GATE, d)
    weights_of(0)
    pass_y(0, 3)
    for d in range(2, n_sp - 1):
        drain(KEY, d)
        neighbours(KEY, d, add_key[0])
    ld_copy.wait_recv()
    tok_f_arrival(1).wait_recv()
    relay(OPEN, 1)
    weights_of(1)
    pass_z(0)
    pass_value()
    add_key[1](sp, True)
    for d in range(1, n_sp - 1):
        neighbours(KEY, d, add_key[1])
    add_value[1](sp, True)
    neighbours(VALUE, 1, add_value[1])
    pass_z(1)
    drain(KEY, n_sp - 1)
    neighbours(KEY, n_sp - 1, adder(acc_k, wk, 0, 2))

    both = 2 * length
    key_proj = silu(acc_k[...])
    for u, (j, h) in enumerate(units):
        keys[u] = unit_rows(key_proj[j * length:(j + 1) * length, h * head_width:(h + 1) * head_width])
    near = row_at // 2 == col_at // 2
    for u in range(n_units):
        grams = bdot(keys[u], keys[u], NT)
        for r in range(2):
            p = 2 * u + r
            beta = jnp.concatenate([betas[p]] * (length // head_width), axis=1)
            lower = jnp.where(same, 0.0, grams * gaps[p] * beta)
            rhs[p] = lower
            xinv[p] = jnp.where(same, 1.0, jnp.where(near, -lower, 0.0))

    service = {
        4: [lambda: pass_z(2)],
        8: [lambda: pass_z(3)],
        32: [lambda: pass_z(4)],
        128: [lambda: pass_z(5)],
    }
    size = 2
    while size < length:
        inside = (row_at // (2 * size) == col_at // (2 * size)) & (row_at // size != col_at // size)
        for p in range(len(pairs)):
            across = jnp.where(inside, rhs[p], 0.0)
            inverse = xinv[p]
            xinv[p] = inverse - bdot(inverse, bdot(across, inverse))
        for act in service.get(size, ()):
            act()
        size *= 2

    for d in range(2, n_sp):
        drain(VALUE, d)
        neighbours(VALUE, d, adder(acc_v, wv, 0, 2))
    value_proj = silu(acc_v[...])
    eye = (
        lax.broadcasted_iota(jnp.int32, (head_width, head_width), 0)
        == lax.broadcasted_iota(jnp.int32, (head_width, head_width), 1)
    )
    for u, r in pairs:
        p = 2 * u + r
        j, h = units[u]
        beta, cum, key = betas[p], cums[p], keys[u]
        value = value_proj[j * length:(j + 1) * length, h * head_width:(h + 1) * head_width]
        total = cum[length - 1:length, :] if r == 0 else cum[0:1, :]
        right = jnp.concatenate([beta * value, beta * key * jnp.exp(cum)], axis=1)
        solved = bdot(xinv[p], right)
        vals[p] = solved.astype(BF16)
        passed = bdot(key * jnp.exp(total - cum), solved, TN)
        ends[p] = passed[:, :head_width]
        maps[p] = (jnp.where(eye, jnp.exp(total), 0.0) - passed[:, head_width:]).astype(BF16)

    def place_of(r):
        return sp if r == 0 else n_sp - 1 - sp

    def chain_copy(r):
        dest = sp + 1 if r == 0 else sp - 1
        return remote(chain_out.at[r], chain_in.at[r], chain_send.at[r], chain_recv.at[r], sp=dest)

    def chain_point(low, high):
        for r in range(2):
            at = place_of(r)

            @pl.when((at >= low) & (at <= high))
            def _(r=r, at=at):
                if low == 0:
                    for u in range(n_units):
                        chain_in[r, u] = jnp.zeros((head_width, head_width), BF16)
                        chain_out[r, u] = ends[2 * u + r].astype(BF16)
                else:
                    chain_copy(r).wait_recv()
                    for u in range(n_units):
                        p = 2 * u + r
                        chain_out[r, u] = (bdot(maps[p], chain_in[r, u]) + ends[p]).astype(BF16)

                @pl.when(at < n_sp - 1)
                def _():
                    chain_copy(r).start()

    chain_point(0, 0)
    pass_z(6)
    relay(QUERY, 1, "inner")
    add_near = adder(acc_ab, wab, 0, 2)
    add_query = adder(acc_q, wq, 0, 2)
    drain(GLU, 1)
    drain(OPEN, 1)

    @pl.when(inner)
    def _():
        add_near(sp, True)

    pass_z(7)
    for c in range(4):
        pass_far(c)
    neighbours(GLU, 1, add_near)
    relay(QUERY, 1, "edge", (0,))
    pass_far(4)
    chain_point(1, 1)
    relay(QUERY, 1, "edge", (1,))
    pass_far(5)
    for d in range(2, n_sp - 1):
        for w in (GLU, OPEN):
            relay(w, d)
            drain(w, d)
        neighbours(GLU, d, add_near)

    def gated(x):
        return (x[:, :channels] * jax.nn.sigmoid(x[:, channels:])).astype(BF16)

    def owner(j):
        return grp if j == 0 else other

    def main_y():
        return remote(gout, main_in.at[grp], main_send.at[0], main_recv.at[grp], grp=other)

    def main_arrival(h):
        return remote(main_in.at[h], main_in.at[h], main_send.at[0], main_recv.at[h], grp=other)

    def far_copy(j):
        return remote(gend.at[j], main_in.at[grp], far_send.at[0], main_recv.at[grp], sp=helped, grp=owner(j))

    def edge_copy(side, j):
        start = length - HALO if side == 0 else 0
        src = main_in.at[grp, pl.ds(start, HALO)] if j == 0 else gout.at[pl.ds(start, HALO)]
        return remote(
            src, edge_in.at[side, grp], edge_send.at[0], edge_recv.at[side, grp],
            sp=sp + 1 if side == 0 else sp - 1, grp=owner(j),
        )

    def rim_copy(side):
        start = length - HALO if side == 0 else 0
        return remote(
            gend.at[1, pl.ds(start, HALO)], edge_in.at[side, grp], rim_send.at[0], edge_recv.at[side, grp], grp=other
        )

    def edge_arrival(side, h):
        place = edge_in.at[side, h]
        return remote(place, place, edge_send.at[0], edge_recv.at[side, h], grp=other)

    @pl.when(inner)
    def _():
        near_rows = gated(acc_ab[...])
        main_in[grp] = near_rows[:length]
        gout[...] = near_rows[length:]
        main_y().start()
        for side in range(2):
            for j in range(2):
                edge_copy(side, j).start()

    def give_far(j):
        gend[j] = gated(dot(nt[(2 + j) * length:(3 + j) * length, :], wab[...]))
        far_copy(j).start()

    @pl.when(helps)
    def _():
        tok_f_arrival(2).wait_recv()
        give_far(0)
        for side, at in ((0, 1), (1, n_sp - 2)):
            @pl.when(sp == at)
            def _(side=side):
                start = length - HALO if side == 0 else 0
                edge_in[side, grp] = gend[0, start:start + HALO, :]

    pass_far(6)
    pass_far(7)

    @pl.when(helps)
    def _():
        tok_f_arrival(3).wait_recv()
        give_far(1)
        for side, at in ((0, 1), (1, n_sp - 2)):
            @pl.when(sp == at)
            def _(side=side):
                rim_copy(side).start()

    for d in range(2, n_sp - 1):
        chain_point(d, d)
        relay(QUERY, d)
    drain(QUERY, 1)
    add_query(sp, True)
    neighbours(QUERY, 1, add_query)
    for d in range(2, n_sp - 1):
        drain(QUERY, d)
        neighbours(QUERY, d, add_query)

    for h in range(2):
        @pl.when(~(inner & (grp == h)))
        def _(h=h):
            main_arrival(h).wait_recv()

        @pl.when((sp > 0) & ~((sp == 1) & (grp == h)))
        def _(h=h):
            edge_arrival(0, h).wait_recv()

        @pl.when((sp < n_sp - 1) & ~((sp == n_sp - 2) & (grp == h)))
        def _(h=h):
            edge_arrival(1, h).wait_recv()

        pad[h, HALO:HALO + length, :] = main_in[h].astype(F32)
        for side, start, none in ((0, 0, 0), (1, HALO + length, n_sp - 1)):
            @pl.when(sp != none)
            def _(h=h, side=side, start=start):
                pad[h, start:start + HALO, :] = edge_in[side, h].astype(F32)

            @pl.when(sp == none)
            def _(h=h, start=start):
                pad[h, start:start + HALO, :] = jnp.zeros((HALO, channels), F32)

    taps = ck.shape[0]
    for h in range(2):
        lanes = slice(h * channels, (h + 1) * channels)
        for at in range(0, length, chunk):
            first = at + HALO - taps // 2
            total = pad[h, first:first + chunk, :] * ck[0:1, lanes]
            for k in range(1, taps):
                total = total + pad[h, first + k:first + k + chunk, :] * ck[k:k + 1, lanes]
            conv[at:at + chunk, lanes] = total
    filtered = conv[...]
    sum_col = jnp.sum(filtered, axis=-1, keepdims=True)
    square_col = jnp.sum(filtered * filtered, axis=-1, keepdims=True)
    stat_out[...] = jnp.zeros(stat_out.shape, F32)
    stat_out[0:1, :] = jnp.sum(jnp.where(same, sum_col, 0.0), axis=0, keepdims=True)
    stat_out[1:2, :] = jnp.sum(jnp.where(same, square_col, 0.0), axis=0, keepdims=True)

    def stat_copy(step):
        return remote(
            stat_out, stat_in.at[step], stat_send.at[0], stat_recv.at[0], tp=lax.rem(tp + step + 1, n_tp)
        )

    for step in range(n_tp - 1):
        stat_copy(step).start()

    def chip_at(q):
        return lax.rem(chip + q, chips)

    def chip_back(q):
        return lax.rem(chip + chips - q, chips)

    def dg_copy(a, q):
        src = dall.at[tp, grp] if a == 0 else dm_out
        where = {"tp": chip_at(q) * 2 + core}
        if a:
            where["grp"] = other
        return remote(src, dall.at[tp, grp], dg_send.at[a], dg_recv.at[a, q], **where)

    def d_block(a, q, side):
        return dall.at[chip_back(q) * 2 + side, other if a else grp]

    def dg_arrival(a, q):
        place = d_block(a, q, core)
        return remote(place, place, dg_send.at[a], dg_recv.at[a, q], tp=sibling)

    def df_copy(a, q):
        place = d_block(a, q, core)
        return remote(place, place, df_send.at[0], df_recv.at[q], tp=sibling)

    def df_arrival(q):
        place = dall.at[chip_back(q) * 2 + 1 - core]
        return remote(place, place, df_send.at[0], df_recv.at[q], tp=sibling)

    def cg_copy(q):
        return remote(call.at[tp], call.at[tp], cg_send.at[0], cg_recv.at[q], tp=chip_at(q) * 2 + core)

    def cg_arrival(q):
        place = call.at[chip_back(q) * 2 + core]
        return remote(place, place, cg_send.at[0], cg_recv.at[q], tp=sibling)

    def cf_copy(q, arriving=False):
        place = call.at[chip_back(q) * 2 + (1 - core if arriving else core)]
        return remote(place, place, cf_send.at[0], cf_recv.at[q], tp=sibling)

    chain_point(n_sp - 1, n_sp - 1)
    stats = stat_out[0:2, :]
    stat_all = remote(stat_in, stat_in, stat_send.at[0], stat_recv.at[0], tp=sibling)
    stat_all.wait_recv()
    for step in range(n_tp - 1):
        stats = stats + stat_in[step, 0:2, :]
    center = jnp.sum(jnp.where(same, stats[0:1, :], 0.0), axis=1, keepdims=True) / conv_total
    squares = jnp.sum(jnp.where(same, stats[1:2, :], 0.0), axis=1, keepdims=True) / conv_total
    spread = squares - center * center
    normal = (conv[...] - center) * lax.rsqrt(spread + EPSILON)
    call[tp] = silu(normal * ng[...] + ns[...]).astype(BF16)
    for q in range(1, chips):
        cg_copy(q).start()
    cf_copy(0).start()

    def delta_term(t):
        return dot(jnp.concatenate([dall[t, 0], dall[t, 1]], axis=1), odg[t], NT)

    def conv_term(t):
        return dot(call[t], ocg[t], NT)

    drain(QUERY, n_sp - 1)
    neighbours(QUERY, n_sp - 1, add_query)

    def read(u):
        j, h = units[u]
        query = silu(acc_q[j * length:(j + 1) * length, h * head_width:(h + 1) * head_width])
        query = unit_rows(query) * head_width ** -0.5
        scores = bdot(query, keys[u], NT)
        for r in range(2):
            p = 2 * u + r
            pair = dot((scores * gaps[p]).astype(BF16), vals[p])
            reads[p] = (query * jnp.exp(cums[p]) - pair[:, head_width:]).astype(BF16)
            if r == 0:
                local_out[u] = pair[:, :head_width]
            else:
                local_out[u] = local_out[u] + pair[:, :head_width]

    def mixed_head(u):
        joined = local_out[u] + dot(reads[2 * u], chain_in[0, u]) + dot(reads[2 * u + 1], chain_in[1, u])
        scale = lax.rsqrt(jnp.mean(joined * joined, axis=-1, keepdims=True) + EPSILON)
        return (joined * scale * hgain[...]).astype(BF16)

    direct = [(a, q) for q in range(chips) for a in (1, 0) if (a, q) != (0, 0)]

    for h in range(heads):
        read(heads + h)
        dm_out[:, h * head_width:(h + 1) * head_width] = mixed_head(heads + h)
    for q in range(chips - 1, -1, -1):
        dg_copy(1, q).start()
    for h in range(heads):
        read(h)
        dall[tp, grp, :, h * head_width:(h + 1) * head_width] = mixed_head(h)
    for q in range(1, chips):
        dg_copy(0, q).start()
    df_copy(0, 0).start()

    for m in range(2):
        od_all(m).wait_recv()
    load_od.wait()
    load_oc.wait()
    result = conv_term(tp)
    for q in range(1, chips):
        cg_arrival(q).wait_recv()
        cf_copy(q).start()
    for q in range(1, chips):
        result = result + conv_term(chip_back(q) * 2 + core)
    for a, q in direct:
        dg_arrival(a, q).wait_recv()
        df_copy(a, q).start()
        if (a, q) == (1, 0):
            for p in range(chips):
                cf_copy(p, True).wait_recv()
                result = result + conv_term(chip_back(p) * 2 + 1 - core)
            result = result + delta_term(tp)
    for q in range(1, chips):
        result = result + delta_term(chip_back(q) * 2 + core)
    for q in range(chips):
        df_arrival(q).wait_recv()
        result = result + delta_term(chip_back(q) * 2 + 1 - core)
    out[...] = result.astype(BF16)

    for side in range(2):
        for q in range(n_sp):
            far = n_sp - 1 if side == 0 else 0
            copies = 0 if q == far else (q + 1 if side == 0 else n_sp - q)
            wide_to = n_sp - 2 if side == 0 else 1
            wide_copies = copies if (q < wide_to if side == 0 else q > wide_to) else 0
            if copies:
                @pl.when(sp == q)
                def _(side=side, copies=copies, wide_copies=wide_copies):
                    place = wg.at[pl.ds(0, copies)]
                    remote(place, place, g_send.at[side], g_send.at[side], tp=sibling).wait_send()
                    total = (3 * cols * copies + 2 * channels * wide_copies) * rows // width
                    place = nt.at[pl.ds(0, total)]
                    remote(place, place, z_send.at[side], z_send.at[side], tp=sibling).wait_send()
    half_rows(ty_send.at[0]).wait_send()
    half_rows(tf_send.at[0]).wait_send()

    @pl.when(edge)
    def _():
        half_rows(tz_send.at[0]).wait_send()

    @pl.when(helps)
    def _():
        half_rows(ty_send.at[1]).wait_send()
        half_rows(tf_send.at[1]).wait_send()
        half_rows(tf_send.at[2]).wait_send()
        remote(gend, gend, far_send.at[0], far_send.at[0], tp=sibling).wait_send()
        rim_copy(0).wait_send()

    ld_copy.wait_send()
    for m in range(2):
        od_all(m).wait_send()
    for r in range(2):
        @pl.when(place_of(r) < n_sp - 1)
        def _(r=r):
            chain_copy(r).wait_send()

    @pl.when(inner)
    def _():
        main_y().wait_send()
        remote(edge_in, edge_in, edge_send.at[0], edge_send.at[0], tp=sibling).wait_send()

    stat_all.wait_send()
    place = dall.at[pl.ds(0, chips), 0]
    remote(place, place, dg_send.at[1], dg_send.at[1], tp=sibling).wait_send()
    if chips > 1:
        place = dall.at[pl.ds(0, chips - 1), 0]
        remote(place, place, dg_send.at[0], dg_send.at[0], tp=sibling).wait_send()
        place = call.at[pl.ds(0, chips - 1)]
        remote(place, place, cg_send.at[0], cg_send.at[0], tp=sibling).wait_send()
    place = dall.at[pl.ds(0, chips)]
    remote(place, place, df_send.at[0], df_send.at[0], tp=sibling).wait_send()
    place = call.at[pl.ds(0, chips)]
    remote(place, place, cf_send.at[0], cf_send.at[0], tp=sibling).wait_send()


def solution(mesh):
    n_grp, n_sp, n_tp = mesh.shape["grp"], mesh.shape["sp"], mesh.shape["tp"]

    def on_device(tokens_in, input_gain, w_query, w_key, w_value, w_gates, w_glu_value,
                  sigmoid_opener_matrix, log_decay, head_gain, conv_kernel, norm_gain, norm_shift,
                  out_delta, out_conv):
        length, width = tokens_in.shape
        head_width = head_gain.shape[0]
        head_cols = w_query.shape[1]
        heads = head_cols // head_width
        channels = w_glu_value.shape[1]
        rows = w_query.shape[0]
        pairs = 2 * heads
        columns = width // n_tp
        dma, vmem = pltpu.SemaphoreType.DMA, pltpu.VMEM
        anywhere = pl.BlockSpec(memory_space=pltpu.HBM)
        inside = pl.BlockSpec(memory_space=pltpu.VMEM)
        if n_grp == 2 and n_sp >= 4 and n_tp % 2 == 0 and heads % 2 == 0 and channels % 256 == 0                 and (3 * head_cols + 2 * channels) * rows * n_sp <= 8 * length * width:
            cols, ch, chips, steps = head_cols // 2, channels // 2, n_tp // 2, n_tp - 1
            pieces = 4
            scratch = [
                vmem((1, width), F32), vmem((pairs, length), F32), vmem((1, head_width), F32),
                vmem(conv_kernel.shape, F32), vmem((1, channels), F32), vmem((1, channels), F32),
                vmem((length, width), BF16), vmem((4 * length, width), BF16),
                vmem((width, cols), BF16), vmem((width, cols), BF16), vmem((width, cols), BF16),
                vmem((width, 2 * ch), BF16), vmem((n_sp, 4 * heads, rows), BF16),
                vmem((n_tp, columns, head_cols), BF16), vmem((n_tp, columns, channels), BF16),
                vmem((pairs, length), F32),
                vmem((heads, length, head_width), F32), vmem((pairs, length, 2 * head_width), BF16),
                vmem((pairs, length, head_width), F32), vmem((pairs, length, head_width), F32),
                vmem((pairs, length, length), F32), vmem((pairs, length, length), F32),
                vmem((pairs, length, length), F32),
                vmem((heads, length, head_width), F32), vmem((pairs, length, head_width), BF16),
                vmem((pairs, head_width, head_width), BF16), vmem((pairs, head_width, head_width), F32),
                vmem((2, heads, head_width, head_width), BF16), vmem((2, heads, head_width, head_width), BF16),
                vmem((length, ch), BF16), vmem((2, length, ch), BF16), vmem((2, length, ch), BF16),
                vmem((2, 2, HALO, ch), BF16),
                vmem((2, length + 2 * HALO, ch), F32), vmem((length, channels), F32),
                vmem((8, length), F32), vmem((steps, 8, length), F32),
                vmem((n_tp, 2, length, cols), BF16), vmem((length, cols), BF16),
                vmem((n_tp, length, channels), BF16), vmem((2 * length, 2 * ch), F32), vmem((2 * length, cols), F32),
                vmem((2 * length, cols), F32), vmem((2 * length, cols), F32),
                dma((15,)),
                dma((2,)), dma((n_sp,)), dma((2,)), dma((n_sp, 12)),
                dma((2,)), dma((pieces,)), dma((2 * pieces,)), dma((3,)), dma((3,)),
                dma((1,)), dma((2 * pieces,)),
                dma((1,)), dma((1,)), dma((2,)), dma((2,)), dma((2,)), dma((2,)),
                dma((1,)), dma((2,)), dma((1,)), dma((2, 2)), dma((1,)), dma((1,)),
                dma((1,)), dma((1,)),
                dma((2,)), dma((2, chips)), dma((1,)), dma((chips,)),
                dma((1,)), dma((chips,)), dma((1,)), dma((chips,)),
            ]
            return pl.pallas_call(
                functools.partial(fused, (n_sp, n_tp, float(channels * n_tp))),
                out_shape=pltpu.VMEM((length, columns), BF16),
                in_specs=[anywhere] * 15,
                out_specs=inside,
                scratch_shapes=scratch,
                compiler_params=pltpu.CompilerParams(
                    collective_id=0, has_side_effects=True, vmem_limit_bytes=58 * 1024 * 1024
                ),
            )(
                tokens_in, input_gain.reshape(1, width), w_key, w_gates.T, w_value, w_query,
                w_glu_value, sigmoid_opener_matrix, log_decay.T,
                head_gain.reshape(1, head_width), conv_kernel, norm_gain.reshape(1, channels),
                norm_shift.reshape(1, channels), out_delta, out_conv,
            )
        scratch = [
            vmem((length, width), BF16), vmem((length, width), BF16),
            vmem((width, head_cols), BF16), vmem((n_sp, 4 * heads, rows), BF16),
            vmem((width, head_cols), BF16), vmem((width, head_cols), BF16),
            vmem((width, channels), BF16), vmem((width, channels), BF16),
            vmem((width, head_cols), BF16), vmem((width, channels), BF16),
            vmem((heads, length, head_width), F32), vmem((pairs, length, 2 * head_width), BF16),
            vmem((pairs, length, head_width), F32), vmem((pairs, length, head_width), F32),
            vmem((pairs, length, length), F32), vmem((pairs, length, length), F32),
            vmem((pairs, length, length), F32),
            vmem((heads, length, head_width), F32), vmem((pairs, length, head_width), BF16),
            vmem((pairs, head_width, head_width), BF16), vmem((pairs, head_width, head_width), F32),
            vmem((2, heads, head_width, head_width), BF16), vmem((2, heads, head_width, head_width), BF16),
            vmem((length, channels), BF16), vmem((2, HALO, channels), BF16),
            vmem((length + 2 * HALO, channels), F32), vmem((length, channels), F32),
            vmem((8, length), F32), vmem((n_tp - 1, 8, length), F32),
            vmem((n_tp, length, columns), F32),
            vmem((n_tp // 2, length, columns), BF16), vmem((n_tp // 2, length, columns), BF16),
            vmem((n_tp // 2, length, columns), BF16), vmem((n_tp // 2, length, columns), BF16),
            dma((9,)),
            dma((6, 2, n_sp - 1)), dma((6, 2, n_sp - 1)),
            dma((6, 2, n_sp - 1)), dma((6, 2, n_sp - 1)),
            dma((2,)), dma((2,)), dma((2,)), dma((2,)),
            dma((n_tp - 1,)), dma((n_tp - 1,)), dma((n_tp // 2,)), dma((n_tp // 2,)),
            dma((n_tp // 2,)), dma((n_tp // 2,)),
        ]
        return pl.pallas_call(
            functools.partial(kernel, (n_grp, n_sp, n_tp, float(channels * n_tp))),
            out_shape=jax.ShapeDtypeStruct((length, columns), BF16),
            in_specs=[anywhere, inside] + [anywhere] * 6 + [inside] * 6 + [anywhere] * 2,
            out_specs=inside,
            scratch_shapes=scratch,
            compiler_params=pltpu.CompilerParams(
                collective_id=0, has_side_effects=True, vmem_limit_bytes=60 * 1024 * 1024
            ),
        )(
            tokens_in, input_gain.reshape(1, width), w_key, w_gates.T, w_value, w_query,
            w_glu_value, sigmoid_opener_matrix, log_decay, log_decay.T,
            head_gain.reshape(1, head_width), conv_kernel, norm_gain.reshape(1, channels),
            norm_shift.reshape(1, channels), out_delta, out_conv,
        )

    placed = (
        P(("grp", "sp"), None), P(), P("sp", "tp"), P("sp", "tp"), P("sp", "tp"), P("sp", "tp"),
        P("sp", "tp"), P("sp", "tp"), P(("grp", "sp"), "tp"), P(), P(None, "tp"), P("tp"), P("tp"),
        P(None, "tp"), P(None, "tp"),
    )
    return jax.shard_map(
        on_device, mesh=mesh, in_specs=placed, out_specs=P(("grp", "sp"), "tp"), check_vma=False
    )
```

```python
import functools

import jax
import jax.numpy as jnp
from jax import lax
from jax.experimental import pallas as pl
from jax.experimental.pallas import tpu as pltpu
from jax.sharding import PartitionSpec as P

EPSILON = 1e-06
BETA_SHIFT = 6.0
HALO = 16
MESH = pl.DeviceIdType.MESH
F32 = jnp.float32
BF16 = jnp.bfloat16
NT = (((1,), (1,)), ((), ()))
TN = (((0,), (0,)), ((), ()))
NN = (((1,), (0,)), ((), ()))
KEY, GATE, VALUE, QUERY, GLU, OPEN = range(6)


def bdot(left, right, dims=NN):
    return lax.dot_general(
        left.astype(BF16), right.astype(BF16), dims, preferred_element_type=F32
    )


def each(count, action):
    if count <= 8:
        for step in range(count):
            action(step)
    else:
        def body(step, carry):
            action(step)
            return carry

        lax.fori_loop(0, count, body, 0)


def kernel(cfg, tok_h, gain, wk_h, wg_h, wv_h, wq_h, wa_h, wb_h, ld, ldt, hgain, ck, ng, ns, od_h, oc_h,
           out,
           tok, normed, wk, wg, wv, wq, wa, wb, od, oc,
           keys, vals, betas, cums, xinv, gaps, rhs, local_out, reads, maps, ends,
           chain_in, chain_out, glu, halo, pad, conv, stat_out, stat_in, conv_acc, part_out, part_in, pair_out, pair_in,
           local_sem, z_send, z_recv, y_send, y_recv, chain_send, chain_recv,
           halo_send, halo_recv, stat_send, stat_recv, part_send, part_recv, pair_send, pair_recv):
    n_grp, n_sp, n_tp, conv_total = cfg
    grp, sp, tp = lax.axis_index("grp"), lax.axis_index("sp"), lax.axis_index("tp")
    length, width = tok.shape
    rows = wk_h.shape[0]
    channels = wa.shape[1]
    head_width = hgain.shape[1]
    heads = wk.shape[1] // head_width
    share = (rows // 2) // 16 * 16 if n_grp == 2 else 0
    pulled = rows - share

    sources = (wk_h, wg_h, wv_h, wq_h, wa_h, wb_h)
    targets = (wk, wg, wv, wq, wa, wb)

    def block_of(w, index, start, count):
        if w == GATE:
            return targets[w].at[index]
        return targets[w].at[pl.ds(pl.multiple_of(index * rows + start, 16), count)]

    load_tok = pltpu.make_async_copy(tok_h, tok, local_sem.at[0])
    load_tok.start()
    own = [
        pltpu.make_async_copy(sources[w], block_of(w, sp, 0, rows), local_sem.at[1 + w])
        for w in range(6)
    ]
    for copy in own:
        copy.start()
    load_od = pltpu.make_async_copy(od_h, od, local_sem.at[7])
    load_oc = pltpu.make_async_copy(oc_h, oc, local_sem.at[8])

    barrier = pltpu.get_barrier_semaphore()

    def greet(axis, me, count):
        def one(step):
            pl.semaphore_signal(
                barrier, inc=1, device_id={axis: lax.rem(me + step + 1, count)}, device_id_type=MESH
            )

        each(count - 1, one)

    greet("sp", sp, n_sp)
    greet("tp", tp, n_tp)
    greet("grp", grp, n_grp)
    pl.semaphore_wait(barrier, n_sp + n_tp + n_grp - 3)

    def origin(side, d):
        return sp - d if side == 0 else sp + d

    def arrives(side, d):
        return sp - d >= 0 if side == 0 else sp + d < n_sp

    def leaves(side, d):
        if side == 0:
            return (sp - (d - 1) >= 0) & (sp < n_sp - 1)
        return (sp + (d - 1) < n_sp) & (sp > 0)

    def part_of(w, index, side_of):
        if w == GATE:
            return block_of(w, index, 0, 0)
        if not share:
            return block_of(w, index, 0, rows)
        if side_of is None:
            return block_of(w, index, pl.multiple_of(grp * share, 16), pulled)
        return block_of(w, index, pl.multiple_of(side_of * pulled, 16), share)

    def z_copy(w, side, d, first=False):
        target = part_of(w, origin(side, d - 1), None)
        source = target
        if first:
            source = sources[w]
            if w != GATE and share:
                source = source.at[pl.ds(pl.multiple_of(grp * share, 16), pulled)]
        return pltpu.make_async_remote_copy(
            src_ref=source, dst_ref=target,
            send_sem=z_send.at[w, side, d - 1], recv_sem=z_recv.at[w, side, d - 1],
            device_id={"sp": sp + 1 if side == 0 else sp - 1}, device_id_type=MESH,
        )

    def z_arrival(w, side, d):
        place = part_of(w, origin(side, d), None)
        return pltpu.make_async_remote_copy(
            src_ref=place, dst_ref=place,
            send_sem=z_send.at[w, side, d - 1], recv_sem=z_recv.at[w, side, d - 1],
            device_id={"sp": sp + 1 if side == 0 else sp - 1}, device_id_type=MESH,
        )

    def y_copy(w, side, d, arriving=False):
        place = part_of(w, origin(side, d), 1 - grp if arriving else grp)
        return pltpu.make_async_remote_copy(
            src_ref=place, dst_ref=place,
            send_sem=y_send.at[w, side, d - 1], recv_sem=y_recv.at[w, side, d - 1],
            device_id={"grp": 1 - grp}, device_id_type=MESH,
        )

    def offer(w):
        for side in range(2):
            @pl.when(leaves(side, 1))
            def _(side=side):
                z_copy(w, side, 1, True).start()

    def relay_hop(w, d):
        for side in range(2):
            @pl.when(arrives(side, d))
            def _(side=side):
                z_arrival(w, side, d).wait_recv()

                @pl.when(leaves(side, d + 1))
                def _():
                    z_copy(w, side, d + 1).start()

                if share and w != GATE:
                    y_copy(w, side, d).start()

    def relay(w, low=1, high=None):
        if high is None:
            each(n_sp - low, lambda step: relay_hop(w, step + low))
        else:
            for d in range(low, min(high, n_sp - 1) + 1):
                relay_hop(w, d)

    def complete(w):
        own[w].wait()
        if share and w != GATE:
            def one(step):
                for side in range(2):
                    @pl.when(arrives(side, step + 1))
                    def _(side=side):
                        y_copy(w, side, step + 1, True).wait_recv()

            each(n_sp - 1, one)

    offer(KEY)
    offer(GATE)
    offer(VALUE)
    load_od.start()
    load_oc.start()

    load_tok.wait()
    chunk = 64
    for at in range(0, length, chunk):
        here = tok[at:at + chunk, :].astype(F32)
        scale = lax.rsqrt(jnp.mean(here * here, axis=-1, keepdims=True) + EPSILON)
        normed[at:at + chunk, :] = (here * scale * gain[...]).astype(BF16)

    def project(w):
        return jnp.dot(normed[...], targets[w][...], preferred_element_type=F32)

    def unit_rows(tensor):
        return tensor * lax.rsqrt(jnp.sum(tensor * tensor, axis=-1, keepdims=True) + EPSILON)

    def silu(tensor):
        return tensor * jax.nn.sigmoid(tensor)

    relay(GATE)
    relay(KEY)
    offer(QUERY)
    complete(GATE)
    gate_cols = jnp.zeros((length, 4 * heads), F32)
    gate_rows = jnp.zeros((4 * heads, length), F32)
    for index in range(n_sp):
        normed_part = normed[:, index * rows:(index + 1) * rows]
        gate_cols = gate_cols + lax.dot_general(normed_part, wg[index], NT, preferred_element_type=F32)
        gate_rows = gate_rows + lax.dot_general(wg[index], normed_part, NT, preferred_element_type=F32)

    row_at = lax.broadcasted_iota(jnp.int32, (length, length), 0)
    col_at = lax.broadcasted_iota(jnp.int32, (length, length), 1)

    complete(KEY)
    key_proj = silu(project(KEY))
    pairs = [(h, r) for h in range(heads) for r in range(2)]
    for h in range(heads):
        keys[h] = unit_rows(key_proj[:, h * head_width:(h + 1) * head_width])
    relay(VALUE, 1, 1)
    for h in range(heads):
        grams = bdot(keys[h], keys[h], NT)
        for r in range(2):
            p = 2 * h + r
            decay_col = ld[:, p:p + 1] * (0.5 + jax.nn.sigmoid(gate_cols[:, 2 * p:2 * p + 1]))
            decay_row = ldt[p:p + 1, :] * (0.5 + jax.nn.sigmoid(gate_rows[2 * p:2 * p + 1, :]))
            beta = jax.nn.sigmoid(gate_cols[:, 2 * p + 1:2 * p + 2] - BETA_SHIFT)
            if r == 0:
                seen_down, seen_across = row_at <= col_at, col_at <= row_at
            else:
                seen_down, seen_across = row_at >= col_at, col_at >= row_at
            cum_row = jnp.sum(jnp.where(seen_down, decay_col, 0.0), axis=0, keepdims=True)
            cum_col = jnp.sum(jnp.where(seen_across, decay_row, 0.0), axis=1, keepdims=True)
            weighting = jnp.where(
                seen_across, jnp.exp(jnp.where(seen_across, cum_col - cum_row, 0.0)), 0.0
            )
            gaps[p] = weighting
            betas[p] = jnp.broadcast_to(beta, (length, head_width))
            cums[p] = jnp.broadcast_to(cum_col, (length, head_width))
            lower = jnp.where(row_at != col_at, grams * weighting * beta, 0.0)
            rhs[p] = lower
            near = (row_at // 2 == col_at // 2)
            xinv[p] = jnp.where(row_at == col_at, 1.0, jnp.where(near, -lower, 0.0))

    size = 2
    while size < length:
        inside = (row_at // (2 * size) == col_at // (2 * size)) & (row_at // size != col_at // size)
        for p in range(len(pairs)):
            across = jnp.where(inside, rhs[p], 0.0)
            inverse = xinv[p]
            xinv[p] = inverse - bdot(inverse, bdot(across, inverse))
        if size == 2:
            relay(VALUE, 2)
            offer(GLU)
        if size == 32:
            relay(QUERY, 1, 1)
        if size == 128:
            relay(QUERY, 2, 2)
        size *= 2

    complete(VALUE)
    value_proj = silu(project(VALUE))
    eye = (
        lax.broadcasted_iota(jnp.int32, (head_width, head_width), 0)
        == lax.broadcasted_iota(jnp.int32, (head_width, head_width), 1)
    )
    for h, r in pairs:
        p = 2 * h + r
        beta, cum, key = betas[p], cums[p], keys[h]
        value = value_proj[:, h * head_width:(h + 1) * head_width]
        total = cum[length - 1:length, :] if r == 0 else cum[0:1, :]
        right = jnp.concatenate([beta * value, beta * key * jnp.exp(cum)], axis=1)
        solved = bdot(xinv[p], right)
        vals[p] = solved.astype(BF16)
        passed = bdot(key * jnp.exp(total - cum), solved, TN)
        ends[p] = passed[:, :head_width]
        maps[p] = (jnp.where(eye, jnp.exp(total), 0.0) - passed[:, head_width:]).astype(BF16)

    def place_of(r):
        return sp if r == 0 else n_sp - 1 - sp

    def chain_copy(r):
        dest = lax.rem(sp + 1, n_sp) if r == 0 else lax.rem(sp + n_sp - 1, n_sp)
        return pltpu.make_async_remote_copy(
            src_ref=chain_out.at[r], dst_ref=chain_in.at[r],
            send_sem=chain_send.at[r], recv_sem=chain_recv.at[r],
            device_id={"sp": dest}, device_id_type=MESH,
        )

    def chain_point(low, high):
        for r in range(2):
            at = place_of(r)

            @pl.when((at >= low) & (at <= high))
            def _(r=r, at=at):
                if low == 0:
                    for h in range(heads):
                        chain_in[r, h] = jnp.zeros((head_width, head_width), BF16)
                        chain_out[r, h] = ends[2 * h + r].astype(BF16)
                else:
                    chain_copy(r).wait_recv()
                    for h in range(heads):
                        p = 2 * h + r
                        chain_out[r, h] = (bdot(maps[p], chain_in[r, h]) + ends[p]).astype(BF16)

                @pl.when(at < n_sp - 1)
                def _():
                    chain_copy(r).start()

    chain_point(0, 0)
    relay(QUERY, 3)
    offer(OPEN)
    relay(GLU, 1, 1)
    complete(QUERY)
    query_proj = silu(project(QUERY))
    for h in range(heads):
        query = unit_rows(query_proj[:, h * head_width:(h + 1) * head_width]) * head_width ** -0.5
        scores = bdot(query, keys[h], NT)
        for r in range(2):
            p = 2 * h + r
            both = jnp.dot((scores * gaps[p]).astype(BF16), vals[p], preferred_element_type=F32)
            reads[p] = (query * jnp.exp(cums[p]) - both[:, head_width:]).astype(BF16)
            if r == 0:
                local_out[h] = both[:, :head_width]
            else:
                local_out[h] = local_out[h] + both[:, :head_width]
    chain_point(1, 1)
    relay(GLU, 2, 2)
    chain_point(2, 2)
    relay(GLU, 3)
    relay(OPEN, 1, 1)
    chain_point(3, n_sp - 1)
    complete(GLU)
    glu_proj = project(GLU)
    relay(OPEN, 2)
    complete(OPEN)
    gated = (glu_proj * jax.nn.sigmoid(project(OPEN))).astype(BF16)
    glu[...] = gated
    pad[HALO:HALO + length, :] = gated.astype(F32)

    def halo_copy(r):
        start = length - HALO if r == 0 else 0
        dest = lax.rem(sp + 1, n_sp) if r == 0 else lax.rem(sp + n_sp - 1, n_sp)
        return pltpu.make_async_remote_copy(
            src_ref=glu.at[pl.ds(start, HALO)], dst_ref=halo.at[r],
            send_sem=halo_send.at[r], recv_sem=halo_recv.at[r],
            device_id={"sp": dest}, device_id_type=MESH,
        )

    for r in range(2):
        @pl.when(place_of(r) < n_sp - 1)
        def _(r=r):
            halo_copy(r).start()
    for r in range(2):
        start = 0 if r == 0 else HALO + length

        @pl.when(place_of(r) > 0)
        def _(r=r, start=start):
            halo_copy(r).wait_recv()
            pad[start:start + HALO, :] = halo[r].astype(F32)

        @pl.when(place_of(r) == 0)
        def _(start=start):
            pad[start:start + HALO, :] = jnp.zeros((HALO, channels), F32)

    taps = ck.shape[0]
    for at in range(0, length, chunk):
        first = at + HALO - taps // 2
        total = pad[first:first + chunk, :] * ck[0:1, :]
        for j in range(1, taps):
            total = total + pad[first + j:first + j + chunk, :] * ck[j:j + 1, :]
        conv[at:at + chunk, :] = total
    filtered = conv[...]
    sum_col = jnp.sum(filtered, axis=-1, keepdims=True)
    square_col = jnp.sum(filtered * filtered, axis=-1, keepdims=True)
    same = row_at == col_at
    stat_out[...] = jnp.zeros(stat_out.shape, F32)
    stat_out[0:1, :] = jnp.sum(jnp.where(same, sum_col, 0.0), axis=0, keepdims=True)
    stat_out[1:2, :] = jnp.sum(jnp.where(same, square_col, 0.0), axis=0, keepdims=True)

    def stat_copy(step):
        return pltpu.make_async_remote_copy(
            src_ref=stat_out, dst_ref=stat_in.at[step],
            send_sem=stat_send.at[step], recv_sem=stat_recv.at[step],
            device_id={"tp": lax.rem(tp + step + 1, n_tp)}, device_id_type=MESH,
        )

    for step in range(n_tp - 1):
        stat_copy(step).start()

    joined_heads = []
    for h in range(heads):
        joined = local_out[h] + jnp.dot(reads[2 * h], chain_in[0, h], preferred_element_type=F32)
        joined = joined + jnp.dot(reads[2 * h + 1], chain_in[1, h], preferred_element_type=F32)
        scale = lax.rsqrt(jnp.mean(joined * joined, axis=-1, keepdims=True) + EPSILON)
        joined_heads.append((joined * scale * hgain[...]).astype(BF16))
    delta_mix = jnp.concatenate(joined_heads, axis=1) if heads > 1 else joined_heads[0]
    load_od.wait()
    load_oc.wait()
    columns = width // n_tp
    for dest in range(n_tp):
        at = slice(dest * columns, (dest + 1) * columns)
        conv_acc[dest] = lax.dot_general(delta_mix, od[at, :], NT, preferred_element_type=F32)

    stats = stat_out[0:2, :]
    for step in range(n_tp - 1):
        stat_copy(step).wait_recv()
        stats = stats + stat_in[step, 0:2, :]
    center = jnp.sum(jnp.where(same, stats[0:1, :], 0.0), axis=1, keepdims=True) / conv_total
    squares = jnp.sum(jnp.where(same, stats[1:2, :], 0.0), axis=1, keepdims=True) / conv_total
    spread = squares - center * center
    normal = (filtered - center) * lax.rsqrt(spread + EPSILON)
    conv_mix = silu(normal * ng[...] + ns[...]).astype(BF16)

    chip, core = tp // 2, lax.rem(tp, 2)
    chips = n_tp // 2
    sibling = chip * 2 + 1 - core

    def there(p, place):
        return lax.rem(chip + p, chips) * 2 + place

    def term_of(dest):
        at = pl.ds(pl.multiple_of(dest * columns, 16), columns)
        return conv_acc[dest] + lax.dot_general(conv_mix, oc[at, :], NT, preferred_element_type=F32)

    def pair_copy(p):
        return pltpu.make_async_remote_copy(
            src_ref=pair_out.at[p], dst_ref=pair_in.at[p],
            send_sem=pair_send.at[p], recv_sem=pair_recv.at[p],
            device_id={"tp": sibling}, device_id_type=MESH,
        )

    def part_copy(p):
        return pltpu.make_async_remote_copy(
            src_ref=part_out.at[p - 1], dst_ref=part_in.at[p - 1],
            send_sem=part_send.at[p - 1], recv_sem=part_recv.at[p - 1],
            device_id={"tp": there(p, core)}, device_id_type=MESH,
        )

    slots = list(range(1, chips)) + [0]
    for p in slots:
        pair_out[p] = term_of(there(p, 1 - core)).astype(BF16)
        pair_copy(p).start()
    for p in slots:
        term = term_of(there(p, core))
        pair_copy(p).wait_recv()
        term = term + pair_in[p].astype(F32)
        if p:
            part_out[p - 1] = term.astype(BF16)
            part_copy(p).start()
        else:
            result = term
    for p in range(1, chips):
        part_copy(p).wait_recv()
        result = result + part_in[p - 1].astype(F32)
    out[...] = result.astype(BF16)

    for w in range(6):
        def one(step, w=w):
            for side in range(2):
                @pl.when(leaves(side, step + 1))
                def _(side=side):
                    z_copy(w, side, step + 1).wait_send()

                if share and w != GATE:
                    @pl.when(arrives(side, step + 1))
                    def _(side=side):
                        y_copy(w, side, step + 1).wait_send()

        each(n_sp - 1, one)
    for r in range(2):
        @pl.when(place_of(r) < n_sp - 1)
        def _(r=r):
            chain_copy(r).wait_send()
            halo_copy(r).wait_send()
    for step in range(n_tp - 1):
        stat_copy(step).wait_send()
    for p in range(chips):
        pair_copy(p).wait_send()
        if p:
            part_copy(p).wait_send()


def fused(cfg, tok_h, gain_h, wk_h, wg_h, wv_h, wq_h, wa_h, wb_h, ldt_h, hgain_h, ck_h, ng_h, ns_h, od_h, oc_h,
          out,
          gain, ldt, hgain, ck, ng, ns,
          tok, nt, wk, wv, wq, wab, wg, odg, ocg, ldo,
          keys, vals, betas, cums, xinv, gaps, rhs, local_out, reads, maps, ends,
          chain_in, chain_out, gout, gend, main_in, edge_in, pad, conv, stat_out, stat_in,
          dall, dm_out, call, acc_ab, acc_q, acc_k, acc_v,
          local_sem, g_send, g_recv, z_send, z_recv, ty_send, ty_recv, tx_recv, tf_send, tf_recv, tz_send, tz_recv,
          ld_send, ld_recv, od_send, od_recv, chain_send, chain_recv,
          main_send, main_recv, edge_send, edge_recv, far_send, rim_send,
          stat_send, stat_recv, dg_send, dg_recv, df_send, df_recv, cg_send, cg_recv, cf_send, cf_recv):
    n_sp, n_tp, conv_total = cfg
    grp, sp, tp = lax.axis_index("grp"), lax.axis_index("sp"), lax.axis_index("tp")
    length, width = tok.shape
    rows = wk_h.shape[0]
    head_width = hgain.shape[1]
    cols = wk.shape[1]
    heads = cols // head_width
    channels = wab.shape[1] // 2
    columns = out.shape[1]
    units = [(j, h) for j in range(2) for h in range(heads)]
    n_units = len(units)
    pairs = [(u, r) for u in range(n_units) for r in range(2)]
    chip, core = tp // 2, lax.rem(tp, 2)
    chips = n_tp // 2
    sibling = tp + 1 - 2 * core
    other = 1 - grp
    edge = (sp == 0) | (sp == n_sp - 1)
    inner = (sp > 0) & (sp < n_sp - 1)
    helps = (sp == 1) | (sp == n_sp - 2)
    helper = jnp.where(sp == 0, 1, n_sp - 2)
    helped = jnp.where(sp == 1, 0, n_sp - 1)
    sources = (wk_h, wg_h, wv_h, wq_h, wa_h, wb_h)
    plain = {KEY: wk, VALUE: wv, QUERY: wq}

    def remote(src, dst, send, recv, **where):
        return pltpu.make_async_remote_copy(
            src_ref=src, dst_ref=dst, send_sem=send, recv_sem=recv, device_id=where, device_id_type=MESH
        )

    counts = (4, 1, 2, 2, 2, 2)
    firsts = (0, 0, 4, 6, 8, 10)

    def source(w):
        if w == GATE:
            return wg_h
        size = channels if w in (GLU, OPEN) else cols
        return sources[w].at[:, pl.ds(pl.multiple_of(grp * size, 128), size)]

    def target(w, index, k=None):
        if w == GATE:
            return wg.at[index]
        slab = rows // counts[w]
        if k is None:
            at = pl.ds(pl.multiple_of(index * rows, 16), rows)
        else:
            at = pl.ds(pl.multiple_of(index * rows + k * slab, 16), slab)
        if w in (GLU, OPEN):
            return wab.at[at, pl.ds(channels if w == OPEN else 0, channels)]
        return plain[w].at[at]

    barrier = pltpu.get_barrier_semaphore()

    def greet(**where):
        pl.semaphore_signal(barrier, inc=1, device_id=where, device_id_type=MESH)

    for step in range(n_tp - 1):
        peer = lax.rem(tp + step + 1, n_tp)
        greet(tp=peer)
        greet(tp=peer, grp=other)
    greet(grp=other)

    @pl.when(sp > 0)
    def _():
        greet(sp=sp - 1)
        greet(sp=sp - 1, grp=other)

    @pl.when(sp < n_sp - 1)
    def _():
        greet(sp=sp + 1)
        greet(sp=sp + 1, grp=other)

    load_tok = pltpu.make_async_copy(tok_h, tok, local_sem.at[0])
    load_tok.start()
    small = [
        pltpu.make_async_copy(src, dst, local_sem.at[9 + i])
        for i, (src, dst) in enumerate(
            ((gain_h, gain), (ldt_h, ldt), (hgain_h, hgain), (ng_h, ng), (ns_h, ns),
             (ck_h.at[:, pl.ds(0, channels)], ck.at[0]), (ck_h.at[:, pl.ds(channels, channels)], ck.at[1]))
        )
    ]
    for copy in small:
        copy.start()
    own = [pltpu.make_async_copy(source(w), target(w, sp), local_sem.at[1 + w]) for w in range(6)]
    for copy in own:
        copy.start()

    def od_rows(index):
        return pl.ds(pl.multiple_of(index * columns, 16), columns)

    load_od = pltpu.make_async_copy(od_h.at[od_rows(tp)], odg.at[tp], local_sem.at[7])
    load_oc = pltpu.make_async_copy(oc_h.at[od_rows(tp)], ocg.at[tp], local_sem.at[8])
    load_od.start()
    load_oc.start()

    load_tok.wait()
    for copy in small:
        copy.wait()
    chunk = 64
    for at in range(0, length, chunk):
        here = tok[at:at + chunk, :].astype(F32)
        scale = lax.rsqrt(jnp.mean(here * here, axis=-1, keepdims=True) + EPSILON)
        nt[at:at + chunk, :] = (here * scale * gain[...]).astype(BF16)

    for w in (GATE, KEY):
        own[w].wait()

    @pl.when(edge)
    def _():
        pl.semaphore_wait(barrier, 2 * n_tp + 1)

    @pl.when(inner)
    def _():
        pl.semaphore_wait(barrier, 2 * n_tp + 3)

    def wide(w):
        return 1 if w in (GLU, OPEN) else 0

    def arrives(w, side, d):
        ok = (sp - d >= 0) if side == 0 else (sp + d < n_sp)
        return ok & inner if wide(w) else ok

    def leaves(w, side, d):
        if side == 0:
            return (sp - (d - 1) >= 0) & (sp < n_sp - 1 - wide(w))
        return (sp + (d - 1) < n_sp) & (sp > wide(w))

    def origin(side, d):
        return sp - d if side == 0 else sp + d

    def z_block(w, index, side, k):
        place = target(w, index, k)
        if w == GATE:
            send, recv = g_send.at[side], g_recv.at[index]
        else:
            send, recv = z_send.at[side], z_recv.at[index, firsts[w] + k]
        return remote(place, place, send, recv, sp=sp + 1 if side == 0 else sp - 1)

    def cuts(w):
        return range(counts[w])

    def offer(w, where, ks=None):
        for side in range(2):
            @pl.when(leaves(w, side, 1) & where)
            def _(side=side):
                for k in cuts(w) if ks is None else ks:
                    z_block(w, sp, side, k).start()

    def from_edge(side, d):
        return (sp - d == 0) if side == 0 else (sp + d == n_sp - 1)

    def relay(w, d, kind=None, ks=None):
        if d > n_sp - 1:
            return
        for k in cuts(w) if ks is None else ks:
            for side in range(2):
                onward = leaves(w, side, d + 1) if d < n_sp - 1 else sp < 0
                here = arrives(w, side, d) & onward
                if kind == "edge":
                    here = here & from_edge(side, d)
                if kind == "inner":
                    here = here & ~from_edge(side, d)

                @pl.when(here)
                def _(side=side, k=k):
                    z_block(w, origin(side, d), side, k).wait_recv()
                    z_block(w, origin(side, d), side, k).start()

    def drain(w, d):
        for k in cuts(w):
            for side in range(2):
                onward = leaves(w, side, d + 1) if d < n_sp - 1 else sp < 0

                @pl.when(arrives(w, side, d) & ~onward)
                def _(side=side, k=k):
                    z_block(w, origin(side, d), side, k).wait_recv()

    pieces = ty_recv.shape[0]
    half = length // 2
    piece = half // pieces
    grains = tz_recv.shape[0]
    grain = half // grains

    def part(block, side, c):
        size = grain if block > 1 else piece
        return nt.at[pl.ds(pl.multiple_of(block * length + side * half + c * size, 16), size)]

    def tok_y(k, c):
        return remote(
            part(2 * k, core, c), part(2 * k + 1, core, c), ty_send.at[k], (ty_recv, tx_recv)[k].at[c], grp=other
        )

    def tok_z(c):
        src = nt.at[pl.ds(pl.multiple_of(core * half + c * grain, 16), grain)]
        return remote(src, part(2, core, c), tz_send.at[0], tz_recv.at[c], sp=helper)

    def tok_f(block, c):
        return remote(
            part(block, core, c), part(block, core, c), tf_send.at[block - 1], tf_recv.at[block - 1], tp=sibling
        )

    def tok_f_arrival(block):
        place = nt.at[pl.ds(pl.multiple_of(block * length + (1 - core) * half, 16), half)]
        return remote(place, place, tf_send.at[block - 1], tf_recv.at[block - 1], tp=sibling)

    def half_rows(send):
        place = nt.at[pl.ds(0, half)]
        return remote(place, place, send, send, tp=sibling)

    def pass_y(k, c):
        tok_y(k, c).wait_recv()
        tok_f(2 * k + 1, c).start()

    def pass_z(c):
        @pl.when(helps)
        def _():
            tok_z(c).wait_recv()
            tok_y(1, c).start()
            tok_f(2, c).start()

    def pass_far(c):
        @pl.when(helps)
        def _():
            pass_y(1, c)

    ld_copy = remote(ldt, ldo, ld_send.at[0], ld_recv.at[0], grp=other)

    def od_copy(m, step):
        dest = lax.rem(tp + step + 1, n_tp)
        src, dst = ((od_h, odg), (oc_h, ocg))[m]
        return remote(src.at[od_rows(dest)], dst.at[tp], od_send.at[m], od_recv.at[m], tp=dest)

    def od_all(m):
        place = (odg, ocg)[m].at[pl.ds(0, n_tp - 1)]
        return remote(place, place, od_send.at[m], od_recv.at[m], tp=sibling)

    everywhere = sp >= 0
    offer(GATE, everywhere)
    offer(KEY, everywhere)
    for c in range(pieces):
        tok_y(0, c).start()
    ld_copy.start()
    for w in (VALUE, GLU, OPEN, QUERY):
        own[w].wait()
    offer(VALUE, edge)
    offer(GLU, edge)
    for first in (0, grains // 2):
        @pl.when(edge)
        def _(first=first):
            for c in range(first, first + grains // 2):
                tok_z(c).start()

        if first == 0:
            offer(OPEN, edge)

    offer(QUERY, edge)
    for m in (1, 0):
        for step in range(n_tp - 1):
            od_copy(m, step).start()

    def dot(a, b, dims=NN):
        return lax.dot_general(a, b, dims, preferred_element_type=F32)

    def unit_rows(tensor):
        return tensor * lax.rsqrt(jnp.sum(tensor * tensor, axis=-1, keepdims=True) + EPSILON)

    def silu(tensor):
        return tensor * jax.nn.sigmoid(tensor)

    def block_dot(first, count, w_ref, index):
        lanes = pl.ds(pl.multiple_of(index * rows, 128), rows)
        at = pl.ds(pl.multiple_of(index * rows, 128), rows)
        return dot(nt[first * length:(first + count) * length, lanes], w_ref[at, :])

    def neighbours(w, d, action):
        for side in range(2):
            @pl.when(arrives(w, side, d))
            def _(side=side):
                action(sp - d if side == 0 else sp + d)

    def adder(acc, w_ref, first, count):
        span = slice(first * length, (first + count) * length)

        def add(index, fresh=False):
            x = block_dot(first, count, w_ref, index)
            acc[span, :] = x if fresh else acc[span, :] + x

        return add

    row_at = lax.broadcasted_iota(jnp.int32, (length, length), 0)
    col_at = lax.broadcasted_iota(jnp.int32, (length, length), 1)
    same = row_at == col_at
    mine = grp == 0
    gates = 4 * heads

    def weights_of(j):
        span = slice(j * length, (j + 1) * length)
        cols_part = jnp.zeros((length, wg.shape[1]), F32)
        for index in range(n_sp):
            cols_part = cols_part + dot(nt[span, index * rows:(index + 1) * rows], wg[index], NT)
        rows_part = jnp.transpose(cols_part)
        gate_cols = jnp.where(mine, cols_part[:, :gates], cols_part[:, gates:])
        gate_rows = jnp.where(mine, rows_part[:gates, :], rows_part[gates:, :])
        log = (ldt, ldo)[j]
        rates = jnp.where(mine, log[:2 * heads, :], log[2 * heads:, :])
        for h in range(heads):
            for r in range(2):
                p = 2 * (j * heads + h) + r
                g = 4 * h + 2 * r
                decay_row = rates[2 * h + r:2 * h + r + 1, :] * (0.5 + jax.nn.sigmoid(gate_rows[g:g + 1, :]))
                beta = jax.nn.sigmoid(gate_cols[:, g + 1:g + 2] - BETA_SHIFT)
                seen = col_at <= row_at if r == 0 else col_at >= row_at
                cum_col = jnp.sum(jnp.where(seen, decay_row, 0.0), axis=1, keepdims=True)
                cum_row = jnp.sum(jnp.where(same, cum_col, 0.0), axis=0, keepdims=True)
                gaps[p] = jnp.where(seen, jnp.exp(jnp.where(seen, cum_col - cum_row, 0.0)), 0.0)
                betas[p] = jnp.broadcast_to(beta, (length, head_width))
                cums[p] = jnp.broadcast_to(cum_col, (length, head_width))

    add_key = [adder(acc_k, wk, j, 1) for j in range(2)]
    add_value = [adder(acc_v, wv, j, 1) for j in range(2)]

    relay(GATE, 1)
    relay(KEY, 1, None, (0, 1))
    offer(VALUE, inner, (0,))
    relay(KEY, 1, None, (2, 3))
    offer(VALUE, inner, (1,))
    offer(GLU, inner)
    relay(GATE, 2)
    pass_y(0, 0)
    for d in range(2, n_sp - 1):
        relay(KEY, d, None, (0, 1))
    relay(VALUE, 1, None, (0,))
    for d in range(2, n_sp - 1):
        relay(KEY, d, None, (2, 3))
    pass_y(0, 1)
    relay(VALUE, 1, None, (1,))
    offer(OPEN, inner)
    def pass_value():
        for d in range(2, n_sp - 1):
            relay(VALUE, d)

    drain(KEY, 1)
    add_key[0](sp, True)
    neighbours(KEY, 1, add_key[0])
    pass_y(0, 2)
    offer(QUERY, inner)
    drain(VALUE, 1)
    add_value[0](sp, True)
    neighbours(VALUE, 1, add_value[0])
    relay(GLU, 1)
    for d in range(1, n_sp):
        drain(GATE, d)
    weights_of(0)
    pass_y(0, 3)
    for d in range(2, n_sp - 1):
        drain(KEY, d)
        neighbours(KEY, d, add_key[0])
    ld_copy.wait_recv()
    tok_f_arrival(1).wait_recv()
    pass_z(0)
    weights_of(1)
    pass_z(1)
    pass_z(2)
    add_key[1](sp, True)
    for d in range(1, n_sp - 1):
        neighbours(KEY, d, add_key[1])
    add_value[1](sp, True)
    neighbours(VALUE, 1, add_value[1])
    pass_z(3)
    drain(KEY, n_sp - 1)
    neighbours(KEY, n_sp - 1, adder(acc_k, wk, 0, 2))
    pass_value()

    both = 2 * length
    key_proj = silu(acc_k[...])
    for u, (j, h) in enumerate(units):
        keys[u] = unit_rows(key_proj[j * length:(j + 1) * length, h * head_width:(h + 1) * head_width])
    near = row_at // 2 == col_at // 2
    for u in range(n_units):
        grams = bdot(keys[u], keys[u], NT)
        for r in range(2):
            p = 2 * u + r
            beta = jnp.concatenate([betas[p]] * (length // head_width), axis=1)
            lower = jnp.where(same, 0.0, grams * gaps[p] * beta)
            rhs[p] = lower
            xinv[p] = jnp.where(same, 1.0, jnp.where(near, -lower, 0.0))

    service = {
        8: [lambda: relay(OPEN, 1)],
        32: [lambda: pass_z(4)],
        128: [lambda: pass_z(5)],
    }
    size = 2
    while size < length:
        inside = (row_at // (2 * size) == col_at // (2 * size)) & (row_at // size != col_at // size)
        for p in range(len(pairs)):
            across = jnp.where(inside, rhs[p], 0.0)
            inverse = xinv[p]
            xinv[p] = inverse - bdot(inverse, bdot(across, inverse))
        for act in service.get(size, ()):
            act()
        size *= 2

    for d in range(2, n_sp):
        drain(VALUE, d)
        neighbours(VALUE, d, adder(acc_v, wv, 0, 2))
    value_proj = silu(acc_v[...])
    eye = (
        lax.broadcasted_iota(jnp.int32, (head_width, head_width), 0)
        == lax.broadcasted_iota(jnp.int32, (head_width, head_width), 1)
    )
    for u, r in pairs:
        p = 2 * u + r
        j, h = units[u]
        beta, cum, key = betas[p], cums[p], keys[u]
        value = value_proj[j * length:(j + 1) * length, h * head_width:(h + 1) * head_width]
        total = cum[length - 1:length, :] if r == 0 else cum[0:1, :]
        right = jnp.concatenate([beta * value, beta * key * jnp.exp(cum)], axis=1)
        solved = bdot(xinv[p], right)
        vals[p] = solved.astype(BF16)
        passed = bdot(key * jnp.exp(total - cum), solved, TN)
        ends[p] = passed[:, :head_width]
        maps[p] = (jnp.where(eye, jnp.exp(total), 0.0) - passed[:, head_width:]).astype(BF16)

    def place_of(r):
        return sp if r == 0 else n_sp - 1 - sp

    def chain_copy(r):
        dest = sp + 1 if r == 0 else sp - 1
        return remote(chain_out.at[r], chain_in.at[r], chain_send.at[r], chain_recv.at[r], sp=dest)

    def chain_point(low, high):
        for r in range(2):
            at = place_of(r)

            @pl.when((at >= low) & (at <= high))
            def _(r=r, at=at):
                if low == 0:
                    for u in range(n_units):
                        chain_in[r, u] = jnp.zeros((head_width, head_width), BF16)
                        chain_out[r, u] = ends[2 * u + r].astype(BF16)
                else:
                    chain_copy(r).wait_recv()
                    for u in range(n_units):
                        p = 2 * u + r
                        chain_out[r, u] = (bdot(maps[p], chain_in[r, u]) + ends[p]).astype(BF16)

                @pl.when(at < n_sp - 1)
                def _():
                    chain_copy(r).start()

    chain_point(0, 0)
    pass_z(6)
    relay(QUERY, 1, "inner")
    add_near = adder(acc_ab, wab, 0, 2)
    add_query = adder(acc_q, wq, 0, 2)
    drain(GLU, 1)
    drain(OPEN, 1)

    @pl.when(inner)
    def _():
        add_near(sp, True)

    pass_z(7)
    for c in range(4):
        pass_far(c)
    neighbours(GLU, 1, add_near)
    relay(QUERY, 1, "edge", (0,))
    pass_far(4)
    relay(QUERY, 1, "edge", (1,))
    pass_far(5)
    for d in range(2, n_sp - 1):
        for w in (GLU, OPEN):
            relay(w, d)
            drain(w, d)
        neighbours(GLU, d, add_near)

    def gated(x):
        return (x[:, :channels] * jax.nn.sigmoid(x[:, channels:])).astype(BF16)

    def owner(j):
        return grp if j == 0 else other

    def main_y():
        return remote(gout, main_in.at[grp], main_send.at[0], main_recv.at[grp], grp=other)

    def main_arrival(h):
        return remote(main_in.at[h], main_in.at[h], main_send.at[0], main_recv.at[h], grp=other)

    def far_copy(j):
        return remote(gend.at[j], main_in.at[grp], far_send.at[0], main_recv.at[grp], sp=helped, grp=owner(j))

    def edge_copy(side, j):
        start = length - HALO if side == 0 else 0
        src = main_in.at[grp, pl.ds(start, HALO)] if j == 0 else gout.at[pl.ds(start, HALO)]
        return remote(
            src, edge_in.at[side, grp], edge_send.at[0], edge_recv.at[side, grp],
            sp=sp + 1 if side == 0 else sp - 1, grp=owner(j),
        )

    def rim_copy(side):
        start = length - HALO if side == 0 else 0
        return remote(
            gend.at[1, pl.ds(start, HALO)], edge_in.at[side, grp], rim_send.at[0], edge_recv.at[side, grp], grp=other
        )

    def edge_arrival(side, h):
        place = edge_in.at[side, h]
        return remote(place, place, edge_send.at[0], edge_recv.at[side, h], grp=other)

    @pl.when(inner)
    def _():
        near_rows = gated(acc_ab[...])
        main_in[grp] = near_rows[:length]
        gout[...] = near_rows[length:]
        main_y().start()
        for side in range(2):
            for j in range(2):
                edge_copy(side, j).start()

    def give_far(j):
        gend[j] = gated(dot(nt[(2 + j) * length:(3 + j) * length, :], wab[...]))
        far_copy(j).start()

    @pl.when(helps)
    def _():
        tok_f_arrival(2).wait_recv()
        give_far(0)
        for side, at in ((0, 1), (1, n_sp - 2)):
            @pl.when(sp == at)
            def _(side=side):
                start = length - HALO if side == 0 else 0
                edge_in[side, grp] = gend[0, start:start + HALO, :]

    pass_far(6)
    chain_point(1, 1)
    pass_far(7)

    @pl.when(helps)
    def _():
        tok_f_arrival(3).wait_recv()
        give_far(1)
        for side, at in ((0, 1), (1, n_sp - 2)):
            @pl.when(sp == at)
            def _(side=side):
                rim_copy(side).start()

    for d in range(2, n_sp - 1):
        chain_point(d, d)
        relay(QUERY, d)
    drain(QUERY, 1)
    add_query(sp, True)
    neighbours(QUERY, 1, add_query)
    for d in range(2, n_sp - 1):
        drain(QUERY, d)
        neighbours(QUERY, d, add_query)

    taps = ck.shape[1]
    for step in range(2):
        h = grp if step == 0 else other
        skip = sp < 0 if step else sp >= 0

        @pl.when(edge if step == 0 else sp >= 0)
        def _(h=h):
            main_arrival(h).wait_recv()

        @pl.when((sp > 0) & ~((sp == 1) & skip))
        def _(h=h):
            edge_arrival(0, h).wait_recv()

        @pl.when((sp < n_sp - 1) & ~((sp == n_sp - 2) & skip))
        def _(h=h):
            edge_arrival(1, h).wait_recv()

        pad[step, HALO:HALO + length, :] = main_in[h].astype(F32)
        for side, start, none in ((0, 0, 0), (1, HALO + length, n_sp - 1)):
            @pl.when(sp != none)
            def _(h=h, step=step, side=side, start=start):
                pad[step, start:start + HALO, :] = edge_in[side, h].astype(F32)

            @pl.when(sp == none)
            def _(step=step, start=start):
                pad[step, start:start + HALO, :] = jnp.zeros((HALO, channels), F32)

        for at in range(0, length, chunk):
            first = at + HALO - taps // 2
            total = pad[step, first:first + chunk, :] * ck[h, 0:1, :]
            for k in range(1, taps):
                total = total + pad[step, first + k:first + k + chunk, :] * ck[h, k:k + 1, :]
            conv[h, at:at + chunk, :] = total
    filtered = jnp.concatenate([conv[0], conv[1]], axis=1)
    sum_col = jnp.sum(filtered, axis=-1, keepdims=True)
    square_col = jnp.sum(filtered * filtered, axis=-1, keepdims=True)
    stat_out[...] = jnp.zeros(stat_out.shape, F32)
    stat_out[0:1, :] = jnp.sum(jnp.where(same, sum_col, 0.0), axis=0, keepdims=True)
    stat_out[1:2, :] = jnp.sum(jnp.where(same, square_col, 0.0), axis=0, keepdims=True)

    def stat_copy(step):
        return remote(
            stat_out, stat_in.at[step], stat_send.at[0], stat_recv.at[0], tp=lax.rem(tp + step + 1, n_tp)
        )

    for step in range(n_tp - 1):
        stat_copy(step).start()

    def chip_at(q):
        return lax.rem(chip + q, chips)

    def chip_back(q):
        return lax.rem(chip + chips - q, chips)

    def dg_copy(a, q):
        src = dall.at[tp, grp] if a == 0 else dm_out
        where = {"tp": chip_at(q) * 2 + core}
        if a:
            where["grp"] = other
        return remote(src, dall.at[tp, grp], dg_send.at[a], dg_recv.at[a, q], **where)

    def d_block(a, q, side):
        return dall.at[chip_back(q) * 2 + side, other if a else grp]

    def dg_arrival(a, q):
        place = d_block(a, q, core)
        return remote(place, place, dg_send.at[a], dg_recv.at[a, q], tp=sibling)

    def df_copy(a, q):
        place = d_block(a, q, core)
        return remote(place, place, df_send.at[0], df_recv.at[q], tp=sibling)

    def df_arrival(q):
        place = dall.at[chip_back(q) * 2 + 1 - core]
        return remote(place, place, df_send.at[0], df_recv.at[q], tp=sibling)

    def cg_copy(q):
        return remote(call.at[tp], call.at[tp], cg_send.at[0], cg_recv.at[q], tp=chip_at(q) * 2 + core)

    def cg_arrival(q):
        place = call.at[chip_back(q) * 2 + core]
        return remote(place, place, cg_send.at[0], cg_recv.at[q], tp=sibling)

    def cf_copy(q, arriving=False):
        place = call.at[chip_back(q) * 2 + (1 - core if arriving else core)]
        return remote(place, place, cf_send.at[0], cf_recv.at[q], tp=sibling)

    stats = stat_out[0:2, :]
    stat_all = remote(stat_in, stat_in, stat_send.at[0], stat_recv.at[0], tp=sibling)
    stat_all.wait_recv()
    for step in range(n_tp - 1):
        stats = stats + stat_in[step, 0:2, :]
    center = jnp.sum(jnp.where(same, stats[0:1, :], 0.0), axis=1, keepdims=True) / conv_total
    squares = jnp.sum(jnp.where(same, stats[1:2, :], 0.0), axis=1, keepdims=True) / conv_total
    spread = squares - center * center
    normal = (jnp.concatenate([conv[0], conv[1]], axis=1) - center) * lax.rsqrt(spread + EPSILON)
    call[tp] = silu(normal * ng[...] + ns[...]).astype(BF16)
    for q in range(1, chips):
        cg_copy(q).start()
    cf_copy(0).start()

    def delta_term(t):
        return dot(jnp.concatenate([dall[t, 0], dall[t, 1]], axis=1), odg[t], NT)

    def conv_term(t):
        return dot(call[t], ocg[t], NT)

    chain_point(n_sp - 1, n_sp - 1)
    drain(QUERY, n_sp - 1)
    neighbours(QUERY, n_sp - 1, add_query)

    def read(u):
        j, h = units[u]
        query = silu(acc_q[j * length:(j + 1) * length, h * head_width:(h + 1) * head_width])
        query = unit_rows(query) * head_width ** -0.5
        scores = bdot(query, keys[u], NT)
        for r in range(2):
            p = 2 * u + r
            pair = dot((scores * gaps[p]).astype(BF16), vals[p])
            reads[p] = (query * jnp.exp(cums[p]) - pair[:, head_width:]).astype(BF16)
            if r == 0:
                local_out[u] = pair[:, :head_width]
            else:
                local_out[u] = local_out[u] + pair[:, :head_width]

    def mixed_head(u):
        joined = local_out[u] + dot(reads[2 * u], chain_in[0, u]) + dot(reads[2 * u + 1], chain_in[1, u])
        scale = lax.rsqrt(jnp.mean(joined * joined, axis=-1, keepdims=True) + EPSILON)
        return (joined * scale * hgain[...]).astype(BF16)

    direct = [(a, q) for q in range(chips) for a in (1, 0) if (a, q) != (0, 0)]

    for h in range(heads):
        read(heads + h)
        dm_out[:, h * head_width:(h + 1) * head_width] = mixed_head(heads + h)
    for q in range(chips - 1, -1, -1):
        dg_copy(1, q).start()
    for h in range(heads):
        read(h)
        dall[tp, grp, :, h * head_width:(h + 1) * head_width] = mixed_head(h)
    for q in range(1, chips):
        dg_copy(0, q).start()
    df_copy(0, 0).start()

    for m in range(2):
        od_all(m).wait_recv()
    load_od.wait()
    load_oc.wait()
    result = conv_term(tp)
    for q in range(1, chips):
        cg_arrival(q).wait_recv()
        cf_copy(q).start()
    for q in range(1, chips):
        result = result + conv_term(chip_back(q) * 2 + core)
    for a, q in direct:
        dg_arrival(a, q).wait_recv()
        df_copy(a, q).start()
        if (a, q) == (1, 0):
            for p in range(chips):
                cf_copy(p, True).wait_recv()
                result = result + conv_term(chip_back(p) * 2 + 1 - core)
            result = result + delta_term(tp)
    for q in range(1, chips):
        result = result + delta_term(chip_back(q) * 2 + core)
    for q in range(chips):
        df_arrival(q).wait_recv()
        result = result + delta_term(chip_back(q) * 2 + 1 - core)
    out[...] = result.astype(BF16)

    for side in range(2):
        for q in range(n_sp):
            far = n_sp - 1 if side == 0 else 0
            copies = 0 if q == far else (q + 1 if side == 0 else n_sp - q)
            wide_to = n_sp - 2 if side == 0 else 1
            wide_copies = copies if (q < wide_to if side == 0 else q > wide_to) else 0
            if copies:
                @pl.when(sp == q)
                def _(side=side, copies=copies, wide_copies=wide_copies):
                    place = wg.at[pl.ds(0, copies)]
                    remote(place, place, g_send.at[side], g_send.at[side], tp=sibling).wait_send()
                    total = (3 * cols * copies + 2 * channels * wide_copies) * rows // width
                    place = nt.at[pl.ds(0, total)]
                    remote(place, place, z_send.at[side], z_send.at[side], tp=sibling).wait_send()
    half_rows(ty_send.at[0]).wait_send()
    half_rows(tf_send.at[0]).wait_send()

    @pl.when(edge)
    def _():
        half_rows(tz_send.at[0]).wait_send()

    @pl.when(helps)
    def _():
        half_rows(ty_send.at[1]).wait_send()
        half_rows(tf_send.at[1]).wait_send()
        half_rows(tf_send.at[2]).wait_send()
        remote(gend, gend, far_send.at[0], far_send.at[0], tp=sibling).wait_send()
        rim_copy(0).wait_send()

    ld_copy.wait_send()
    for m in range(2):
        od_all(m).wait_send()
    for r in range(2):
        @pl.when(place_of(r) < n_sp - 1)
        def _(r=r):
            chain_copy(r).wait_send()

    @pl.when(inner)
    def _():
        main_y().wait_send()
        remote(edge_in, edge_in, edge_send.at[0], edge_send.at[0], tp=sibling).wait_send()

    stat_all.wait_send()
    place = dall.at[pl.ds(0, chips), 0]
    remote(place, place, dg_send.at[1], dg_send.at[1], tp=sibling).wait_send()
    if chips > 1:
        place = dall.at[pl.ds(0, chips - 1), 0]
        remote(place, place, dg_send.at[0], dg_send.at[0], tp=sibling).wait_send()
        place = call.at[pl.ds(0, chips - 1)]
        remote(place, place, cg_send.at[0], cg_send.at[0], tp=sibling).wait_send()
    place = dall.at[pl.ds(0, chips)]
    remote(place, place, df_send.at[0], df_send.at[0], tp=sibling).wait_send()
    place = call.at[pl.ds(0, chips)]
    remote(place, place, cf_send.at[0], cf_send.at[0], tp=sibling).wait_send()


def solution(mesh):
    n_grp, n_sp, n_tp = mesh.shape["grp"], mesh.shape["sp"], mesh.shape["tp"]

    def on_device(tokens_in, input_gain, w_query, w_key, w_value, w_gates, w_glu_value,
                  sigmoid_opener_matrix, log_decay, head_gain, conv_kernel, norm_gain, norm_shift,
                  out_delta, out_conv):
        length, width = tokens_in.shape
        head_width = head_gain.shape[0]
        head_cols = w_query.shape[1]
        heads = head_cols // head_width
        channels = w_glu_value.shape[1]
        rows = w_query.shape[0]
        pairs = 2 * heads
        columns = width // n_tp
        dma, vmem = pltpu.SemaphoreType.DMA, pltpu.VMEM
        anywhere = pl.BlockSpec(memory_space=pltpu.HBM)
        inside = pl.BlockSpec(memory_space=pltpu.VMEM)
        if n_grp == 2 and n_sp >= 4 and n_tp % 2 == 0 and heads % 2 == 0 and channels % 256 == 0                 and (3 * head_cols + 2 * channels) * rows * n_sp <= 8 * length * width:
            cols, ch, chips, steps = head_cols // 2, channels // 2, n_tp // 2, n_tp - 1
            pieces = 4
            scratch = [
                vmem((1, width), F32), vmem((pairs, length), F32), vmem((1, head_width), F32),
                vmem((2, conv_kernel.shape[0], ch), F32), vmem((1, channels), F32), vmem((1, channels), F32),
                vmem((length, width), BF16), vmem((4 * length, width), BF16),
                vmem((width, cols), BF16), vmem((width, cols), BF16), vmem((width, cols), BF16),
                vmem((width, 2 * ch), BF16), vmem((n_sp, 4 * heads, rows), BF16),
                vmem((n_tp, columns, head_cols), BF16), vmem((n_tp, columns, channels), BF16),
                vmem((pairs, length), F32),
                vmem((heads, length, head_width), F32), vmem((pairs, length, 2 * head_width), BF16),
                vmem((pairs, length, head_width), F32), vmem((pairs, length, head_width), F32),
                vmem((pairs, length, length), F32), vmem((pairs, length, length), F32),
                vmem((pairs, length, length), F32),
                vmem((heads, length, head_width), F32), vmem((pairs, length, head_width), BF16),
                vmem((pairs, head_width, head_width), BF16), vmem((pairs, head_width, head_width), F32),
                vmem((2, heads, head_width, head_width), BF16), vmem((2, heads, head_width, head_width), BF16),
                vmem((length, ch), BF16), vmem((2, length, ch), BF16), vmem((2, length, ch), BF16),
                vmem((2, 2, HALO, ch), BF16),
                vmem((2, length + 2 * HALO, ch), F32), vmem((2, length, ch), F32),
                vmem((8, length), F32), vmem((steps, 8, length), F32),
                vmem((n_tp, 2, length, cols), BF16), vmem((length, cols), BF16),
                vmem((n_tp, length, channels), BF16), vmem((2 * length, 2 * ch), F32), vmem((2 * length, cols), F32),
                vmem((2 * length, cols), F32), vmem((2 * length, cols), F32),
                dma((16,)),
                dma((2,)), dma((n_sp,)), dma((2,)), dma((n_sp, 12)),
                dma((2,)), dma((pieces,)), dma((2 * pieces,)), dma((3,)), dma((3,)),
                dma((1,)), dma((2 * pieces,)),
                dma((1,)), dma((1,)), dma((2,)), dma((2,)), dma((2,)), dma((2,)),
                dma((1,)), dma((2,)), dma((1,)), dma((2, 2)), dma((1,)), dma((1,)),
                dma((1,)), dma((1,)),
                dma((2,)), dma((2, chips)), dma((1,)), dma((chips,)),
                dma((1,)), dma((chips,)), dma((1,)), dma((chips,)),
            ]
            return pl.pallas_call(
                functools.partial(fused, (n_sp, n_tp, float(channels * n_tp))),
                out_shape=pltpu.VMEM((length, columns), BF16),
                in_specs=[anywhere] * 15,
                out_specs=inside,
                scratch_shapes=scratch,
                compiler_params=pltpu.CompilerParams(
                    collective_id=0, has_side_effects=True, vmem_limit_bytes=58 * 1024 * 1024
                ),
            )(
                tokens_in, input_gain.reshape(1, width), w_key, w_gates.T, w_value, w_query,
                w_glu_value, sigmoid_opener_matrix, log_decay.T,
                head_gain.reshape(1, head_width), conv_kernel, norm_gain.reshape(1, channels),
                norm_shift.reshape(1, channels), out_delta, out_conv,
            )
        scratch = [
            vmem((length, width), BF16), vmem((length, width), BF16),
            vmem((width, head_cols), BF16), vmem((n_sp, 4 * heads, rows), BF16),
            vmem((width, head_cols), BF16), vmem((width, head_cols), BF16),
            vmem((width, channels), BF16), vmem((width, channels), BF16),
            vmem((width, head_cols), BF16), vmem((width, channels), BF16),
            vmem((heads, length, head_width), F32), vmem((pairs, length, 2 * head_width), BF16),
            vmem((pairs, length, head_width), F32), vmem((pairs, length, head_width), F32),
            vmem((pairs, length, length), F32), vmem((pairs, length, length), F32),
            vmem((pairs, length, length), F32),
            vmem((heads, length, head_width), F32), vmem((pairs, length, head_width), BF16),
            vmem((pairs, head_width, head_width), BF16), vmem((pairs, head_width, head_width), F32),
            vmem((2, heads, head_width, head_width), BF16), vmem((2, heads, head_width, head_width), BF16),
            vmem((length, channels), BF16), vmem((2, HALO, channels), BF16),
            vmem((length + 2 * HALO, channels), F32), vmem((length, channels), F32),
            vmem((8, length), F32), vmem((n_tp - 1, 8, length), F32),
            vmem((n_tp, length, columns), F32),
            vmem((n_tp // 2, length, columns), BF16), vmem((n_tp // 2, length, columns), BF16),
            vmem((n_tp // 2, length, columns), BF16), vmem((n_tp // 2, length, columns), BF16),
            dma((9,)),
            dma((6, 2, n_sp - 1)), dma((6, 2, n_sp - 1)),
            dma((6, 2, n_sp - 1)), dma((6, 2, n_sp - 1)),
            dma((2,)), dma((2,)), dma((2,)), dma((2,)),
            dma((n_tp - 1,)), dma((n_tp - 1,)), dma((n_tp // 2,)), dma((n_tp // 2,)),
            dma((n_tp // 2,)), dma((n_tp // 2,)),
        ]
        return pl.pallas_call(
            functools.partial(kernel, (n_grp, n_sp, n_tp, float(channels * n_tp))),
            out_shape=jax.ShapeDtypeStruct((length, columns), BF16),
            in_specs=[anywhere, inside] + [anywhere] * 6 + [inside] * 6 + [anywhere] * 2,
            out_specs=inside,
            scratch_shapes=scratch,
            compiler_params=pltpu.CompilerParams(
                collective_id=0, has_side_effects=True, vmem_limit_bytes=60 * 1024 * 1024
            ),
        )(
            tokens_in, input_gain.reshape(1, width), w_key, w_gates.T, w_value, w_query,
            w_glu_value, sigmoid_opener_matrix, log_decay, log_decay.T,
            head_gain.reshape(1, head_width), conv_kernel, norm_gain.reshape(1, channels),
            norm_shift.reshape(1, channels), out_delta, out_conv,
        )

    placed = (
        P(("grp", "sp"), None), P(), P("sp", "tp"), P("sp", "tp"), P("sp", "tp"), P("sp", "tp"),
        P("sp", "tp"), P("sp", "tp"), P(("grp", "sp"), "tp"), P(), P(None, "tp"), P("tp"), P("tp"),
        P(None, "tp"), P(None, "tp"),
    )
    return jax.shard_map(
        on_device, mesh=mesh, in_specs=placed, out_specs=P(("grp", "sp"), "tp"), check_vma=False
    )
```

```python
import functools

import jax
import jax.numpy as jnp
from jax import lax
from jax.experimental import pallas as pl
from jax.experimental.pallas import tpu as pltpu
from jax.sharding import PartitionSpec as P

EPSILON = 1e-06
BETA_SHIFT = 6.0
HALO = 16
MESH = pl.DeviceIdType.MESH
F32 = jnp.float32
BF16 = jnp.bfloat16
NT = (((1,), (1,)), ((), ()))
TN = (((0,), (0,)), ((), ()))
NN = (((1,), (0,)), ((), ()))
KEY, GATE, VALUE, QUERY, GLU, OPEN = range(6)


def bdot(left, right, dims=NN):
    return lax.dot_general(
        left.astype(BF16), right.astype(BF16), dims, preferred_element_type=F32
    )


def each(count, action):
    if count <= 8:
        for step in range(count):
            action(step)
    else:
        def body(step, carry):
            action(step)
            return carry

        lax.fori_loop(0, count, body, 0)


def kernel(cfg, tok_h, gain, wk_h, wg_h, wv_h, wq_h, wa_h, wb_h, ld, ldt, hgain, ck, ng, ns, od_h, oc_h,
           out,
           tok, normed, wk, wg, wv, wq, wa, wb, od, oc,
           keys, vals, betas, cums, xinv, gaps, rhs, local_out, reads, maps, ends,
           chain_in, chain_out, glu, halo, pad, conv, stat_out, stat_in, conv_acc, part_out, part_in, pair_out, pair_in,
           local_sem, z_send, z_recv, y_send, y_recv, chain_send, chain_recv,
           halo_send, halo_recv, stat_send, stat_recv, part_send, part_recv, pair_send, pair_recv):
    n_grp, n_sp, n_tp, conv_total = cfg
    grp, sp, tp = lax.axis_index("grp"), lax.axis_index("sp"), lax.axis_index("tp")
    length, width = tok.shape
    rows = wk_h.shape[0]
    channels = wa.shape[1]
    head_width = hgain.shape[1]
    heads = wk.shape[1] // head_width
    share = (rows // 2) // 16 * 16 if n_grp == 2 else 0
    pulled = rows - share

    sources = (wk_h, wg_h, wv_h, wq_h, wa_h, wb_h)
    targets = (wk, wg, wv, wq, wa, wb)

    def block_of(w, index, start, count):
        if w == GATE:
            return targets[w].at[index]
        return targets[w].at[pl.ds(pl.multiple_of(index * rows + start, 16), count)]

    load_tok = pltpu.make_async_copy(tok_h, tok, local_sem.at[0])
    load_tok.start()
    own = [
        pltpu.make_async_copy(sources[w], block_of(w, sp, 0, rows), local_sem.at[1 + w])
        for w in range(6)
    ]
    for copy in own:
        copy.start()
    load_od = pltpu.make_async_copy(od_h, od, local_sem.at[7])
    load_oc = pltpu.make_async_copy(oc_h, oc, local_sem.at[8])

    barrier = pltpu.get_barrier_semaphore()

    def greet(axis, me, count):
        def one(step):
            pl.semaphore_signal(
                barrier, inc=1, device_id={axis: lax.rem(me + step + 1, count)}, device_id_type=MESH
            )

        each(count - 1, one)

    greet("sp", sp, n_sp)
    greet("tp", tp, n_tp)
    greet("grp", grp, n_grp)
    pl.semaphore_wait(barrier, n_sp + n_tp + n_grp - 3)

    def origin(side, d):
        return sp - d if side == 0 else sp + d

    def arrives(side, d):
        return sp - d >= 0 if side == 0 else sp + d < n_sp

    def leaves(side, d):
        if side == 0:
            return (sp - (d - 1) >= 0) & (sp < n_sp - 1)
        return (sp + (d - 1) < n_sp) & (sp > 0)

    def part_of(w, index, side_of):
        if w == GATE:
            return block_of(w, index, 0, 0)
        if not share:
            return block_of(w, index, 0, rows)
        if side_of is None:
            return block_of(w, index, pl.multiple_of(grp * share, 16), pulled)
        return block_of(w, index, pl.multiple_of(side_of * pulled, 16), share)

    def z_copy(w, side, d, first=False):
        target = part_of(w, origin(side, d - 1), None)
        source = target
        if first:
            source = sources[w]
            if w != GATE and share:
                source = source.at[pl.ds(pl.multiple_of(grp * share, 16), pulled)]
        return pltpu.make_async_remote_copy(
            src_ref=source, dst_ref=target,
            send_sem=z_send.at[w, side, d - 1], recv_sem=z_recv.at[w, side, d - 1],
            device_id={"sp": sp + 1 if side == 0 else sp - 1}, device_id_type=MESH,
        )

    def z_arrival(w, side, d):
        place = part_of(w, origin(side, d), None)
        return pltpu.make_async_remote_copy(
            src_ref=place, dst_ref=place,
            send_sem=z_send.at[w, side, d - 1], recv_sem=z_recv.at[w, side, d - 1],
            device_id={"sp": sp + 1 if side == 0 else sp - 1}, device_id_type=MESH,
        )

    def y_copy(w, side, d, arriving=False):
        place = part_of(w, origin(side, d), 1 - grp if arriving else grp)
        return pltpu.make_async_remote_copy(
            src_ref=place, dst_ref=place,
            send_sem=y_send.at[w, side, d - 1], recv_sem=y_recv.at[w, side, d - 1],
            device_id={"grp": 1 - grp}, device_id_type=MESH,
        )

    def offer(w):
        for side in range(2):
            @pl.when(leaves(side, 1))
            def _(side=side):
                z_copy(w, side, 1, True).start()

    def relay_hop(w, d):
        for side in range(2):
            @pl.when(arrives(side, d))
            def _(side=side):
                z_arrival(w, side, d).wait_recv()

                @pl.when(leaves(side, d + 1))
                def _():
                    z_copy(w, side, d + 1).start()

                if share and w != GATE:
                    y_copy(w, side, d).start()

    def relay(w, low=1, high=None):
        if high is None:
            each(n_sp - low, lambda step: relay_hop(w, step + low))
        else:
            for d in range(low, min(high, n_sp - 1) + 1):
                relay_hop(w, d)

    def complete(w):
        own[w].wait()
        if share and w != GATE:
            def one(step):
                for side in range(2):
                    @pl.when(arrives(side, step + 1))
                    def _(side=side):
                        y_copy(w, side, step + 1, True).wait_recv()

            each(n_sp - 1, one)

    offer(KEY)
    offer(GATE)
    offer(VALUE)
    load_od.start()
    load_oc.start()

    load_tok.wait()
    chunk = 64
    for at in range(0, length, chunk):
        here = tok[at:at + chunk, :].astype(F32)
        scale = lax.rsqrt(jnp.mean(here * here, axis=-1, keepdims=True) + EPSILON)
        normed[at:at + chunk, :] = (here * scale * gain[...]).astype(BF16)

    def project(w):
        return jnp.dot(normed[...], targets[w][...], preferred_element_type=F32)

    def unit_rows(tensor):
        return tensor * lax.rsqrt(jnp.sum(tensor * tensor, axis=-1, keepdims=True) + EPSILON)

    def silu(tensor):
        return tensor * jax.nn.sigmoid(tensor)

    relay(GATE)
    relay(KEY)
    offer(QUERY)
    complete(GATE)
    gate_cols = jnp.zeros((length, 4 * heads), F32)
    gate_rows = jnp.zeros((4 * heads, length), F32)
    for index in range(n_sp):
        normed_part = normed[:, index * rows:(index + 1) * rows]
        gate_cols = gate_cols + lax.dot_general(normed_part, wg[index], NT, preferred_element_type=F32)
        gate_rows = gate_rows + lax.dot_general(wg[index], normed_part, NT, preferred_element_type=F32)

    row_at = lax.broadcasted_iota(jnp.int32, (length, length), 0)
    col_at = lax.broadcasted_iota(jnp.int32, (length, length), 1)

    complete(KEY)
    key_proj = silu(project(KEY))
    pairs = [(h, r) for h in range(heads) for r in range(2)]
    for h in range(heads):
        keys[h] = unit_rows(key_proj[:, h * head_width:(h + 1) * head_width])
    relay(VALUE, 1, 1)
    for h in range(heads):
        grams = bdot(keys[h], keys[h], NT)
        for r in range(2):
            p = 2 * h + r
            decay_col = ld[:, p:p + 1] * (0.5 + jax.nn.sigmoid(gate_cols[:, 2 * p:2 * p + 1]))
            decay_row = ldt[p:p + 1, :] * (0.5 + jax.nn.sigmoid(gate_rows[2 * p:2 * p + 1, :]))
            beta = jax.nn.sigmoid(gate_cols[:, 2 * p + 1:2 * p + 2] - BETA_SHIFT)
            if r == 0:
                seen_down, seen_across = row_at <= col_at, col_at <= row_at
            else:
                seen_down, seen_across = row_at >= col_at, col_at >= row_at
            cum_row = jnp.sum(jnp.where(seen_down, decay_col, 0.0), axis=0, keepdims=True)
            cum_col = jnp.sum(jnp.where(seen_across, decay_row, 0.0), axis=1, keepdims=True)
            weighting = jnp.where(
                seen_across, jnp.exp(jnp.where(seen_across, cum_col - cum_row, 0.0)), 0.0
            )
            gaps[p] = weighting
            betas[p] = jnp.broadcast_to(beta, (length, head_width))
            cums[p] = jnp.broadcast_to(cum_col, (length, head_width))
            lower = jnp.where(row_at != col_at, grams * weighting * beta, 0.0)
            rhs[p] = lower
            near = (row_at // 2 == col_at // 2)
            xinv[p] = jnp.where(row_at == col_at, 1.0, jnp.where(near, -lower, 0.0))

    size = 2
    while size < length:
        inside = (row_at // (2 * size) == col_at // (2 * size)) & (row_at // size != col_at // size)
        for p in range(len(pairs)):
            across = jnp.where(inside, rhs[p], 0.0)
            inverse = xinv[p]
            xinv[p] = inverse - bdot(inverse, bdot(across, inverse))
        if size == 2:
            relay(VALUE, 2)
            offer(GLU)
        if size == 32:
            relay(QUERY, 1, 1)
        if size == 128:
            relay(QUERY, 2, 2)
        size *= 2

    complete(VALUE)
    value_proj = silu(project(VALUE))
    eye = (
        lax.broadcasted_iota(jnp.int32, (head_width, head_width), 0)
        == lax.broadcasted_iota(jnp.int32, (head_width, head_width), 1)
    )
    for h, r in pairs:
        p = 2 * h + r
        beta, cum, key = betas[p], cums[p], keys[h]
        value = value_proj[:, h * head_width:(h + 1) * head_width]
        total = cum[length - 1:length, :] if r == 0 else cum[0:1, :]
        right = jnp.concatenate([beta * value, beta * key * jnp.exp(cum)], axis=1)
        solved = bdot(xinv[p], right)
        vals[p] = solved.astype(BF16)
        passed = bdot(key * jnp.exp(total - cum), solved, TN)
        ends[p] = passed[:, :head_width]
        maps[p] = (jnp.where(eye, jnp.exp(total), 0.0) - passed[:, head_width:]).astype(BF16)

    def place_of(r):
        return sp if r == 0 else n_sp - 1 - sp

    def chain_copy(r):
        dest = lax.rem(sp + 1, n_sp) if r == 0 else lax.rem(sp + n_sp - 1, n_sp)
        return pltpu.make_async_remote_copy(
            src_ref=chain_out.at[r], dst_ref=chain_in.at[r],
            send_sem=chain_send.at[r], recv_sem=chain_recv.at[r],
            device_id={"sp": dest}, device_id_type=MESH,
        )

    def chain_point(low, high):
        for r in range(2):
            at = place_of(r)

            @pl.when((at >= low) & (at <= high))
            def _(r=r, at=at):
                if low == 0:
                    for h in range(heads):
                        chain_in[r, h] = jnp.zeros((head_width, head_width), BF16)
                        chain_out[r, h] = ends[2 * h + r].astype(BF16)
                else:
                    chain_copy(r).wait_recv()
                    for h in range(heads):
                        p = 2 * h + r
                        chain_out[r, h] = (bdot(maps[p], chain_in[r, h]) + ends[p]).astype(BF16)

                @pl.when(at < n_sp - 1)
                def _():
                    chain_copy(r).start()

    chain_point(0, 0)
    relay(QUERY, 3)
    offer(OPEN)
    relay(GLU, 1, 1)
    complete(QUERY)
    query_proj = silu(project(QUERY))
    for h in range(heads):
        query = unit_rows(query_proj[:, h * head_width:(h + 1) * head_width]) * head_width ** -0.5
        scores = bdot(query, keys[h], NT)
        for r in range(2):
            p = 2 * h + r
            both = jnp.dot((scores * gaps[p]).astype(BF16), vals[p], preferred_element_type=F32)
            reads[p] = (query * jnp.exp(cums[p]) - both[:, head_width:]).astype(BF16)
            if r == 0:
                local_out[h] = both[:, :head_width]
            else:
                local_out[h] = local_out[h] + both[:, :head_width]
    chain_point(1, 1)
    relay(GLU, 2, 2)
    chain_point(2, 2)
    relay(GLU, 3)
    relay(OPEN, 1, 1)
    chain_point(3, n_sp - 1)
    complete(GLU)
    glu_proj = project(GLU)
    relay(OPEN, 2)
    complete(OPEN)
    gated = (glu_proj * jax.nn.sigmoid(project(OPEN))).astype(BF16)
    glu[...] = gated
    pad[HALO:HALO + length, :] = gated.astype(F32)

    def halo_copy(r):
        start = length - HALO if r == 0 else 0
        dest = lax.rem(sp + 1, n_sp) if r == 0 else lax.rem(sp + n_sp - 1, n_sp)
        return pltpu.make_async_remote_copy(
            src_ref=glu.at[pl.ds(start, HALO)], dst_ref=halo.at[r],
            send_sem=halo_send.at[r], recv_sem=halo_recv.at[r],
            device_id={"sp": dest}, device_id_type=MESH,
        )

    for r in range(2):
        @pl.when(place_of(r) < n_sp - 1)
        def _(r=r):
            halo_copy(r).start()
    for r in range(2):
        start = 0 if r == 0 else HALO + length

        @pl.when(place_of(r) > 0)
        def _(r=r, start=start):
            halo_copy(r).wait_recv()
            pad[start:start + HALO, :] = halo[r].astype(F32)

        @pl.when(place_of(r) == 0)
        def _(start=start):
            pad[start:start + HALO, :] = jnp.zeros((HALO, channels), F32)

    taps = ck.shape[0]
    for at in range(0, length, chunk):
        first = at + HALO - taps // 2
        total = pad[first:first + chunk, :] * ck[0:1, :]
        for j in range(1, taps):
            total = total + pad[first + j:first + j + chunk, :] * ck[j:j + 1, :]
        conv[at:at + chunk, :] = total
    filtered = conv[...]
    sum_col = jnp.sum(filtered, axis=-1, keepdims=True)
    square_col = jnp.sum(filtered * filtered, axis=-1, keepdims=True)
    same = row_at == col_at
    stat_out[...] = jnp.zeros(stat_out.shape, F32)
    stat_out[0:1, :] = jnp.sum(jnp.where(same, sum_col, 0.0), axis=0, keepdims=True)
    stat_out[1:2, :] = jnp.sum(jnp.where(same, square_col, 0.0), axis=0, keepdims=True)

    def stat_copy(step):
        return pltpu.make_async_remote_copy(
            src_ref=stat_out, dst_ref=stat_in.at[step],
            send_sem=stat_send.at[step], recv_sem=stat_recv.at[step],
            device_id={"tp": lax.rem(tp + step + 1, n_tp)}, device_id_type=MESH,
        )

    for step in range(n_tp - 1):
        stat_copy(step).start()

    joined_heads = []
    for h in range(heads):
        joined = local_out[h] + jnp.dot(reads[2 * h], chain_in[0, h], preferred_element_type=F32)
        joined = joined + jnp.dot(reads[2 * h + 1], chain_in[1, h], preferred_element_type=F32)
        scale = lax.rsqrt(jnp.mean(joined * joined, axis=-1, keepdims=True) + EPSILON)
        joined_heads.append((joined * scale * hgain[...]).astype(BF16))
    delta_mix = jnp.concatenate(joined_heads, axis=1) if heads > 1 else joined_heads[0]
    load_od.wait()
    load_oc.wait()
    columns = width // n_tp
    for dest in range(n_tp):
        at = slice(dest * columns, (dest + 1) * columns)
        conv_acc[dest] = lax.dot_general(delta_mix, od[at, :], NT, preferred_element_type=F32)

    stats = stat_out[0:2, :]
    for step in range(n_tp - 1):
        stat_copy(step).wait_recv()
        stats = stats + stat_in[step, 0:2, :]
    center = jnp.sum(jnp.where(same, stats[0:1, :], 0.0), axis=1, keepdims=True) / conv_total
    squares = jnp.sum(jnp.where(same, stats[1:2, :], 0.0), axis=1, keepdims=True) / conv_total
    spread = squares - center * center
    normal = (filtered - center) * lax.rsqrt(spread + EPSILON)
    conv_mix = silu(normal * ng[...] + ns[...]).astype(BF16)

    chip, core = tp // 2, lax.rem(tp, 2)
    chips = n_tp // 2
    sibling = chip * 2 + 1 - core

    def there(p, place):
        return lax.rem(chip + p, chips) * 2 + place

    def term_of(dest):
        at = pl.ds(pl.multiple_of(dest * columns, 16), columns)
        return conv_acc[dest] + lax.dot_general(conv_mix, oc[at, :], NT, preferred_element_type=F32)

    def pair_copy(p):
        return pltpu.make_async_remote_copy(
            src_ref=pair_out.at[p], dst_ref=pair_in.at[p],
            send_sem=pair_send.at[p], recv_sem=pair_recv.at[p],
            device_id={"tp": sibling}, device_id_type=MESH,
        )

    def part_copy(p):
        return pltpu.make_async_remote_copy(
            src_ref=part_out.at[p - 1], dst_ref=part_in.at[p - 1],
            send_sem=part_send.at[p - 1], recv_sem=part_recv.at[p - 1],
            device_id={"tp": there(p, core)}, device_id_type=MESH,
        )

    slots = list(range(1, chips)) + [0]
    for p in slots:
        pair_out[p] = term_of(there(p, 1 - core)).astype(BF16)
        pair_copy(p).start()
    for p in slots:
        term = term_of(there(p, core))
        pair_copy(p).wait_recv()
        term = term + pair_in[p].astype(F32)
        if p:
            part_out[p - 1] = term.astype(BF16)
            part_copy(p).start()
        else:
            result = term
    for p in range(1, chips):
        part_copy(p).wait_recv()
        result = result + part_in[p - 1].astype(F32)
    out[...] = result.astype(BF16)

    for w in range(6):
        def one(step, w=w):
            for side in range(2):
                @pl.when(leaves(side, step + 1))
                def _(side=side):
                    z_copy(w, side, step + 1).wait_send()

                if share and w != GATE:
                    @pl.when(arrives(side, step + 1))
                    def _(side=side):
                        y_copy(w, side, step + 1).wait_send()

        each(n_sp - 1, one)
    for r in range(2):
        @pl.when(place_of(r) < n_sp - 1)
        def _(r=r):
            chain_copy(r).wait_send()
            halo_copy(r).wait_send()
    for step in range(n_tp - 1):
        stat_copy(step).wait_send()
    for p in range(chips):
        pair_copy(p).wait_send()
        if p:
            part_copy(p).wait_send()


def fused(cfg, tok_h, gain_h, wk_h, wg_h, wv_h, wq_h, wa_h, wb_h, ldt_h, hgain_h, ck_h, ng_h, ns_h, od_h, oc_h,
          out,
          gain, ldt, hgain, ck, ng, ns,
          tok, nt, wk, wv, wq, wab, wg, odg, ocg, ldo,
          keys, vals, betas, cums, xinv, gaps, rhs, local_out, reads, maps, ends,
          chain_in, chain_out, gout, gend, main_in, edge_in, pad, conv, stat_out, stat_in,
          dall, dm_out, call, acc_ab, acc_q, acc_k, acc_v,
          local_sem, g_send, g_recv, z_send, z_recv, t_send, ty_recv, tx_recv, tf_recv, tz_recv,
          ld_send, ld_recv, od_send, od_recv, chain_send, chain_recv,
          main_send, main_recv, edge_send, edge_recv, far_send, rim_send,
          stat_send, stat_recv, dg_send, dg_recv, df_send, df_recv, cg_send, cg_recv, cf_send, cf_recv):
    n_sp, n_tp, conv_total = cfg
    grp, sp, tp = lax.axis_index("grp"), lax.axis_index("sp"), lax.axis_index("tp")
    length, width = tok.shape
    rows = wk_h.shape[0]
    head_width = hgain.shape[1]
    cols = wk.shape[1]
    heads = cols // head_width
    channels = wab.shape[1] // 2
    columns = out.shape[1]
    units = [(j, h) for j in range(2) for h in range(heads)]
    n_units = len(units)
    pairs = [(u, r) for u in range(n_units) for r in range(2)]
    chip, core = tp // 2, lax.rem(tp, 2)
    chips = n_tp // 2
    sibling = tp + 1 - 2 * core
    other = 1 - grp
    edge = (sp == 0) | (sp == n_sp - 1)
    inner = (sp > 0) & (sp < n_sp - 1)
    helps = (sp == 1) | (sp == n_sp - 2)
    helper = jnp.where(sp == 0, 1, n_sp - 2)
    helped = jnp.where(sp == 1, 0, n_sp - 1)
    sources = (wk_h, wg_h, wv_h, wq_h, wa_h, wb_h)
    plain = {KEY: wk, VALUE: wv, QUERY: wq}

    def remote(src, dst, send, recv, **where):
        return pltpu.make_async_remote_copy(
            src_ref=src, dst_ref=dst, send_sem=send, recv_sem=recv, device_id=where, device_id_type=MESH
        )

    counts = (4, 1, 2, 2, 1, 1)
    firsts = (0, 0, 4, 6, 8, 9)

    def source(w):
        if w == GATE:
            return wg_h
        size = channels if w in (GLU, OPEN) else cols
        return sources[w].at[:, pl.ds(pl.multiple_of(grp * size, 128), size)]

    def target(w, index, k=None):
        if w == GATE:
            return wg.at[index]
        slab = rows // counts[w]
        if k is None:
            at = pl.ds(pl.multiple_of(index * rows, 16), rows)
        else:
            at = pl.ds(pl.multiple_of(index * rows + k * slab, 16), slab)
        if w in (GLU, OPEN):
            return wab.at[at, pl.ds(channels if w == OPEN else 0, channels)]
        return plain[w].at[at]

    barrier = pltpu.get_barrier_semaphore()

    def greet(**where):
        pl.semaphore_signal(barrier, inc=1, device_id=where, device_id_type=MESH)

    for step in range(n_tp - 1):
        peer = lax.rem(tp + step + 1, n_tp)
        greet(tp=peer)
        greet(tp=peer, grp=other)
    greet(grp=other)

    @pl.when(sp > 0)
    def _():
        greet(sp=sp - 1)
        greet(sp=sp - 1, grp=other)

    @pl.when(sp < n_sp - 1)
    def _():
        greet(sp=sp + 1)
        greet(sp=sp + 1, grp=other)

    load_tok = pltpu.make_async_copy(tok_h, tok, local_sem.at[0])
    load_tok.start()
    small = [
        pltpu.make_async_copy(src, dst, local_sem.at[9 + i])
        for i, (src, dst) in enumerate(
            ((gain_h, gain), (ldt_h, ldt), (hgain_h, hgain), (ng_h, ng), (ns_h, ns),
             (ck_h.at[:, pl.ds(0, channels)], ck.at[0]), (ck_h.at[:, pl.ds(channels, channels)], ck.at[1]))
        )
    ]
    for copy in small:
        copy.start()
    own = [pltpu.make_async_copy(source(w), target(w, sp), local_sem.at[1 + w]) for w in range(6)]
    for copy in own:
        copy.start()

    def od_rows(index):
        return pl.ds(pl.multiple_of(index * columns, 16), columns)

    load_od = pltpu.make_async_copy(od_h.at[od_rows(tp)], odg.at[tp], local_sem.at[7])
    load_oc = pltpu.make_async_copy(oc_h.at[od_rows(tp)], ocg.at[tp], local_sem.at[8])
    load_od.start()
    load_oc.start()

    load_tok.wait()
    for copy in small:
        copy.wait()
    chunk = 64
    for at in range(0, length, chunk):
        here = tok[at:at + chunk, :].astype(F32)
        scale = lax.rsqrt(jnp.mean(here * here, axis=-1, keepdims=True) + EPSILON)
        nt[at:at + chunk, :] = (here * scale * gain[...]).astype(BF16)

    for w in (GATE, KEY):
        own[w].wait()

    @pl.when(edge)
    def _():
        pl.semaphore_wait(barrier, 2 * n_tp + 1)

    @pl.when(inner)
    def _():
        pl.semaphore_wait(barrier, 2 * n_tp + 3)

    def wide(w):
        return 1 if w in (GLU, OPEN) else 0

    def arrives(w, side, d):
        ok = (sp - d >= 0) if side == 0 else (sp + d < n_sp)
        return ok & inner if wide(w) else ok

    def leaves(w, side, d):
        if side == 0:
            return (sp - (d - 1) >= 0) & (sp < n_sp - 1 - wide(w))
        return (sp + (d - 1) < n_sp) & (sp > wide(w))

    def origin(side, d):
        return sp - d if side == 0 else sp + d

    def z_block(w, index, side, k, here=False):
        ahead = sp + 1 if side == 0 else sp - 1
        place = target(w, index, k)
        slot = jnp.where(index > (sp if here else ahead), index - 1, index)
        if w == GATE:
            send, recv = g_send.at[side], g_recv.at[slot]
        else:
            send, recv = z_send.at[side], z_recv.at[slot, firsts[w] + k]
        return remote(place, place, send, recv, sp=ahead)

    def cuts(w):
        return range(counts[w])

    def offer(w, where, ks=None):
        for side in range(2):
            @pl.when(leaves(w, side, 1) & where)
            def _(side=side):
                for k in cuts(w) if ks is None else ks:
                    z_block(w, sp, side, k).start()

    def from_edge(side, d):
        return (sp - d == 0) if side == 0 else (sp + d == n_sp - 1)

    def relay(w, d, kind=None, ks=None):
        if d > n_sp - 1:
            return
        for k in cuts(w) if ks is None else ks:
            for side in range(2):
                onward = leaves(w, side, d + 1) if d < n_sp - 1 else sp < 0
                here = arrives(w, side, d) & onward
                if kind == "edge":
                    here = here & from_edge(side, d)
                if kind == "inner":
                    here = here & ~from_edge(side, d)

                @pl.when(here)
                def _(side=side, k=k):
                    z_block(w, origin(side, d), side, k, True).wait_recv()
                    z_block(w, origin(side, d), side, k).start()

    def drain(w, d):
        for k in cuts(w):
            for side in range(2):
                onward = leaves(w, side, d + 1) if d < n_sp - 1 else sp < 0

                @pl.when(arrives(w, side, d) & ~onward)
                def _(side=side, k=k):
                    z_block(w, origin(side, d), side, k, True).wait_recv()

    pieces = ty_recv.shape[0]
    half = length // 2
    piece = half // pieces
    grains = tz_recv.shape[0]
    grain = half // grains

    def part(block, side, c):
        size = grain if block > 1 else piece
        return nt.at[pl.ds(pl.multiple_of(block * length + side * half + c * size, 16), size)]

    def tok_y(k, c):
        return remote(
            part(2 * k, core, c), part(2 * k + 1, core, c), t_send.at[0], (ty_recv, tx_recv)[k].at[c], grp=other
        )

    def tok_z(c):
        src = nt.at[pl.ds(pl.multiple_of(core * half + c * grain, 16), grain)]
        return remote(src, part(2, core, c), t_send.at[0], tz_recv.at[c], sp=helper)

    def tok_f(block, c):
        return remote(
            part(block, core, c), part(block, core, c), t_send.at[0], tf_recv.at[block - 1], tp=sibling
        )

    def tok_f_arrival(block):
        place = nt.at[pl.ds(pl.multiple_of(block * length + (1 - core) * half, 16), half)]
        return remote(place, place, t_send.at[0], tf_recv.at[block - 1], tp=sibling)

    def sent_rows(count):
        place = nt.at[pl.ds(0, count * half)]
        return remote(place, place, t_send.at[0], t_send.at[0], tp=sibling)

    def pass_y(k, c):
        tok_y(k, c).wait_recv()
        tok_f(2 * k + 1, c).start()

    def pass_z(c):
        @pl.when(helps)
        def _():
            tok_z(c).wait_recv()
            tok_y(1, c).start()
            tok_f(2, c).start()

    def pass_far(c):
        @pl.when(helps)
        def _():
            pass_y(1, c)

    ld_copy = remote(ldt, ldo, ld_send.at[0], ld_recv.at[0], grp=other)

    def od_copy(m, step):
        dest = lax.rem(tp + step + 1, n_tp)
        src, dst = ((od_h, odg), (oc_h, ocg))[m]
        return remote(src.at[od_rows(dest)], dst.at[tp], od_send.at[m], od_recv.at[m], tp=dest)

    def od_all(m):
        place = (odg, ocg)[m].at[pl.ds(0, n_tp - 1)]
        return remote(place, place, od_send.at[m], od_recv.at[m], tp=sibling)

    everywhere = sp >= 0
    offer(GATE, everywhere)
    offer(KEY, everywhere)
    for c in range(pieces):
        tok_y(0, c).start()
    ld_copy.start()
    for w in (VALUE, GLU, OPEN, QUERY):
        own[w].wait()
    offer(VALUE, edge)
    offer(GLU, edge)
    for first in (0, grains // 2):
        @pl.when(edge)
        def _(first=first):
            for c in range(first, first + grains // 2):
                tok_z(c).start()

        if first == 0:
            offer(OPEN, edge)

    offer(QUERY, edge)
    for m in (1, 0):
        for step in range(n_tp - 1):
            od_copy(m, step).start()

    def dot(a, b, dims=NN):
        return lax.dot_general(a, b, dims, preferred_element_type=F32)

    def unit_rows(tensor):
        return tensor * lax.rsqrt(jnp.sum(tensor * tensor, axis=-1, keepdims=True) + EPSILON)

    def silu(tensor):
        return tensor * jax.nn.sigmoid(tensor)

    def block_dot(first, count, w_ref, index):
        lanes = pl.ds(pl.multiple_of(index * rows, 128), rows)
        at = pl.ds(pl.multiple_of(index * rows, 128), rows)
        return dot(nt[first * length:(first + count) * length, lanes], w_ref[at, :])

    def neighbours(w, d, action):
        for side in range(2):
            @pl.when(arrives(w, side, d))
            def _(side=side):
                action(sp - d if side == 0 else sp + d)

    def adder(acc, w_ref, first, count):
        span = slice(first * length, (first + count) * length)

        def add(index, fresh=False):
            x = block_dot(first, count, w_ref, index)
            acc[span, :] = x if fresh else acc[span, :] + x

        return add

    row_at = lax.broadcasted_iota(jnp.int32, (length, length), 0)
    col_at = lax.broadcasted_iota(jnp.int32, (length, length), 1)
    same = row_at == col_at
    mine = grp == 0
    gates = 4 * heads

    def weights_of(j):
        span = slice(j * length, (j + 1) * length)
        cols_part = jnp.zeros((length, wg.shape[1]), F32)
        for index in range(n_sp):
            cols_part = cols_part + dot(nt[span, index * rows:(index + 1) * rows], wg[index], NT)
        rows_part = jnp.transpose(cols_part)
        gate_cols = jnp.where(mine, cols_part[:, :gates], cols_part[:, gates:])
        gate_rows = jnp.where(mine, rows_part[:gates, :], rows_part[gates:, :])
        log = (ldt, ldo)[j]
        rates = jnp.where(mine, log[:2 * heads, :], log[2 * heads:, :])
        for h in range(heads):
            for r in range(2):
                p = 2 * (j * heads + h) + r
                g = 4 * h + 2 * r
                decay_row = rates[2 * h + r:2 * h + r + 1, :] * (0.5 + jax.nn.sigmoid(gate_rows[g:g + 1, :]))
                beta = jax.nn.sigmoid(gate_cols[:, g + 1:g + 2] - BETA_SHIFT)
                seen = col_at <= row_at if r == 0 else col_at >= row_at
                cum_col = jnp.sum(jnp.where(seen, decay_row, 0.0), axis=1, keepdims=True)
                cum_row = jnp.sum(jnp.where(same, cum_col, 0.0), axis=0, keepdims=True)
                gaps[p] = jnp.where(seen, jnp.exp(jnp.where(seen, cum_col - cum_row, 0.0)), 0.0)
                betas[p] = jnp.broadcast_to(beta, (length, head_width))
                cums[p] = jnp.broadcast_to(cum_col, (length, head_width))

    add_key = [adder(acc_k, wk, j, 1) for j in range(2)]
    add_value = [adder(acc_v, wv, j, 1) for j in range(2)]

    relay(GATE, 1)
    relay(KEY, 1, None, (0, 1))
    offer(VALUE, inner, (0,))
    relay(KEY, 1, None, (2, 3))
    offer(VALUE, inner, (1,))
    offer(GLU, inner)
    relay(GATE, 2)
    pass_y(0, 0)
    for d in range(2, n_sp - 1):
        relay(KEY, d, None, (0, 1))
    relay(VALUE, 1, None, (0,))
    for d in range(2, n_sp - 1):
        relay(KEY, d, None, (2, 3))
    pass_y(0, 1)
    relay(VALUE, 1, None, (1,))
    offer(OPEN, inner)
    def pass_value():
        for d in range(2, n_sp - 1):
            relay(VALUE, d)

    drain(KEY, 1)
    add_key[0](sp, True)
    neighbours(KEY, 1, add_key[0])
    pass_y(0, 2)
    offer(QUERY, inner)
    drain(VALUE, 1)
    add_value[0](sp, True)
    neighbours(VALUE, 1, add_value[0])
    relay(GLU, 1)
    for d in range(1, n_sp):
        drain(GATE, d)
    weights_of(0)
    pass_y(0, 3)
    for d in range(2, n_sp - 1):
        drain(KEY, d)
        neighbours(KEY, d, add_key[0])
    ld_copy.wait_recv()
    tok_f_arrival(1).wait_recv()
    pass_z(0)
    weights_of(1)
    pass_z(1)
    pass_z(2)
    add_key[1](sp, True)
    for d in range(1, n_sp - 1):
        neighbours(KEY, d, add_key[1])
    add_value[1](sp, True)
    neighbours(VALUE, 1, add_value[1])
    pass_z(3)
    drain(KEY, n_sp - 1)
    neighbours(KEY, n_sp - 1, adder(acc_k, wk, 0, 2))
    pass_value()

    both = 2 * length
    key_proj = silu(acc_k[...])
    for u, (j, h) in enumerate(units):
        keys[u] = unit_rows(key_proj[j * length:(j + 1) * length, h * head_width:(h + 1) * head_width])
    near = row_at // 2 == col_at // 2
    for u in range(n_units):
        grams = bdot(keys[u], keys[u], NT)
        for r in range(2):
            p = 2 * u + r
            beta = jnp.concatenate([betas[p]] * (length // head_width), axis=1)
            lower = jnp.where(same, 0.0, grams * gaps[p] * beta)
            rhs[p] = lower
            xinv[p] = jnp.where(same, 1.0, jnp.where(near, -lower, 0.0))

    service = {
        8: [lambda: relay(OPEN, 1)],
        32: [lambda: pass_z(4)],
        128: [lambda: pass_z(5)],
    }
    size = 2
    while size < length:
        inside = (row_at // (2 * size) == col_at // (2 * size)) & (row_at // size != col_at // size)
        for p in range(len(pairs)):
            across = jnp.where(inside, rhs[p], 0.0)
            inverse = xinv[p]
            xinv[p] = inverse - bdot(inverse, bdot(across, inverse))
        for act in service.get(size, ()):
            act()
        size *= 2

    for d in range(2, n_sp):
        drain(VALUE, d)
        neighbours(VALUE, d, adder(acc_v, wv, 0, 2))
    value_proj = silu(acc_v[...])
    eye = (
        lax.broadcasted_iota(jnp.int32, (head_width, head_width), 0)
        == lax.broadcasted_iota(jnp.int32, (head_width, head_width), 1)
    )
    for u, r in pairs:
        p = 2 * u + r
        j, h = units[u]
        beta, cum, key = betas[p], cums[p], keys[u]
        value = value_proj[j * length:(j + 1) * length, h * head_width:(h + 1) * head_width]
        total = cum[length - 1:length, :] if r == 0 else cum[0:1, :]
        right = jnp.concatenate([beta * value, beta * key * jnp.exp(cum)], axis=1)
        solved = bdot(xinv[p], right)
        vals[p] = solved.astype(BF16)
        passed = bdot(key * jnp.exp(total - cum), solved, TN)
        ends[p] = passed[:, :head_width]
        maps[p] = (jnp.where(eye, jnp.exp(total), 0.0) - passed[:, head_width:]).astype(BF16)

    def place_of(r):
        return sp if r == 0 else n_sp - 1 - sp

    def chain_copy(r):
        dest = sp + 1 if r == 0 else sp - 1
        return remote(chain_out.at[r], chain_in.at[r], chain_send.at[r], chain_recv.at[r], sp=dest)

    def chain_point(low, high):
        for r in range(2):
            at = place_of(r)

            @pl.when((at >= low) & (at <= high))
            def _(r=r, at=at):
                if low == 0:
                    for u in range(n_units):
                        chain_in[r, u] = jnp.zeros((head_width, head_width), BF16)
                        chain_out[r, u] = ends[2 * u + r].astype(BF16)
                else:
                    chain_copy(r).wait_recv()
                    for u in range(n_units):
                        p = 2 * u + r
                        chain_out[r, u] = (bdot(maps[p], chain_in[r, u]) + ends[p]).astype(BF16)

                @pl.when(at < n_sp - 1)
                def _():
                    chain_copy(r).start()

    chain_point(0, 0)
    pass_z(6)
    relay(QUERY, 1, "inner")
    add_near = adder(acc_ab, wab, 0, 2)
    add_query = adder(acc_q, wq, 0, 2)
    drain(GLU, 1)
    drain(OPEN, 1)

    @pl.when(inner)
    def _():
        add_near(sp, True)

    pass_z(7)
    for c in range(4):
        pass_far(c)
    neighbours(GLU, 1, add_near)
    relay(QUERY, 1, "edge", (0,))
    pass_far(4)
    relay(QUERY, 1, "edge", (1,))
    pass_far(5)
    for d in range(2, n_sp - 1):
        for w in (GLU, OPEN):
            relay(w, d)
            drain(w, d)
        neighbours(GLU, d, add_near)

    def gated(x):
        return (x[:, :channels] * jax.nn.sigmoid(x[:, channels:])).astype(BF16)

    def owner(j):
        return grp if j == 0 else other

    def main_y():
        return remote(gout, main_in.at[grp], main_send.at[0], main_recv.at[grp], grp=other)

    def main_arrival(h):
        return remote(main_in.at[h], main_in.at[h], main_send.at[0], main_recv.at[h], grp=other)

    def far_copy(j):
        return remote(gend.at[j], main_in.at[grp], far_send.at[0], main_recv.at[grp], sp=helped, grp=owner(j))

    def edge_copy(side, j):
        start = length - HALO if side == 0 else 0
        src = main_in.at[grp, pl.ds(start, HALO)] if j == 0 else gout.at[pl.ds(start, HALO)]
        return remote(
            src, edge_in.at[side, grp], edge_send.at[0], edge_recv.at[side, grp],
            sp=sp + 1 if side == 0 else sp - 1, grp=owner(j),
        )

    def rim_copy(side):
        start = length - HALO if side == 0 else 0
        return remote(
            gend.at[1, pl.ds(start, HALO)], edge_in.at[side, grp], rim_send.at[0], edge_recv.at[side, grp], grp=other
        )

    def edge_arrival(side, h):
        place = edge_in.at[side, h]
        return remote(place, place, edge_send.at[0], edge_recv.at[side, h], grp=other)

    @pl.when(inner)
    def _():
        near_rows = gated(acc_ab[...])
        main_in[grp] = near_rows[:length]
        gout[...] = near_rows[length:]
        main_y().start()
        for side in range(2):
            for j in range(2):
                edge_copy(side, j).start()

    def give_far(j):
        gend[j] = gated(dot(nt[(2 + j) * length:(3 + j) * length, :], wab[...]))
        far_copy(j).start()

    @pl.when(helps)
    def _():
        tok_f_arrival(2).wait_recv()
        give_far(0)
        for side, at in ((0, 1), (1, n_sp - 2)):
            @pl.when(sp == at)
            def _(side=side):
                start = length - HALO if side == 0 else 0
                edge_in[side, grp] = gend[0, start:start + HALO, :]

    pass_far(6)
    chain_point(1, 1)
    pass_far(7)

    @pl.when(helps)
    def _():
        tok_f_arrival(3).wait_recv()
        give_far(1)
        for side, at in ((0, 1), (1, n_sp - 2)):
            @pl.when(sp == at)
            def _(side=side):
                rim_copy(side).start()

    for d in range(2, n_sp - 1):
        relay(QUERY, d)
        chain_point(d, d)
    drain(QUERY, 1)
    add_query(sp, True)
    neighbours(QUERY, 1, add_query)
    for d in range(2, n_sp - 1):
        drain(QUERY, d)
        neighbours(QUERY, d, add_query)

    taps = ck.shape[1]
    for step in range(2):
        h = grp if step == 0 else other
        skip = sp < 0 if step else sp >= 0

        @pl.when(edge if step == 0 else sp >= 0)
        def _(h=h):
            main_arrival(h).wait_recv()

        @pl.when((sp > 0) & ~((sp == 1) & skip))
        def _(h=h):
            edge_arrival(0, h).wait_recv()

        @pl.when((sp < n_sp - 1) & ~((sp == n_sp - 2) & skip))
        def _(h=h):
            edge_arrival(1, h).wait_recv()

        pad[step, HALO:HALO + length, :] = main_in[h].astype(F32)
        for side, start, none in ((0, 0, 0), (1, HALO + length, n_sp - 1)):
            @pl.when(sp != none)
            def _(h=h, step=step, side=side, start=start):
                pad[step, start:start + HALO, :] = edge_in[side, h].astype(F32)

            @pl.when(sp == none)
            def _(step=step, start=start):
                pad[step, start:start + HALO, :] = jnp.zeros((HALO, channels), F32)

        for at in range(0, length, chunk):
            first = at + HALO - taps // 2
            total = pad[step, first:first + chunk, :] * ck[h, 0:1, :]
            for k in range(1, taps):
                total = total + pad[step, first + k:first + k + chunk, :] * ck[h, k:k + 1, :]
            conv[h, at:at + chunk, :] = total
    filtered = jnp.concatenate([conv[0], conv[1]], axis=1)
    sum_col = jnp.sum(filtered, axis=-1, keepdims=True)
    square_col = jnp.sum(filtered * filtered, axis=-1, keepdims=True)
    stat_out[...] = jnp.zeros(stat_out.shape, F32)
    stat_out[0:1, :] = jnp.sum(jnp.where(same, sum_col, 0.0), axis=0, keepdims=True)
    stat_out[1:2, :] = jnp.sum(jnp.where(same, square_col, 0.0), axis=0, keepdims=True)

    def stat_copy(step):
        return remote(
            stat_out, stat_in.at[step], stat_send.at[0], stat_recv.at[0], tp=lax.rem(tp + step + 1, n_tp)
        )

    for step in range(n_tp - 1):
        stat_copy(step).start()

    def chip_at(q):
        return lax.rem(chip + q, chips)

    def chip_back(q):
        return lax.rem(chip + chips - q, chips)

    def dg_copy(a, q):
        src = dall.at[tp, grp] if a == 0 else dm_out
        where = {"tp": chip_at(q) * 2 + core}
        if a:
            where["grp"] = other
        return remote(src, dall.at[tp, grp], dg_send.at[a], dg_recv.at[a, q], **where)

    def d_block(a, q, side):
        return dall.at[chip_back(q) * 2 + side, other if a else grp]

    def dg_arrival(a, q):
        place = d_block(a, q, core)
        return remote(place, place, dg_send.at[a], dg_recv.at[a, q], tp=sibling)

    def df_copy(a, q):
        place = d_block(a, q, core)
        return remote(place, place, df_send.at[0], df_recv.at[q], tp=sibling)

    def df_arrival(q):
        place = dall.at[chip_back(q) * 2 + 1 - core]
        return remote(place, place, df_send.at[0], df_recv.at[q], tp=sibling)

    def cg_copy(q):
        return remote(call.at[tp], call.at[tp], cg_send.at[0], cg_recv.at[q], tp=chip_at(q) * 2 + core)

    def cg_arrival(q):
        place = call.at[chip_back(q) * 2 + core]
        return remote(place, place, cg_send.at[0], cg_recv.at[q], tp=sibling)

    def cf_copy(q, arriving=False):
        place = call.at[chip_back(q) * 2 + (1 - core if arriving else core)]
        return remote(place, place, cf_send.at[0], cf_recv.at[q], tp=sibling)

    stats = stat_out[0:2, :]
    stat_all = remote(stat_in, stat_in, stat_send.at[0], stat_recv.at[0], tp=sibling)
    stat_all.wait_recv()
    for step in range(n_tp - 1):
        stats = stats + stat_in[step, 0:2, :]
    center = jnp.sum(jnp.where(same, stats[0:1, :], 0.0), axis=1, keepdims=True) / conv_total
    squares = jnp.sum(jnp.where(same, stats[1:2, :], 0.0), axis=1, keepdims=True) / conv_total
    spread = squares - center * center
    normal = (jnp.concatenate([conv[0], conv[1]], axis=1) - center) * lax.rsqrt(spread + EPSILON)
    call[tp] = silu(normal * ng[...] + ns[...]).astype(BF16)
    for q in range(1, chips):
        cg_copy(q).start()
    cf_copy(0).start()

    def delta_term(t):
        return dot(jnp.concatenate([dall[t, 0], dall[t, 1]], axis=1), odg[t], NT)

    def conv_term(t):
        return dot(call[t], ocg[t], NT)

    drain(QUERY, n_sp - 1)
    neighbours(QUERY, n_sp - 1, add_query)

    def read(u):
        j, h = units[u]
        query = silu(acc_q[j * length:(j + 1) * length, h * head_width:(h + 1) * head_width])
        query = unit_rows(query) * head_width ** -0.5
        scores = bdot(query, keys[u], NT)
        for r in range(2):
            p = 2 * u + r
            pair = dot((scores * gaps[p]).astype(BF16), vals[p])
            reads[p] = (query * jnp.exp(cums[p]) - pair[:, head_width:]).astype(BF16)
            if r == 0:
                local_out[u] = pair[:, :head_width]
            else:
                local_out[u] = local_out[u] + pair[:, :head_width]

    def mixed_head(u):
        joined = local_out[u] + dot(reads[2 * u], chain_in[0, u]) + dot(reads[2 * u + 1], chain_in[1, u])
        scale = lax.rsqrt(jnp.mean(joined * joined, axis=-1, keepdims=True) + EPSILON)
        return (joined * scale * hgain[...]).astype(BF16)

    direct = [(a, q) for q in range(chips) for a in (1, 0) if (a, q) != (0, 0)]

    for u in range(n_units):
        read(u)
    chain_point(n_sp - 1, n_sp - 1)
    for h in range(heads):
        dm_out[:, h * head_width:(h + 1) * head_width] = mixed_head(heads + h)
    for q in range(chips - 1, -1, -1):
        dg_copy(1, q).start()
    for h in range(heads):
        dall[tp, grp, :, h * head_width:(h + 1) * head_width] = mixed_head(h)
    for q in range(1, chips):
        dg_copy(0, q).start()
    df_copy(0, 0).start()

    for m in range(2):
        od_all(m).wait_recv()
    load_od.wait()
    load_oc.wait()
    result = conv_term(tp)
    for q in range(1, chips):
        cg_arrival(q).wait_recv()
        cf_copy(q).start()
    for q in range(1, chips):
        result = result + conv_term(chip_back(q) * 2 + core)
    for a, q in direct:
        dg_arrival(a, q).wait_recv()
        df_copy(a, q).start()
        if (a, q) == (1, 0):
            for p in range(chips):
                cf_copy(p, True).wait_recv()
                result = result + conv_term(chip_back(p) * 2 + 1 - core)
            result = result + delta_term(tp)
    for q in range(1, chips):
        result = result + delta_term(chip_back(q) * 2 + core)
    for q in range(chips):
        df_arrival(q).wait_recv()
        result = result + delta_term(chip_back(q) * 2 + 1 - core)
    out[...] = result.astype(BF16)

    for side in range(2):
        for q in range(n_sp):
            far = n_sp - 1 if side == 0 else 0
            copies = 0 if q == far else (q + 1 if side == 0 else n_sp - q)
            wide_to = n_sp - 2 if side == 0 else 1
            wide_copies = copies if (q < wide_to if side == 0 else q > wide_to) else 0
            if copies:
                @pl.when(sp == q)
                def _(side=side, copies=copies, wide_copies=wide_copies):
                    place = wg.at[pl.ds(0, copies)]
                    remote(place, place, g_send.at[side], g_send.at[side], tp=sibling).wait_send()
                    total = (3 * cols * copies + 2 * channels * wide_copies) * rows // width
                    place = nt.at[pl.ds(0, total)]
                    remote(place, place, z_send.at[side], z_send.at[side], tp=sibling).wait_send()
    @pl.when(edge)
    def _():
        sent_rows(3).wait_send()

    @pl.when(inner & ~helps)
    def _():
        sent_rows(2).wait_send()

    @pl.when(helps)
    def _():
        sent_rows(5).wait_send()
        remote(gend, gend, far_send.at[0], far_send.at[0], tp=sibling).wait_send()
        rim_copy(0).wait_send()

    ld_copy.wait_send()
    for m in range(2):
        od_all(m).wait_send()
    for r in range(2):
        @pl.when(place_of(r) < n_sp - 1)
        def _(r=r):
            chain_copy(r).wait_send()

    @pl.when(inner)
    def _():
        main_y().wait_send()
        remote(edge_in, edge_in, edge_send.at[0], edge_send.at[0], tp=sibling).wait_send()

    stat_all.wait_send()
    place = dall.at[pl.ds(0, chips), 0]
    remote(place, place, dg_send.at[1], dg_send.at[1], tp=sibling).wait_send()
    if chips > 1:
        place = dall.at[pl.ds(0, chips - 1), 0]
        remote(place, place, dg_send.at[0], dg_send.at[0], tp=sibling).wait_send()
        place = call.at[pl.ds(0, chips - 1)]
        remote(place, place, cg_send.at[0], cg_send.at[0], tp=sibling).wait_send()
    place = dall.at[pl.ds(0, chips)]
    remote(place, place, df_send.at[0], df_send.at[0], tp=sibling).wait_send()
    place = call.at[pl.ds(0, chips)]
    remote(place, place, cf_send.at[0], cf_send.at[0], tp=sibling).wait_send()


def solution(mesh):
    n_grp, n_sp, n_tp = mesh.shape["grp"], mesh.shape["sp"], mesh.shape["tp"]

    def on_device(tokens_in, input_gain, w_query, w_key, w_value, w_gates, w_glu_value,
                  sigmoid_opener_matrix, log_decay, head_gain, conv_kernel, norm_gain, norm_shift,
                  out_delta, out_conv):
        length, width = tokens_in.shape
        head_width = head_gain.shape[0]
        head_cols = w_query.shape[1]
        heads = head_cols // head_width
        channels = w_glu_value.shape[1]
        rows = w_query.shape[0]
        pairs = 2 * heads
        columns = width // n_tp
        dma, vmem = pltpu.SemaphoreType.DMA, pltpu.VMEM
        anywhere = pl.BlockSpec(memory_space=pltpu.HBM)
        inside = pl.BlockSpec(memory_space=pltpu.VMEM)
        if n_grp == 2 and n_sp >= 4 and n_tp % 2 == 0 and heads % 2 == 0 and channels % 256 == 0                 and (3 * head_cols + 2 * channels) * rows * n_sp <= 8 * length * width:
            cols, ch, chips, steps = head_cols // 2, channels // 2, n_tp // 2, n_tp - 1
            pieces = 4
            scratch = [
                vmem((1, width), F32), vmem((pairs, length), F32), vmem((1, head_width), F32),
                vmem((2, conv_kernel.shape[0], ch), F32), vmem((1, channels), F32), vmem((1, channels), F32),
                vmem((length, width), BF16), vmem((4 * length, width), BF16),
                vmem((width, cols), BF16), vmem((width, cols), BF16), vmem((width, cols), BF16),
                vmem((width, 2 * ch), BF16), vmem((n_sp, 4 * heads, rows), BF16),
                vmem((n_tp, columns, head_cols), BF16), vmem((n_tp, columns, channels), BF16),
                vmem((pairs, length), F32),
                vmem((heads, length, head_width), F32), vmem((pairs, length, 2 * head_width), BF16),
                vmem((pairs, length, head_width), F32), vmem((pairs, length, head_width), F32),
                vmem((pairs, length, length), F32), vmem((pairs, length, length), F32),
                vmem((pairs, length, length), F32),
                vmem((heads, length, head_width), F32), vmem((pairs, length, head_width), BF16),
                vmem((pairs, head_width, head_width), BF16), vmem((pairs, head_width, head_width), F32),
                vmem((2, heads, head_width, head_width), BF16), vmem((2, heads, head_width, head_width), BF16),
                vmem((length, ch), BF16), vmem((2, length, ch), BF16), vmem((2, length, ch), BF16),
                vmem((2, 2, HALO, ch), BF16),
                vmem((2, length + 2 * HALO, ch), F32), vmem((2, length, ch), F32),
                vmem((8, length), F32), vmem((steps, 8, length), F32),
                vmem((n_tp, 2, length, cols), BF16), vmem((length, cols), BF16),
                vmem((n_tp, length, channels), BF16), vmem((2 * length, 2 * ch), F32), vmem((2 * length, cols), F32),
                vmem((2 * length, cols), F32), vmem((2 * length, cols), F32),
                dma((16,)),
                dma((2,)), dma((n_sp - 1,)), dma((2,)), dma((n_sp - 1, 10)),
                dma((1,)), dma((pieces,)), dma((2 * pieces,)), dma((3,)), dma((2 * pieces,)),
                dma((1,)), dma((1,)), dma((2,)), dma((2,)), dma((2,)), dma((2,)),
                dma((1,)), dma((2,)), dma((1,)), dma((2, 2)), dma((1,)), dma((1,)),
                dma((1,)), dma((1,)),
                dma((2,)), dma((2, chips)), dma((1,)), dma((chips,)),
                dma((1,)), dma((chips,)), dma((1,)), dma((chips,)),
            ]
            return pl.pallas_call(
                functools.partial(fused, (n_sp, n_tp, float(channels * n_tp))),
                out_shape=pltpu.VMEM((length, columns), BF16),
                in_specs=[anywhere] * 15,
                out_specs=inside,
                scratch_shapes=scratch,
                compiler_params=pltpu.CompilerParams(
                    collective_id=0, has_side_effects=True, vmem_limit_bytes=58 * 1024 * 1024
                ),
            )(
                tokens_in, input_gain.reshape(1, width), w_key, w_gates.T, w_value, w_query,
                w_glu_value, sigmoid_opener_matrix, log_decay.T,
                head_gain.reshape(1, head_width), conv_kernel, norm_gain.reshape(1, channels),
                norm_shift.reshape(1, channels), out_delta, out_conv,
            )
        scratch = [
            vmem((length, width), BF16), vmem((length, width), BF16),
            vmem((width, head_cols), BF16), vmem((n_sp, 4 * heads, rows), BF16),
            vmem((width, head_cols), BF16), vmem((width, head_cols), BF16),
            vmem((width, channels), BF16), vmem((width, channels), BF16),
            vmem((width, head_cols), BF16), vmem((width, channels), BF16),
            vmem((heads, length, head_width), F32), vmem((pairs, length, 2 * head_width), BF16),
            vmem((pairs, length, head_width), F32), vmem((pairs, length, head_width), F32),
            vmem((pairs, length, length), F32), vmem((pairs, length, length), F32),
            vmem((pairs, length, length), F32),
            vmem((heads, length, head_width), F32), vmem((pairs, length, head_width), BF16),
            vmem((pairs, head_width, head_width), BF16), vmem((pairs, head_width, head_width), F32),
            vmem((2, heads, head_width, head_width), BF16), vmem((2, heads, head_width, head_width), BF16),
            vmem((length, channels), BF16), vmem((2, HALO, channels), BF16),
            vmem((length + 2 * HALO, channels), F32), vmem((length, channels), F32),
            vmem((8, length), F32), vmem((n_tp - 1, 8, length), F32),
            vmem((n_tp, length, columns), F32),
            vmem((n_tp // 2, length, columns), BF16), vmem((n_tp // 2, length, columns), BF16),
            vmem((n_tp // 2, length, columns), BF16), vmem((n_tp // 2, length, columns), BF16),
            dma((9,)),
            dma((6, 2, n_sp - 1)), dma((6, 2, n_sp - 1)),
            dma((6, 2, n_sp - 1)), dma((6, 2, n_sp - 1)),
            dma((2,)), dma((2,)), dma((2,)), dma((2,)),
            dma((n_tp - 1,)), dma((n_tp - 1,)), dma((n_tp // 2,)), dma((n_tp // 2,)),
            dma((n_tp // 2,)), dma((n_tp // 2,)),
        ]
        return pl.pallas_call(
            functools.partial(kernel, (n_grp, n_sp, n_tp, float(channels * n_tp))),
            out_shape=jax.ShapeDtypeStruct((length, columns), BF16),
            in_specs=[anywhere, inside] + [anywhere] * 6 + [inside] * 6 + [anywhere] * 2,
            out_specs=inside,
            scratch_shapes=scratch,
            compiler_params=pltpu.CompilerParams(
                collective_id=0, has_side_effects=True, vmem_limit_bytes=60 * 1024 * 1024
            ),
        )(
            tokens_in, input_gain.reshape(1, width), w_key, w_gates.T, w_value, w_query,
            w_glu_value, sigmoid_opener_matrix, log_decay, log_decay.T,
            head_gain.reshape(1, head_width), conv_kernel, norm_gain.reshape(1, channels),
            norm_shift.reshape(1, channels), out_delta, out_conv,
        )

    placed = (
        P(("grp", "sp"), None), P(), P("sp", "tp"), P("sp", "tp"), P("sp", "tp"), P("sp", "tp"),
        P("sp", "tp"), P("sp", "tp"), P(("grp", "sp"), "tp"), P(), P(None, "tp"), P("tp"), P("tp"),
        P(None, "tp"), P(None, "tp"),
    )
    return jax.shard_map(
        on_device, mesh=mesh, in_specs=placed, out_specs=P(("grp", "sp"), "tp"), check_vma=False
    )
```

```python
import functools

import jax
import jax.numpy as jnp
from jax import lax
from jax.experimental import pallas as pl
from jax.experimental.pallas import tpu as pltpu
from jax.sharding import PartitionSpec as P

EPSILON = 1e-06
BETA_SHIFT = 6.0
HALO = 16
MESH = pl.DeviceIdType.MESH
F32 = jnp.float32
BF16 = jnp.bfloat16
NT = (((1,), (1,)), ((), ()))
TN = (((0,), (0,)), ((), ()))
NN = (((1,), (0,)), ((), ()))
KEY, GATE, VALUE, QUERY, GLU, OPEN = range(6)


def bdot(left, right, dims=NN):
    return lax.dot_general(
        left.astype(BF16), right.astype(BF16), dims, preferred_element_type=F32
    )


def each(count, action):
    if count <= 8:
        for step in range(count):
            action(step)
    else:
        def body(step, carry):
            action(step)
            return carry

        lax.fori_loop(0, count, body, 0)


def kernel(cfg, tok_h, gain, wk_h, wg_h, wv_h, wq_h, wa_h, wb_h, ld, ldt, hgain, ck, ng, ns, od_h, oc_h,
           out,
           tok, normed, wk, wg, wv, wq, wa, wb, od, oc,
           keys, vals, betas, cums, xinv, gaps, rhs, local_out, reads, maps, ends,
           chain_in, chain_out, glu, halo, pad, conv, stat_out, stat_in, conv_acc, part_out, part_in, pair_out, pair_in,
           local_sem, z_send, z_recv, y_send, y_recv, chain_send, chain_recv,
           halo_send, halo_recv, stat_send, stat_recv, part_send, part_recv, pair_send, pair_recv):
    n_grp, n_sp, n_tp, conv_total = cfg
    grp, sp, tp = lax.axis_index("grp"), lax.axis_index("sp"), lax.axis_index("tp")
    length, width = tok.shape
    rows = wk_h.shape[0]
    channels = wa.shape[1]
    head_width = hgain.shape[1]
    heads = wk.shape[1] // head_width
    share = (rows // 2) // 16 * 16 if n_grp == 2 else 0
    pulled = rows - share

    sources = (wk_h, wg_h, wv_h, wq_h, wa_h, wb_h)
    targets = (wk, wg, wv, wq, wa, wb)

    def block_of(w, index, start, count):
        if w == GATE:
            return targets[w].at[index]
        return targets[w].at[pl.ds(pl.multiple_of(index * rows + start, 16), count)]

    load_tok = pltpu.make_async_copy(tok_h, tok, local_sem.at[0])
    load_tok.start()
    own = [
        pltpu.make_async_copy(sources[w], block_of(w, sp, 0, rows), local_sem.at[1 + w])
        for w in range(6)
    ]
    for copy in own:
        copy.start()
    load_od = pltpu.make_async_copy(od_h, od, local_sem.at[7])
    load_oc = pltpu.make_async_copy(oc_h, oc, local_sem.at[8])

    barrier = pltpu.get_barrier_semaphore()

    def greet(axis, me, count):
        def one(step):
            pl.semaphore_signal(
                barrier, inc=1, device_id={axis: lax.rem(me + step + 1, count)}, device_id_type=MESH
            )

        each(count - 1, one)

    greet("sp", sp, n_sp)
    greet("tp", tp, n_tp)
    greet("grp", grp, n_grp)
    pl.semaphore_wait(barrier, n_sp + n_tp + n_grp - 3)

    def origin(side, d):
        return sp - d if side == 0 else sp + d

    def arrives(side, d):
        return sp - d >= 0 if side == 0 else sp + d < n_sp

    def leaves(side, d):
        if side == 0:
            return (sp - (d - 1) >= 0) & (sp < n_sp - 1)
        return (sp + (d - 1) < n_sp) & (sp > 0)

    def part_of(w, index, side_of):
        if w == GATE:
            return block_of(w, index, 0, 0)
        if not share:
            return block_of(w, index, 0, rows)
        if side_of is None:
            return block_of(w, index, pl.multiple_of(grp * share, 16), pulled)
        return block_of(w, index, pl.multiple_of(side_of * pulled, 16), share)

    def z_copy(w, side, d, first=False):
        target = part_of(w, origin(side, d - 1), None)
        source = target
        if first:
            source = sources[w]
            if w != GATE and share:
                source = source.at[pl.ds(pl.multiple_of(grp * share, 16), pulled)]
        return pltpu.make_async_remote_copy(
            src_ref=source, dst_ref=target,
            send_sem=z_send.at[w, side, d - 1], recv_sem=z_recv.at[w, side, d - 1],
            device_id={"sp": sp + 1 if side == 0 else sp - 1}, device_id_type=MESH,
        )

    def z_arrival(w, side, d):
        place = part_of(w, origin(side, d), None)
        return pltpu.make_async_remote_copy(
            src_ref=place, dst_ref=place,
            send_sem=z_send.at[w, side, d - 1], recv_sem=z_recv.at[w, side, d - 1],
            device_id={"sp": sp + 1 if side == 0 else sp - 1}, device_id_type=MESH,
        )

    def y_copy(w, side, d, arriving=False):
        place = part_of(w, origin(side, d), 1 - grp if arriving else grp)
        return pltpu.make_async_remote_copy(
            src_ref=place, dst_ref=place,
            send_sem=y_send.at[w, side, d - 1], recv_sem=y_recv.at[w, side, d - 1],
            device_id={"grp": 1 - grp}, device_id_type=MESH,
        )

    def offer(w):
        for side in range(2):
            @pl.when(leaves(side, 1))
            def _(side=side):
                z_copy(w, side, 1, True).start()

    def relay_hop(w, d):
        for side in range(2):
            @pl.when(arrives(side, d))
            def _(side=side):
                z_arrival(w, side, d).wait_recv()

                @pl.when(leaves(side, d + 1))
                def _():
                    z_copy(w, side, d + 1).start()

                if share and w != GATE:
                    y_copy(w, side, d).start()

    def relay(w, low=1, high=None):
        if high is None:
            each(n_sp - low, lambda step: relay_hop(w, step + low))
        else:
            for d in range(low, min(high, n_sp - 1) + 1):
                relay_hop(w, d)

    def complete(w):
        own[w].wait()
        if share and w != GATE:
            def one(step):
                for side in range(2):
                    @pl.when(arrives(side, step + 1))
                    def _(side=side):
                        y_copy(w, side, step + 1, True).wait_recv()

            each(n_sp - 1, one)

    offer(KEY)
    offer(GATE)
    offer(VALUE)
    load_od.start()
    load_oc.start()

    load_tok.wait()
    chunk = 64
    for at in range(0, length, chunk):
        here = tok[at:at + chunk, :].astype(F32)
        scale = lax.rsqrt(jnp.mean(here * here, axis=-1, keepdims=True) + EPSILON)
        normed[at:at + chunk, :] = (here * scale * gain[...]).astype(BF16)

    def project(w):
        return jnp.dot(normed[...], targets[w][...], preferred_element_type=F32)

    def unit_rows(tensor):
        return tensor * lax.rsqrt(jnp.sum(tensor * tensor, axis=-1, keepdims=True) + EPSILON)

    def silu(tensor):
        return tensor * jax.nn.sigmoid(tensor)

    relay(GATE)
    relay(KEY)
    offer(QUERY)
    complete(GATE)
    gate_cols = jnp.zeros((length, 4 * heads), F32)
    gate_rows = jnp.zeros((4 * heads, length), F32)
    for index in range(n_sp):
        normed_part = normed[:, index * rows:(index + 1) * rows]
        gate_cols = gate_cols + lax.dot_general(normed_part, wg[index], NT, preferred_element_type=F32)
        gate_rows = gate_rows + lax.dot_general(wg[index], normed_part, NT, preferred_element_type=F32)

    row_at = lax.broadcasted_iota(jnp.int32, (length, length), 0)
    col_at = lax.broadcasted_iota(jnp.int32, (length, length), 1)

    complete(KEY)
    key_proj = silu(project(KEY))
    pairs = [(h, r) for h in range(heads) for r in range(2)]
    for h in range(heads):
        keys[h] = unit_rows(key_proj[:, h * head_width:(h + 1) * head_width])
    relay(VALUE, 1, 1)
    for h in range(heads):
        grams = bdot(keys[h], keys[h], NT)
        for r in range(2):
            p = 2 * h + r
            decay_col = ld[:, p:p + 1] * (0.5 + jax.nn.sigmoid(gate_cols[:, 2 * p:2 * p + 1]))
            decay_row = ldt[p:p + 1, :] * (0.5 + jax.nn.sigmoid(gate_rows[2 * p:2 * p + 1, :]))
            beta = jax.nn.sigmoid(gate_cols[:, 2 * p + 1:2 * p + 2] - BETA_SHIFT)
            if r == 0:
                seen_down, seen_across = row_at <= col_at, col_at <= row_at
            else:
                seen_down, seen_across = row_at >= col_at, col_at >= row_at
            cum_row = jnp.sum(jnp.where(seen_down, decay_col, 0.0), axis=0, keepdims=True)
            cum_col = jnp.sum(jnp.where(seen_across, decay_row, 0.0), axis=1, keepdims=True)
            weighting = jnp.where(
                seen_across, jnp.exp(jnp.where(seen_across, cum_col - cum_row, 0.0)), 0.0
            )
            gaps[p] = weighting
            betas[p] = jnp.broadcast_to(beta, (length, head_width))
            cums[p] = jnp.broadcast_to(cum_col, (length, head_width))
            lower = jnp.where(row_at != col_at, grams * weighting * beta, 0.0)
            rhs[p] = lower
            near = (row_at // 2 == col_at // 2)
            xinv[p] = jnp.where(row_at == col_at, 1.0, jnp.where(near, -lower, 0.0))

    size = 2
    while size < length:
        inside = (row_at // (2 * size) == col_at // (2 * size)) & (row_at // size != col_at // size)
        for p in range(len(pairs)):
            across = jnp.where(inside, rhs[p], 0.0)
            inverse = xinv[p]
            xinv[p] = inverse - bdot(inverse, bdot(across, inverse))
        if size == 2:
            relay(VALUE, 2)
            offer(GLU)
        if size == 32:
            relay(QUERY, 1, 1)
        if size == 128:
            relay(QUERY, 2, 2)
        size *= 2

    complete(VALUE)
    value_proj = silu(project(VALUE))
    eye = (
        lax.broadcasted_iota(jnp.int32, (head_width, head_width), 0)
        == lax.broadcasted_iota(jnp.int32, (head_width, head_width), 1)
    )
    for h, r in pairs:
        p = 2 * h + r
        beta, cum, key = betas[p], cums[p], keys[h]
        value = value_proj[:, h * head_width:(h + 1) * head_width]
        total = cum[length - 1:length, :] if r == 0 else cum[0:1, :]
        right = jnp.concatenate([beta * value, beta * key * jnp.exp(cum)], axis=1)
        solved = bdot(xinv[p], right)
        vals[p] = solved.astype(BF16)
        passed = bdot(key * jnp.exp(total - cum), solved, TN)
        ends[p] = passed[:, :head_width]
        maps[p] = (jnp.where(eye, jnp.exp(total), 0.0) - passed[:, head_width:]).astype(BF16)

    def place_of(r):
        return sp if r == 0 else n_sp - 1 - sp

    def chain_copy(r):
        dest = lax.rem(sp + 1, n_sp) if r == 0 else lax.rem(sp + n_sp - 1, n_sp)
        return pltpu.make_async_remote_copy(
            src_ref=chain_out.at[r], dst_ref=chain_in.at[r],
            send_sem=chain_send.at[r], recv_sem=chain_recv.at[r],
            device_id={"sp": dest}, device_id_type=MESH,
        )

    def chain_point(low, high):
        for r in range(2):
            at = place_of(r)

            @pl.when((at >= low) & (at <= high))
            def _(r=r, at=at):
                if low == 0:
                    for h in range(heads):
                        chain_in[r, h] = jnp.zeros((head_width, head_width), BF16)
                        chain_out[r, h] = ends[2 * h + r].astype(BF16)
                else:
                    chain_copy(r).wait_recv()
                    for h in range(heads):
                        p = 2 * h + r
                        chain_out[r, h] = (bdot(maps[p], chain_in[r, h]) + ends[p]).astype(BF16)

                @pl.when(at < n_sp - 1)
                def _():
                    chain_copy(r).start()

    chain_point(0, 0)
    relay(QUERY, 3)
    offer(OPEN)
    relay(GLU, 1, 1)
    complete(QUERY)
    query_proj = silu(project(QUERY))
    for h in range(heads):
        query = unit_rows(query_proj[:, h * head_width:(h + 1) * head_width]) * head_width ** -0.5
        scores = bdot(query, keys[h], NT)
        for r in range(2):
            p = 2 * h + r
            both = jnp.dot((scores * gaps[p]).astype(BF16), vals[p], preferred_element_type=F32)
            reads[p] = (query * jnp.exp(cums[p]) - both[:, head_width:]).astype(BF16)
            if r == 0:
                local_out[h] = both[:, :head_width]
            else:
                local_out[h] = local_out[h] + both[:, :head_width]
    chain_point(1, 1)
    relay(GLU, 2, 2)
    chain_point(2, 2)
    relay(GLU, 3)
    relay(OPEN, 1, 1)
    chain_point(3, n_sp - 1)
    complete(GLU)
    glu_proj = project(GLU)
    relay(OPEN, 2)
    complete(OPEN)
    gated = (glu_proj * jax.nn.sigmoid(project(OPEN))).astype(BF16)
    glu[...] = gated
    pad[HALO:HALO + length, :] = gated.astype(F32)

    def halo_copy(r):
        start = length - HALO if r == 0 else 0
        dest = lax.rem(sp + 1, n_sp) if r == 0 else lax.rem(sp + n_sp - 1, n_sp)
        return pltpu.make_async_remote_copy(
            src_ref=glu.at[pl.ds(start, HALO)], dst_ref=halo.at[r],
            send_sem=halo_send.at[r], recv_sem=halo_recv.at[r],
            device_id={"sp": dest}, device_id_type=MESH,
        )

    for r in range(2):
        @pl.when(place_of(r) < n_sp - 1)
        def _(r=r):
            halo_copy(r).start()
    for r in range(2):
        start = 0 if r == 0 else HALO + length

        @pl.when(place_of(r) > 0)
        def _(r=r, start=start):
            halo_copy(r).wait_recv()
            pad[start:start + HALO, :] = halo[r].astype(F32)

        @pl.when(place_of(r) == 0)
        def _(start=start):
            pad[start:start + HALO, :] = jnp.zeros((HALO, channels), F32)

    taps = ck.shape[0]
    for at in range(0, length, chunk):
        first = at + HALO - taps // 2
        total = pad[first:first + chunk, :] * ck[0:1, :]
        for j in range(1, taps):
            total = total + pad[first + j:first + j + chunk, :] * ck[j:j + 1, :]
        conv[at:at + chunk, :] = total
    filtered = conv[...]
    sum_col = jnp.sum(filtered, axis=-1, keepdims=True)
    square_col = jnp.sum(filtered * filtered, axis=-1, keepdims=True)
    same = row_at == col_at
    stat_out[...] = jnp.zeros(stat_out.shape, F32)
    stat_out[0:1, :] = jnp.sum(jnp.where(same, sum_col, 0.0), axis=0, keepdims=True)
    stat_out[1:2, :] = jnp.sum(jnp.where(same, square_col, 0.0), axis=0, keepdims=True)

    def stat_copy(step):
        return pltpu.make_async_remote_copy(
            src_ref=stat_out, dst_ref=stat_in.at[step],
            send_sem=stat_send.at[step], recv_sem=stat_recv.at[step],
            device_id={"tp": lax.rem(tp + step + 1, n_tp)}, device_id_type=MESH,
        )

    for step in range(n_tp - 1):
        stat_copy(step).start()

    joined_heads = []
    for h in range(heads):
        joined = local_out[h] + jnp.dot(reads[2 * h], chain_in[0, h], preferred_element_type=F32)
        joined = joined + jnp.dot(reads[2 * h + 1], chain_in[1, h], preferred_element_type=F32)
        scale = lax.rsqrt(jnp.mean(joined * joined, axis=-1, keepdims=True) + EPSILON)
        joined_heads.append((joined * scale * hgain[...]).astype(BF16))
    delta_mix = jnp.concatenate(joined_heads, axis=1) if heads > 1 else joined_heads[0]
    load_od.wait()
    load_oc.wait()
    columns = width // n_tp
    for dest in range(n_tp):
        at = slice(dest * columns, (dest + 1) * columns)
        conv_acc[dest] = lax.dot_general(delta_mix, od[at, :], NT, preferred_element_type=F32)

    stats = stat_out[0:2, :]
    for step in range(n_tp - 1):
        stat_copy(step).wait_recv()
        stats = stats + stat_in[step, 0:2, :]
    center = jnp.sum(jnp.where(same, stats[0:1, :], 0.0), axis=1, keepdims=True) / conv_total
    squares = jnp.sum(jnp.where(same, stats[1:2, :], 0.0), axis=1, keepdims=True) / conv_total
    spread = squares - center * center
    normal = (filtered - center) * lax.rsqrt(spread + EPSILON)
    conv_mix = silu(normal * ng[...] + ns[...]).astype(BF16)

    chip, core = tp // 2, lax.rem(tp, 2)
    chips = n_tp // 2
    sibling = chip * 2 + 1 - core

    def there(p, place):
        return lax.rem(chip + p, chips) * 2 + place

    def term_of(dest):
        at = pl.ds(pl.multiple_of(dest * columns, 16), columns)
        return conv_acc[dest] + lax.dot_general(conv_mix, oc[at, :], NT, preferred_element_type=F32)

    def pair_copy(p):
        return pltpu.make_async_remote_copy(
            src_ref=pair_out.at[p], dst_ref=pair_in.at[p],
            send_sem=pair_send.at[p], recv_sem=pair_recv.at[p],
            device_id={"tp": sibling}, device_id_type=MESH,
        )

    def part_copy(p):
        return pltpu.make_async_remote_copy(
            src_ref=part_out.at[p - 1], dst_ref=part_in.at[p - 1],
            send_sem=part_send.at[p - 1], recv_sem=part_recv.at[p - 1],
            device_id={"tp": there(p, core)}, device_id_type=MESH,
        )

    slots = list(range(1, chips)) + [0]
    for p in slots:
        pair_out[p] = term_of(there(p, 1 - core)).astype(BF16)
        pair_copy(p).start()
    for p in slots:
        term = term_of(there(p, core))
        pair_copy(p).wait_recv()
        term = term + pair_in[p].astype(F32)
        if p:
            part_out[p - 1] = term.astype(BF16)
            part_copy(p).start()
        else:
            result = term
    for p in range(1, chips):
        part_copy(p).wait_recv()
        result = result + part_in[p - 1].astype(F32)
    out[...] = result.astype(BF16)

    for w in range(6):
        def one(step, w=w):
            for side in range(2):
                @pl.when(leaves(side, step + 1))
                def _(side=side):
                    z_copy(w, side, step + 1).wait_send()

                if share and w != GATE:
                    @pl.when(arrives(side, step + 1))
                    def _(side=side):
                        y_copy(w, side, step + 1).wait_send()

        each(n_sp - 1, one)
    for r in range(2):
        @pl.when(place_of(r) < n_sp - 1)
        def _(r=r):
            chain_copy(r).wait_send()
            halo_copy(r).wait_send()
    for step in range(n_tp - 1):
        stat_copy(step).wait_send()
    for p in range(chips):
        pair_copy(p).wait_send()
        if p:
            part_copy(p).wait_send()


def fused(cfg, tok_h, gain_h, wk_h, wg_h, wv_h, wq_h, wa_h, wb_h, ldt_h, hgain_h, ck_h, ng_h, ns_h, od_h, oc_h,
          out,
          gain, ldt, hgain, ck, ng, ns,
          tok, nt, wk, wv, wq, wab, wg, odg, ocg, ldo,
          keys, vals, betas, cums, xinv, gaps, rhs, local_out, reads, maps, ends,
          chain_in, chain_out, gout, gend, main_in, edge_in, pad, conv, stat_out, stat_in,
          dall, dm_out, call, acc_ab, acc_q, acc_k, acc_v,
          local_sem, g_send, g_recv, z_send, z_recv, t_send, ty_recv, tx_recv, tf_recv, tz_recv,
          ld_send, ld_recv, od_send, od_recv, chain_send, chain_recv,
          main_send, main_recv, edge_send, edge_recv, far_send, rim_send,
          stat_send, stat_recv, dg_send, dg_recv, df_send, df_recv, cg_send, cg_recv, cf_send, cf_recv):
    n_sp, n_tp, conv_total = cfg
    grp, sp, tp = lax.axis_index("grp"), lax.axis_index("sp"), lax.axis_index("tp")
    length, width = tok.shape
    rows = wk_h.shape[0]
    head_width = hgain.shape[1]
    cols = wk.shape[1]
    heads = cols // head_width
    channels = wab.shape[1] // 2
    columns = out.shape[1]
    units = [(j, h) for j in range(2) for h in range(heads)]
    n_units = len(units)
    pairs = [(u, r) for u in range(n_units) for r in range(2)]
    chip, core = tp // 2, lax.rem(tp, 2)
    chips = n_tp // 2
    sibling = tp + 1 - 2 * core
    other = 1 - grp
    edge = (sp == 0) | (sp == n_sp - 1)
    inner = (sp > 0) & (sp < n_sp - 1)
    helps = (sp == 1) | (sp == n_sp - 2)
    helper = jnp.where(sp == 0, 1, n_sp - 2)
    helped = jnp.where(sp == 1, 0, n_sp - 1)
    sources = (wk_h, wg_h, wv_h, wq_h, wa_h, wb_h)
    plain = {KEY: wk, VALUE: wv, QUERY: wq}

    def remote(src, dst, send, recv, **where):
        return pltpu.make_async_remote_copy(
            src_ref=src, dst_ref=dst, send_sem=send, recv_sem=recv, device_id=where, device_id_type=MESH
        )

    counts = (4, 1, 2, 2, 1, 1)
    firsts = (0, 0, 4, 6, 8, 9)

    def source(w):
        if w == GATE:
            return wg_h
        size = channels if w in (GLU, OPEN) else cols
        return sources[w].at[:, pl.ds(pl.multiple_of(grp * size, 128), size)]

    def target(w, index, k=None):
        if w == GATE:
            return wg.at[index]
        slab = rows // counts[w]
        if k is None:
            at = pl.ds(pl.multiple_of(index * rows, 16), rows)
        else:
            at = pl.ds(pl.multiple_of(index * rows + k * slab, 16), slab)
        if w in (GLU, OPEN):
            return wab.at[at, pl.ds(channels if w == OPEN else 0, channels)]
        return plain[w].at[at]

    barrier = pltpu.get_barrier_semaphore()

    def greet(**where):
        pl.semaphore_signal(barrier, inc=1, device_id=where, device_id_type=MESH)

    for step in range(n_tp - 1):
        peer = lax.rem(tp + step + 1, n_tp)
        greet(tp=peer)
        greet(tp=peer, grp=other)
    greet(grp=other)

    @pl.when(sp > 0)
    def _():
        greet(sp=sp - 1)
        greet(sp=sp - 1, grp=other)

    @pl.when(sp < n_sp - 1)
    def _():
        greet(sp=sp + 1)
        greet(sp=sp + 1, grp=other)

    load_tok = pltpu.make_async_copy(tok_h, tok, local_sem.at[0])
    load_tok.start()
    small = [
        pltpu.make_async_copy(src, dst, local_sem.at[9 + i])
        for i, (src, dst) in enumerate(
            ((gain_h, gain), (ldt_h, ldt), (hgain_h, hgain), (ng_h, ng), (ns_h, ns),
             (ck_h.at[:, pl.ds(0, channels)], ck.at[0]), (ck_h.at[:, pl.ds(channels, channels)], ck.at[1]))
        )
    ]
    for copy in small:
        copy.start()
    own = [pltpu.make_async_copy(source(w), target(w, sp), local_sem.at[1 + w]) for w in range(6)]
    for copy in own:
        copy.start()

    def od_rows(index):
        return pl.ds(pl.multiple_of(index * columns, 16), columns)

    load_od = pltpu.make_async_copy(od_h.at[od_rows(tp)], odg.at[tp], local_sem.at[7])
    load_oc = pltpu.make_async_copy(oc_h.at[od_rows(tp)], ocg.at[tp], local_sem.at[8])
    load_od.start()
    load_oc.start()

    load_tok.wait()
    for copy in small:
        copy.wait()
    chunk = 64
    for at in range(0, length, chunk):
        here = tok[at:at + chunk, :].astype(F32)
        scale = lax.rsqrt(jnp.mean(here * here, axis=-1, keepdims=True) + EPSILON)
        nt[at:at + chunk, :] = (here * scale * gain[...]).astype(BF16)

    for w in (GATE, KEY):
        own[w].wait()

    @pl.when(edge)
    def _():
        pl.semaphore_wait(barrier, 2 * n_tp + 1)

    @pl.when(inner)
    def _():
        pl.semaphore_wait(barrier, 2 * n_tp + 3)

    def wide(w):
        return 1 if w in (GLU, OPEN) else 0

    def arrives(w, side, d):
        ok = (sp - d >= 0) if side == 0 else (sp + d < n_sp)
        return ok & inner if wide(w) else ok

    def leaves(w, side, d):
        if side == 0:
            return (sp - (d - 1) >= 0) & (sp < n_sp - 1 - wide(w))
        return (sp + (d - 1) < n_sp) & (sp > wide(w))

    def origin(side, d):
        return sp - d if side == 0 else sp + d

    def z_block(w, index, side, k, here=False):
        ahead = sp + 1 if side == 0 else sp - 1
        place = target(w, index, k)
        slot = jnp.where(index > (sp if here else ahead), index - 1, index)
        if w == GATE:
            send, recv = g_send.at[side], g_recv.at[slot]
        else:
            send, recv = z_send.at[side], z_recv.at[slot, firsts[w] + k]
        return remote(place, place, send, recv, sp=ahead)

    def cuts(w):
        return range(counts[w])

    def offer(w, where, ks=None):
        for side in range(2):
            @pl.when(leaves(w, side, 1) & where)
            def _(side=side):
                for k in cuts(w) if ks is None else ks:
                    z_block(w, sp, side, k).start()

    def from_edge(side, d):
        return (sp - d == 0) if side == 0 else (sp + d == n_sp - 1)

    def relay(w, d, kind=None, ks=None):
        if d > n_sp - 1:
            return
        for k in cuts(w) if ks is None else ks:
            for side in range(2):
                onward = leaves(w, side, d + 1) if d < n_sp - 1 else sp < 0
                here = arrives(w, side, d) & onward
                if kind == "edge":
                    here = here & from_edge(side, d)
                if kind == "inner":
                    here = here & ~from_edge(side, d)

                @pl.when(here)
                def _(side=side, k=k):
                    z_block(w, origin(side, d), side, k, True).wait_recv()
                    z_block(w, origin(side, d), side, k).start()

    def drain(w, d):
        for k in cuts(w):
            for side in range(2):
                onward = leaves(w, side, d + 1) if d < n_sp - 1 else sp < 0

                @pl.when(arrives(w, side, d) & ~onward)
                def _(side=side, k=k):
                    z_block(w, origin(side, d), side, k, True).wait_recv()

    pieces = ty_recv.shape[0]
    half = length // 2
    piece = half // pieces
    grains = tz_recv.shape[0]
    grain = half // grains

    def part(block, side, c):
        size = grain if block > 1 else piece
        return nt.at[pl.ds(pl.multiple_of(block * length + side * half + c * size, 16), size)]

    def tok_y(k, c):
        return remote(
            part(2 * k, core, c), part(2 * k + 1, core, c), t_send.at[0], (ty_recv, tx_recv)[k].at[c], grp=other
        )

    def tok_z(c):
        src = nt.at[pl.ds(pl.multiple_of(core * half + c * grain, 16), grain)]
        return remote(src, part(2, core, c), t_send.at[0], tz_recv.at[c], sp=helper)

    def tok_f(block, c):
        return remote(
            part(block, core, c), part(block, core, c), t_send.at[0],
            tf_recv.at[3 if block == 3 and c >= grains // 2 else block - 1], tp=sibling
        )

    def tok_f_arrival(block):
        place = nt.at[pl.ds(pl.multiple_of(block * length + (1 - core) * half, 16), half)]
        return remote(place, place, t_send.at[0], tf_recv.at[block - 1], tp=sibling)

    def tok_late(k):
        start = 3 * length + (1 - core) * half + k * (half // 2)
        place = nt.at[pl.ds(pl.multiple_of(start, 16), half // 2)]
        return remote(place, place, t_send.at[0], tf_recv.at[2 + k], tp=sibling)

    def sent_rows(count):
        place = nt.at[pl.ds(0, count * half)]
        return remote(place, place, t_send.at[0], t_send.at[0], tp=sibling)

    def pass_y(k, c):
        tok_y(k, c).wait_recv()
        tok_f(2 * k + 1, c).start()

    def pass_z(c):
        @pl.when(helps)
        def _():
            tok_z(c).wait_recv()
            tok_y(1, c).start()
            tok_f(2, c).start()

    def pass_far(c):
        @pl.when(helps)
        def _():
            pass_y(1, c)

    ld_copy = remote(ldt, ldo, ld_send.at[0], ld_recv.at[0], grp=other)

    def od_copy(m, step):
        dest = lax.rem(tp + step + 1, n_tp)
        src, dst = ((od_h, odg), (oc_h, ocg))[m]
        return remote(src.at[od_rows(dest)], dst.at[tp], od_send.at[m], od_recv.at[m], tp=dest)

    def od_all(m):
        place = (odg, ocg)[m].at[pl.ds(0, n_tp - 1)]
        return remote(place, place, od_send.at[m], od_recv.at[m], tp=sibling)

    everywhere = sp >= 0
    offer(GATE, everywhere)
    offer(KEY, everywhere)
    for c in range(pieces):
        tok_y(0, c).start()
    ld_copy.start()
    for w in (VALUE, GLU, OPEN, QUERY):
        own[w].wait()
    offer(VALUE, edge)
    offer(GLU, edge)
    for first in (0, grains // 2):
        @pl.when(edge)
        def _(first=first):
            for c in range(first, first + grains // 2):
                tok_z(c).start()

        if first == 0:
            offer(OPEN, edge)

    offer(QUERY, edge)
    for m in (1, 0):
        for step in range(n_tp - 1):
            od_copy(m, step).start()

    def dot(a, b, dims=NN):
        return lax.dot_general(a, b, dims, preferred_element_type=F32)

    def unit_rows(tensor):
        return tensor * lax.rsqrt(jnp.sum(tensor * tensor, axis=-1, keepdims=True) + EPSILON)

    def silu(tensor):
        return tensor * jax.nn.sigmoid(tensor)

    def block_dot(first, count, w_ref, index):
        lanes = pl.ds(pl.multiple_of(index * rows, 128), rows)
        at = pl.ds(pl.multiple_of(index * rows, 128), rows)
        return dot(nt[first * length:(first + count) * length, lanes], w_ref[at, :])

    def neighbours(w, d, action):
        for side in range(2):
            @pl.when(arrives(w, side, d))
            def _(side=side):
                action(sp - d if side == 0 else sp + d)

    def adder(acc, w_ref, first, count):
        span = slice(first * length, (first + count) * length)

        def add(index, fresh=False):
            x = block_dot(first, count, w_ref, index)
            acc[span, :] = x if fresh else acc[span, :] + x

        return add

    row_at = lax.broadcasted_iota(jnp.int32, (length, length), 0)
    col_at = lax.broadcasted_iota(jnp.int32, (length, length), 1)
    same = row_at == col_at
    mine = grp == 0
    gates = 4 * heads

    def weights_of(j):
        span = slice(j * length, (j + 1) * length)
        cols_part = jnp.zeros((length, wg.shape[1]), F32)
        for index in range(n_sp):
            cols_part = cols_part + dot(nt[span, index * rows:(index + 1) * rows], wg[index], NT)
        rows_part = jnp.transpose(cols_part)
        gate_cols = jnp.where(mine, cols_part[:, :gates], cols_part[:, gates:])
        gate_rows = jnp.where(mine, rows_part[:gates, :], rows_part[gates:, :])
        log = (ldt, ldo)[j]
        rates = jnp.where(mine, log[:2 * heads, :], log[2 * heads:, :])
        for h in range(heads):
            for r in range(2):
                p = 2 * (j * heads + h) + r
                g = 4 * h + 2 * r
                decay_row = rates[2 * h + r:2 * h + r + 1, :] * (0.5 + jax.nn.sigmoid(gate_rows[g:g + 1, :]))
                beta = jax.nn.sigmoid(gate_cols[:, g + 1:g + 2] - BETA_SHIFT)
                seen = col_at <= row_at if r == 0 else col_at >= row_at
                cum_col = jnp.sum(jnp.where(seen, decay_row, 0.0), axis=1, keepdims=True)
                cum_row = jnp.sum(jnp.where(same, cum_col, 0.0), axis=0, keepdims=True)
                gaps[p] = jnp.where(seen, jnp.exp(jnp.where(seen, cum_col - cum_row, 0.0)), 0.0)
                betas[p] = jnp.broadcast_to(beta, (length, head_width))
                cums[p] = jnp.broadcast_to(cum_col, (length, head_width))

    add_key = [adder(acc_k, wk, j, 1) for j in range(2)]
    add_value = [adder(acc_v, wv, j, 1) for j in range(2)]

    relay(GATE, 1)
    relay(KEY, 1, None, (0, 1))
    offer(VALUE, inner, (0,))
    relay(KEY, 1, None, (2, 3))
    offer(VALUE, inner, (1,))
    offer(GLU, inner)
    relay(GATE, 2)
    pass_y(0, 0)
    for d in range(2, n_sp - 1):
        relay(KEY, d, None, (0, 1))
    relay(VALUE, 1, None, (0,))
    for d in range(2, n_sp - 1):
        relay(KEY, d, None, (2, 3))
    pass_y(0, 1)
    relay(VALUE, 1, None, (1,))
    offer(OPEN, inner)
    def pass_value():
        for d in range(2, n_sp - 1):
            relay(VALUE, d)

    drain(KEY, 1)
    add_key[0](sp, True)
    neighbours(KEY, 1, add_key[0])
    pass_y(0, 2)
    offer(QUERY, inner)
    drain(VALUE, 1)
    add_value[0](sp, True)
    neighbours(VALUE, 1, add_value[0])
    relay(GLU, 1)
    for d in range(1, n_sp):
        drain(GATE, d)
    weights_of(0)
    pass_y(0, 3)
    for d in range(2, n_sp - 1):
        drain(KEY, d)
        neighbours(KEY, d, add_key[0])
    ld_copy.wait_recv()
    tok_f_arrival(1).wait_recv()
    pass_z(0)
    weights_of(1)
    pass_z(1)
    pass_z(2)
    add_key[1](sp, True)
    for d in range(1, n_sp - 1):
        neighbours(KEY, d, add_key[1])
    add_value[1](sp, True)
    neighbours(VALUE, 1, add_value[1])
    pass_z(3)
    drain(KEY, n_sp - 1)
    neighbours(KEY, n_sp - 1, adder(acc_k, wk, 0, 2))
    pass_value()

    both = 2 * length
    key_proj = silu(acc_k[...])
    for u, (j, h) in enumerate(units):
        keys[u] = unit_rows(key_proj[j * length:(j + 1) * length, h * head_width:(h + 1) * head_width])
    near = row_at // 2 == col_at // 2
    for u in range(n_units):
        grams = bdot(keys[u], keys[u], NT)
        for r in range(2):
            p = 2 * u + r
            beta = jnp.concatenate([betas[p]] * (length // head_width), axis=1)
            lower = jnp.where(same, 0.0, grams * gaps[p] * beta)
            rhs[p] = lower
            xinv[p] = jnp.where(same, 1.0, jnp.where(near, -lower, 0.0))

    service = {
        8: [lambda: relay(OPEN, 1)],
        32: [lambda: pass_z(4)],
        128: [lambda: pass_z(5)],
    }
    size = 2
    while size < length:
        inside = (row_at // (2 * size) == col_at // (2 * size)) & (row_at // size != col_at // size)
        for p in range(len(pairs)):
            across = jnp.where(inside, rhs[p], 0.0)
            inverse = xinv[p]
            xinv[p] = inverse - bdot(inverse, bdot(across, inverse))
        for act in service.get(size, ()):
            act()
        size *= 2

    for d in range(2, n_sp):
        drain(VALUE, d)
        neighbours(VALUE, d, adder(acc_v, wv, 0, 2))
    value_proj = silu(acc_v[...])
    eye = (
        lax.broadcasted_iota(jnp.int32, (head_width, head_width), 0)
        == lax.broadcasted_iota(jnp.int32, (head_width, head_width), 1)
    )
    for u, r in pairs:
        p = 2 * u + r
        j, h = units[u]
        beta, cum, key = betas[p], cums[p], keys[u]
        value = value_proj[j * length:(j + 1) * length, h * head_width:(h + 1) * head_width]
        total = cum[length - 1:length, :] if r == 0 else cum[0:1, :]
        right = jnp.concatenate([beta * value, beta * key * jnp.exp(cum)], axis=1)
        solved = bdot(xinv[p], right)
        vals[p] = solved.astype(BF16)
        passed = bdot(key * jnp.exp(total - cum), solved, TN)
        ends[p] = passed[:, :head_width]
        maps[p] = (jnp.where(eye, jnp.exp(total), 0.0) - passed[:, head_width:]).astype(BF16)

    def place_of(r):
        return sp if r == 0 else n_sp - 1 - sp

    def chain_copy(r):
        dest = sp + 1 if r == 0 else sp - 1
        return remote(chain_out.at[r], chain_in.at[r], chain_send.at[r], chain_recv.at[r], sp=dest)

    def chain_point(low, high):
        for r in range(2):
            at = place_of(r)

            @pl.when((at >= low) & (at <= high))
            def _(r=r, at=at):
                if low == 0:
                    for u in range(n_units):
                        chain_in[r, u] = jnp.zeros((head_width, head_width), BF16)
                        chain_out[r, u] = ends[2 * u + r].astype(BF16)
                else:
                    chain_copy(r).wait_recv()
                    for u in range(n_units):
                        p = 2 * u + r
                        chain_out[r, u] = (bdot(maps[p], chain_in[r, u]) + ends[p]).astype(BF16)

                @pl.when(at < n_sp - 1)
                def _():
                    chain_copy(r).start()

    chain_point(0, 0)
    pass_z(6)
    relay(QUERY, 1, "inner")
    add_near = adder(acc_ab, wab, 0, 2)
    add_query = adder(acc_q, wq, 0, 2)
    drain(GLU, 1)
    drain(OPEN, 1)

    @pl.when(inner)
    def _():
        add_near(sp, True)

    pass_z(7)
    for c in range(4):
        pass_far(c)
    neighbours(GLU, 1, add_near)
    relay(QUERY, 1, "edge", (0,))
    pass_far(4)
    relay(QUERY, 1, "edge", (1,))
    pass_far(5)
    for d in range(2, n_sp - 1):
        for w in (GLU, OPEN):
            relay(w, d)
            drain(w, d)
        neighbours(GLU, d, add_near)

    def gated(x):
        return (x[:, :channels] * jax.nn.sigmoid(x[:, channels:])).astype(BF16)

    def owner(j):
        return grp if j == 0 else other

    def main_y():
        return remote(gout, main_in.at[grp], main_send.at[0], main_recv.at[grp], grp=other)

    def main_arrival(h):
        return remote(main_in.at[h], main_in.at[h], main_send.at[0], main_recv.at[h], grp=other)

    def far_copy(j):
        return remote(gend.at[j], main_in.at[grp], far_send.at[0], main_recv.at[grp], sp=helped, grp=owner(j))

    def edge_copy(side, j):
        start = length - HALO if side == 0 else 0
        src = main_in.at[grp, pl.ds(start, HALO)] if j == 0 else gout.at[pl.ds(start, HALO)]
        return remote(
            src, edge_in.at[side, grp], edge_send.at[0], edge_recv.at[side, grp],
            sp=sp + 1 if side == 0 else sp - 1, grp=owner(j),
        )

    def rim_copy(side):
        start = length - HALO if side == 0 else 0
        return remote(
            gend.at[1, pl.ds(start, HALO)], edge_in.at[side, grp], rim_send.at[0], edge_recv.at[side, grp], grp=other
        )

    def edge_arrival(side, h):
        place = edge_in.at[side, h]
        return remote(place, place, edge_send.at[0], edge_recv.at[side, h], grp=other)

    @pl.when(inner)
    def _():
        near_rows = gated(acc_ab[...])
        main_in[grp] = near_rows[:length]
        gout[...] = near_rows[length:]
        main_y().start()
        for side in range(2):
            for j in range(2):
                edge_copy(side, j).start()

    def give_far(j):
        gend[j] = gated(dot(nt[(2 + j) * length:(3 + j) * length, :], wab[...]))
        far_copy(j).start()

    def give_late(k):
        tok_late(k).wait_recv()
        size = half // 2
        spots = (k * size, half + k * size)
        x = jnp.concatenate([nt[3 * length + at:3 * length + at + size, :] for at in spots], axis=0)
        late = gated(dot(x, wab[...]))
        for i, at in enumerate(spots):
            gend[1, at:at + size, :] = late[i * size:(i + 1) * size]
        for at in spots:
            remote(
                gend.at[1, pl.ds(at, size)], main_in.at[grp, pl.ds(at, size)],
                far_send.at[0], main_recv.at[grp], sp=helped, grp=other,
            ).start()

    @pl.when(helps)
    def _():
        tok_f_arrival(2).wait_recv()
        give_far(0)
        give_late(0)
        for side, at in ((0, 1), (1, n_sp - 2)):
            @pl.when(sp == at)
            def _(side=side):
                start = length - HALO if side == 0 else 0
                edge_in[side, grp] = gend[0, start:start + HALO, :]

    pass_far(6)
    chain_point(1, 1)
    pass_far(7)

    @pl.when(helps)
    def _():
        give_late(1)
        for side, at in ((0, 1), (1, n_sp - 2)):
            @pl.when(sp == at)
            def _(side=side):
                rim_copy(side).start()

    for d in range(2, n_sp - 1):
        relay(QUERY, d)
        chain_point(d, d)
    drain(QUERY, 1)
    add_query(sp, True)
    neighbours(QUERY, 1, add_query)
    for d in range(2, n_sp - 1):
        drain(QUERY, d)
        neighbours(QUERY, d, add_query)

    taps = ck.shape[1]
    for step in range(2):
        h = grp if step == 0 else other
        skip = sp < 0 if step else sp >= 0

        @pl.when(edge if step == 0 else sp >= 0)
        def _(h=h):
            main_arrival(h).wait_recv()

        @pl.when((sp > 0) & ~((sp == 1) & skip))
        def _(h=h):
            edge_arrival(0, h).wait_recv()

        @pl.when((sp < n_sp - 1) & ~((sp == n_sp - 2) & skip))
        def _(h=h):
            edge_arrival(1, h).wait_recv()

        pad[step, HALO:HALO + length, :] = main_in[h].astype(F32)
        for side, start, none in ((0, 0, 0), (1, HALO + length, n_sp - 1)):
            @pl.when(sp != none)
            def _(h=h, step=step, side=side, start=start):
                pad[step, start:start + HALO, :] = edge_in[side, h].astype(F32)

            @pl.when(sp == none)
            def _(step=step, start=start):
                pad[step, start:start + HALO, :] = jnp.zeros((HALO, channels), F32)

        for at in range(0, length, chunk):
            first = at + HALO - taps // 2
            total = pad[step, first:first + chunk, :] * ck[h, 0:1, :]
            for k in range(1, taps):
                total = total + pad[step, first + k:first + k + chunk, :] * ck[h, k:k + 1, :]
            conv[h, at:at + chunk, :] = total
    filtered = jnp.concatenate([conv[0], conv[1]], axis=1)
    sum_col = jnp.sum(filtered, axis=-1, keepdims=True)
    square_col = jnp.sum(filtered * filtered, axis=-1, keepdims=True)
    stat_out[...] = jnp.zeros(stat_out.shape, F32)
    stat_out[0:1, :] = jnp.sum(jnp.where(same, sum_col, 0.0), axis=0, keepdims=True)
    stat_out[1:2, :] = jnp.sum(jnp.where(same, square_col, 0.0), axis=0, keepdims=True)

    def stat_copy(step):
        return remote(
            stat_out, stat_in.at[step], stat_send.at[0], stat_recv.at[0], tp=lax.rem(tp + step + 1, n_tp)
        )

    for step in range(n_tp - 1):
        stat_copy(step).start()

    def chip_at(q):
        return lax.rem(chip + q, chips)

    def chip_back(q):
        return lax.rem(chip + chips - q, chips)

    def dg_copy(a, q):
        src = dall.at[tp, grp] if a == 0 else dm_out
        where = {"tp": chip_at(q) * 2 + core}
        if a:
            where["grp"] = other
        return remote(src, dall.at[tp, grp], dg_send.at[a], dg_recv.at[a, q], **where)

    def d_block(a, q, side):
        return dall.at[chip_back(q) * 2 + side, other if a else grp]

    def dg_arrival(a, q):
        place = d_block(a, q, core)
        return remote(place, place, dg_send.at[a], dg_recv.at[a, q], tp=sibling)

    def df_copy(a, q):
        place = d_block(a, q, core)
        return remote(place, place, df_send.at[0], df_recv.at[q], tp=sibling)

    def df_arrival(q):
        place = dall.at[chip_back(q) * 2 + 1 - core]
        return remote(place, place, df_send.at[0], df_recv.at[q], tp=sibling)

    def cg_copy(q):
        return remote(call.at[tp], call.at[tp], cg_send.at[0], cg_recv.at[q], tp=chip_at(q) * 2 + core)

    def cg_arrival(q):
        place = call.at[chip_back(q) * 2 + core]
        return remote(place, place, cg_send.at[0], cg_recv.at[q], tp=sibling)

    def cf_copy(q, arriving=False):
        place = call.at[chip_back(q) * 2 + (1 - core if arriving else core)]
        return remote(place, place, cf_send.at[0], cf_recv.at[q], tp=sibling)

    stats = stat_out[0:2, :]
    stat_all = remote(stat_in, stat_in, stat_send.at[0], stat_recv.at[0], tp=sibling)
    stat_all.wait_recv()
    for step in range(n_tp - 1):
        stats = stats + stat_in[step, 0:2, :]
    center = jnp.sum(jnp.where(same, stats[0:1, :], 0.0), axis=1, keepdims=True) / conv_total
    squares = jnp.sum(jnp.where(same, stats[1:2, :], 0.0), axis=1, keepdims=True) / conv_total
    spread = squares - center * center
    normal = (jnp.concatenate([conv[0], conv[1]], axis=1) - center) * lax.rsqrt(spread + EPSILON)
    call[tp] = silu(normal * ng[...] + ns[...]).astype(BF16)
    for q in range(1, chips):
        cg_copy(q).start()
    cf_copy(0).start()

    def delta_term(t):
        return dot(jnp.concatenate([dall[t, 0], dall[t, 1]], axis=1), odg[t], NT)

    def conv_term(t):
        return dot(call[t], ocg[t], NT)

    drain(QUERY, n_sp - 1)
    neighbours(QUERY, n_sp - 1, add_query)

    def read(u):
        j, h = units[u]
        query = silu(acc_q[j * length:(j + 1) * length, h * head_width:(h + 1) * head_width])
        query = unit_rows(query) * head_width ** -0.5
        scores = bdot(query, keys[u], NT)
        for r in range(2):
            p = 2 * u + r
            pair = dot((scores * gaps[p]).astype(BF16), vals[p])
            reads[p] = (query * jnp.exp(cums[p]) - pair[:, head_width:]).astype(BF16)
            if r == 0:
                local_out[u] = pair[:, :head_width]
            else:
                local_out[u] = local_out[u] + pair[:, :head_width]

    def mixed_head(u):
        joined = local_out[u] + dot(reads[2 * u], chain_in[0, u]) + dot(reads[2 * u + 1], chain_in[1, u])
        scale = lax.rsqrt(jnp.mean(joined * joined, axis=-1, keepdims=True) + EPSILON)
        return (joined * scale * hgain[...]).astype(BF16)

    direct = [(a, q) for q in range(chips) for a in (1, 0) if (a, q) != (0, 0)]

    for u in range(n_units):
        read(u)
    chain_point(n_sp - 1, n_sp - 1)
    for h in range(heads):
        dm_out[:, h * head_width:(h + 1) * head_width] = mixed_head(heads + h)
    for q in range(chips - 1, -1, -1):
        dg_copy(1, q).start()
    for h in range(heads):
        dall[tp, grp, :, h * head_width:(h + 1) * head_width] = mixed_head(h)
    for q in range(1, chips):
        dg_copy(0, q).start()
    df_copy(0, 0).start()

    for m in range(2):
        od_all(m).wait_recv()
    load_od.wait()
    load_oc.wait()
    result = conv_term(tp)
    for q in range(1, chips):
        cg_arrival(q).wait_recv()
        cf_copy(q).start()
    for q in range(1, chips):
        result = result + conv_term(chip_back(q) * 2 + core)
    for a, q in direct:
        dg_arrival(a, q).wait_recv()
        df_copy(a, q).start()
        if (a, q) == (1, 0):
            for p in range(chips):
                cf_copy(p, True).wait_recv()
                result = result + conv_term(chip_back(p) * 2 + 1 - core)
            result = result + delta_term(tp)
    for q in range(1, chips):
        result = result + delta_term(chip_back(q) * 2 + core)
    for q in range(chips):
        df_arrival(q).wait_recv()
        result = result + delta_term(chip_back(q) * 2 + 1 - core)
    out[...] = result.astype(BF16)

    for side in range(2):
        for q in range(n_sp):
            far = n_sp - 1 if side == 0 else 0
            copies = 0 if q == far else (q + 1 if side == 0 else n_sp - q)
            wide_to = n_sp - 2 if side == 0 else 1
            wide_copies = copies if (q < wide_to if side == 0 else q > wide_to) else 0
            if copies:
                @pl.when(sp == q)
                def _(side=side, copies=copies, wide_copies=wide_copies):
                    place = wg.at[pl.ds(0, copies)]
                    remote(place, place, g_send.at[side], g_send.at[side], tp=sibling).wait_send()
                    total = (3 * cols * copies + 2 * channels * wide_copies) * rows // width
                    place = nt.at[pl.ds(0, total)]
                    remote(place, place, z_send.at[side], z_send.at[side], tp=sibling).wait_send()
    @pl.when(edge)
    def _():
        sent_rows(3).wait_send()

    @pl.when(inner & ~helps)
    def _():
        sent_rows(2).wait_send()

    @pl.when(helps)
    def _():
        sent_rows(5).wait_send()
        remote(gend, gend, far_send.at[0], far_send.at[0], tp=sibling).wait_send()
        rim_copy(0).wait_send()

    ld_copy.wait_send()
    for m in range(2):
        od_all(m).wait_send()
    for r in range(2):
        @pl.when(place_of(r) < n_sp - 1)
        def _(r=r):
            chain_copy(r).wait_send()

    @pl.when(inner)
    def _():
        main_y().wait_send()
        remote(edge_in, edge_in, edge_send.at[0], edge_send.at[0], tp=sibling).wait_send()

    stat_all.wait_send()
    place = dall.at[pl.ds(0, chips), 0]
    remote(place, place, dg_send.at[1], dg_send.at[1], tp=sibling).wait_send()
    if chips > 1:
        place = dall.at[pl.ds(0, chips - 1), 0]
        remote(place, place, dg_send.at[0], dg_send.at[0], tp=sibling).wait_send()
        place = call.at[pl.ds(0, chips - 1)]
        remote(place, place, cg_send.at[0], cg_send.at[0], tp=sibling).wait_send()
    place = dall.at[pl.ds(0, chips)]
    remote(place, place, df_send.at[0], df_send.at[0], tp=sibling).wait_send()
    place = call.at[pl.ds(0, chips)]
    remote(place, place, cf_send.at[0], cf_send.at[0], tp=sibling).wait_send()


def solution(mesh):
    n_grp, n_sp, n_tp = mesh.shape["grp"], mesh.shape["sp"], mesh.shape["tp"]

    def on_device(tokens_in, input_gain, w_query, w_key, w_value, w_gates, w_glu_value,
                  sigmoid_opener_matrix, log_decay, head_gain, conv_kernel, norm_gain, norm_shift,
                  out_delta, out_conv):
        length, width = tokens_in.shape
        head_width = head_gain.shape[0]
        head_cols = w_query.shape[1]
        heads = head_cols // head_width
        channels = w_glu_value.shape[1]
        rows = w_query.shape[0]
        pairs = 2 * heads
        columns = width // n_tp
        dma, vmem = pltpu.SemaphoreType.DMA, pltpu.VMEM
        anywhere = pl.BlockSpec(memory_space=pltpu.HBM)
        inside = pl.BlockSpec(memory_space=pltpu.VMEM)
        if n_grp == 2 and n_sp >= 4 and n_tp % 2 == 0 and heads % 2 == 0 and channels % 256 == 0                 and (3 * head_cols + 2 * channels) * rows * n_sp <= 8 * length * width:
            cols, ch, chips, steps = head_cols // 2, channels // 2, n_tp // 2, n_tp - 1
            pieces = 4
            scratch = [
                vmem((1, width), F32), vmem((pairs, length), F32), vmem((1, head_width), F32),
                vmem((2, conv_kernel.shape[0], ch), F32), vmem((1, channels), F32), vmem((1, channels), F32),
                vmem((length, width), BF16), vmem((4 * length, width), BF16),
                vmem((width, cols), BF16), vmem((width, cols), BF16), vmem((width, cols), BF16),
                vmem((width, 2 * ch), BF16), vmem((n_sp, 4 * heads, rows), BF16),
                vmem((n_tp, columns, head_cols), BF16), vmem((n_tp, columns, channels), BF16),
                vmem((pairs, length), F32),
                vmem((heads, length, head_width), F32), vmem((pairs, length, 2 * head_width), BF16),
                vmem((pairs, length, head_width), F32), vmem((pairs, length, head_width), F32),
                vmem((pairs, length, length), F32), vmem((pairs, length, length), F32),
                vmem((pairs, length, length), F32),
                vmem((heads, length, head_width), F32), vmem((pairs, length, head_width), BF16),
                vmem((pairs, head_width, head_width), BF16), vmem((pairs, head_width, head_width), F32),
                vmem((2, heads, head_width, head_width), BF16), vmem((2, heads, head_width, head_width), BF16),
                vmem((length, ch), BF16), vmem((2, length, ch), BF16), vmem((2, length, ch), BF16),
                vmem((2, 2, HALO, ch), BF16),
                vmem((2, length + 2 * HALO, ch), F32), vmem((2, length, ch), F32),
                vmem((8, length), F32), vmem((steps, 8, length), F32),
                vmem((n_tp, 2, length, cols), BF16), vmem((length, cols), BF16),
                vmem((n_tp, length, channels), BF16), vmem((2 * length, 2 * ch), F32), vmem((2 * length, cols), F32),
                vmem((2 * length, cols), F32), vmem((2 * length, cols), F32),
                dma((16,)),
                dma((2,)), dma((n_sp - 1,)), dma((2,)), dma((n_sp - 1, 10)),
                dma((1,)), dma((pieces,)), dma((2 * pieces,)), dma((4,)), dma((2 * pieces,)),
                dma((1,)), dma((1,)), dma((2,)), dma((2,)), dma((2,)), dma((2,)),
                dma((1,)), dma((2,)), dma((1,)), dma((2, 2)), dma((1,)), dma((1,)),
                dma((1,)), dma((1,)),
                dma((2,)), dma((2, chips)), dma((1,)), dma((chips,)),
                dma((1,)), dma((chips,)), dma((1,)), dma((chips,)),
            ]
            return pl.pallas_call(
                functools.partial(fused, (n_sp, n_tp, float(channels * n_tp))),
                out_shape=pltpu.VMEM((length, columns), BF16),
                in_specs=[anywhere] * 15,
                out_specs=inside,
                scratch_shapes=scratch,
                compiler_params=pltpu.CompilerParams(
                    collective_id=0, has_side_effects=True, vmem_limit_bytes=58 * 1024 * 1024
                ),
            )(
                tokens_in, input_gain.reshape(1, width), w_key, w_gates.T, w_value, w_query,
                w_glu_value, sigmoid_opener_matrix, log_decay.T,
                head_gain.reshape(1, head_width), conv_kernel, norm_gain.reshape(1, channels),
                norm_shift.reshape(1, channels), out_delta, out_conv,
            )
        scratch = [
            vmem((length, width), BF16), vmem((length, width), BF16),
            vmem((width, head_cols), BF16), vmem((n_sp, 4 * heads, rows), BF16),
            vmem((width, head_cols), BF16), vmem((width, head_cols), BF16),
            vmem((width, channels), BF16), vmem((width, channels), BF16),
            vmem((width, head_cols), BF16), vmem((width, channels), BF16),
            vmem((heads, length, head_width), F32), vmem((pairs, length, 2 * head_width), BF16),
            vmem((pairs, length, head_width), F32), vmem((pairs, length, head_width), F32),
            vmem((pairs, length, length), F32), vmem((pairs, length, length), F32),
            vmem((pairs, length, length), F32),
            vmem((heads, length, head_width), F32), vmem((pairs, length, head_width), BF16),
            vmem((pairs, head_width, head_width), BF16), vmem((pairs, head_width, head_width), F32),
            vmem((2, heads, head_width, head_width), BF16), vmem((2, heads, head_width, head_width), BF16),
            vmem((length, channels), BF16), vmem((2, HALO, channels), BF16),
            vmem((length + 2 * HALO, channels), F32), vmem((length, channels), F32),
            vmem((8, length), F32), vmem((n_tp - 1, 8, length), F32),
            vmem((n_tp, length, columns), F32),
            vmem((n_tp // 2, length, columns), BF16), vmem((n_tp // 2, length, columns), BF16),
            vmem((n_tp // 2, length, columns), BF16), vmem((n_tp // 2, length, columns), BF16),
            dma((9,)),
            dma((6, 2, n_sp - 1)), dma((6, 2, n_sp - 1)),
            dma((6, 2, n_sp - 1)), dma((6, 2, n_sp - 1)),
            dma((2,)), dma((2,)), dma((2,)), dma((2,)),
            dma((n_tp - 1,)), dma((n_tp - 1,)), dma((n_tp // 2,)), dma((n_tp // 2,)),
            dma((n_tp // 2,)), dma((n_tp // 2,)),
        ]
        return pl.pallas_call(
            functools.partial(kernel, (n_grp, n_sp, n_tp, float(channels * n_tp))),
            out_shape=jax.ShapeDtypeStruct((length, columns), BF16),
            in_specs=[anywhere, inside] + [anywhere] * 6 + [inside] * 6 + [anywhere] * 2,
            out_specs=inside,
            scratch_shapes=scratch,
            compiler_params=pltpu.CompilerParams(
                collective_id=0, has_side_effects=True, vmem_limit_bytes=60 * 1024 * 1024
            ),
        )(
            tokens_in, input_gain.reshape(1, width), w_key, w_gates.T, w_value, w_query,
            w_glu_value, sigmoid_opener_matrix, log_decay, log_decay.T,
            head_gain.reshape(1, head_width), conv_kernel, norm_gain.reshape(1, channels),
            norm_shift.reshape(1, channels), out_delta, out_conv,
        )

    placed = (
        P(("grp", "sp"), None), P(), P("sp", "tp"), P("sp", "tp"), P("sp", "tp"), P("sp", "tp"),
        P("sp", "tp"), P("sp", "tp"), P(("grp", "sp"), "tp"), P(), P(None, "tp"), P("tp"), P("tp"),
        P(None, "tp"), P(None, "tp"),
    )
    return jax.shard_map(
        on_device, mesh=mesh, in_specs=placed, out_specs=P(("grp", "sp"), "tp"), check_vma=False
    )
```
